256 devices in a mesh: kv: 32 (over z, y), tp: 8 (over x, core).
Axes of the slice: x: 4, y: 4, z: 8, core: 2. Of those that a mesh axis runs over, the one named last changes fastest.
Arguments:
- tokens: bfloat16 [64, 4096], P(None, ('kv', 'tp')), may hold values from -8 to 8
- gate_weights: bfloat16 [2, 4096, 11264], P(None, None, ('kv', 'tp')), may hold values from -0.09375 to 0.09375
- up_weights: bfloat16 [2, 4096, 11264], P(None, None, ('kv', 'tp')), may hold values from -0.09375 to 0.09375
- down_weights: bfloat16 [2, 11264, 4096], P(None, ('kv', 'tp')), may hold values from -1 to 1
- norm_gain: bfloat16 [3, 4096], P(None, ('kv', 'tp')), may hold values from 0.25 to 4.5
- norm_bias: bfloat16 [3, 4096], P(None, ('kv', 'tp')), may hold values from -3 to 3
- query_weight: bfloat16 [4096, 4096], P('kv', 'tp'), may hold values from -0.09375 to 0.09375
- forget_weight: bfloat16 [4096, 4096], P('kv', 'tp'), may hold values from -0.09375 to 0.09375
- input_weight: bfloat16 [4096, 4096], P('kv', 'tp'), may hold values from -0.09375 to 0.09375
- outgate_weight: bfloat16 [4096, 4096], P('kv', 'tp'), may hold values from -0.09375 to 0.09375
- lower_bound: float32 [4096], P('tp'), may hold values from 0.05 to 0.9
- head_gain: float32 [4096], P('tp'), may hold values from 0.1 to 1.9
- out_weight: bfloat16 [4096, 4096], P('tp'), may hold values from -0.25 to 0.25
- state: float32 [64, 32, 128, 128], P('kv', 'tp'), may hold values from -3 to 3
Outputs:
- mixed: bfloat16 [64, 4096], P(None, ('kv', 'tp'))
- new_state: float32 [64, 32, 128, 128], P('kv', 'tp')
The draws below stay inside these ranges and needn't reach their ends.
All inputs are finite; a program needn't handle non-finite values.
Results may differ from the reference program's by a relative error of at most 0.022.
Values may be sent and summed in bfloat16 or wider, within the bound.
No kernel may reach another device: no remote copies, remote signals or barrier semaphores. Data moves between devices by JAX's collectives and lax.ppermute only.
A program may use at most 64 MiB of HBM per device.

```python
import math
import jax
import jax.numpy as jnp
from jax import lax

D = 4096
FF = 11264
HEAD = 128
HEADS = 32
BATCH = 64


def draw_tokens(key, part):
    position = jnp.arange(D, dtype=jnp.float32)[None, :] / D
    values = jax.random.normal(key, (BATCH, D), jnp.float32) * 0.4 * 4.0 ** position
    return jnp.clip(values, -8.0, 8.0).astype(jnp.bfloat16)


def draw_norm_gain(key, part):
    position = jnp.arange(D, dtype=jnp.float32)[None, :] / D
    jitter = 1.0 + 0.3 * jax.random.uniform(key, (3, D), jnp.float32, -1.0, 1.0)
    values = 0.6 * 3.0 ** position * jitter
    return values.astype(jnp.bfloat16)


def with_spikes(result, own_key, source, target, parts, factor):
    owner, partner = [(jnp.arange(result.shape[dim]) // (result.shape[dim] // parts)).reshape([-1 if axis == dim else 1 for axis in range(result.ndim)]) for dim in (source, target)]
    chosen = jax.random.permutation(own_key, parts)[partner]
    strong = (owner == chosen) | (owner == (partner + parts // 2) % parts)
    return jnp.where(strong, factor * result, result)


def block_scale(key, dims, cuts, least, top_value):
    factor_of, own = 1.0, jax.random.fold_in(key, 6)
    for dim, blocks in cuts:
        steps = jnp.exp(jax.random.uniform(jax.random.fold_in(own, dim), (blocks,), jnp.float32, least / len(cuts), top_value / len(cuts)))
        factor_of = factor_of * jnp.repeat(steps, dims[dim] // blocks).reshape([-1 if axis == dim else 1 for axis in range(len(dims))])
    return factor_of


def noise(rng, shape, scale, bound, cuts=(), held_as=jnp.bfloat16):
    drawn = scale * jax.random.normal(rng, shape, jnp.float32)
    if cuts:
        drawn = drawn * block_scale(rng, shape, cuts, -0.22, 0.18)
    return jnp.clip(drawn, -bound, bound).astype(held_as)


def noise_with(rng, shape, scale, reach, cuts, heavy, held_as=jnp.bfloat16):
    array = scale * jax.random.normal(rng, shape, jnp.float32)
    if cuts:
        array = array * block_scale(rng, shape, cuts, -0.22, 0.18)
    return jnp.clip(with_spikes(array, jax.random.fold_in(rng, 3), *heavy), -reach, reach).astype(held_as)


def setup_inputs(seed: int = 0) -> dict:
    arg_keys = jax.random.split(jax.random.key(seed), 15)
    tokens = draw_tokens(jax.random.fold_in(arg_keys[14], 71), 0)
    gate_weights = noise(arg_keys[1], (2, D, FF), D ** -0.5, 0.09375, ((2, 256),))
    up_weights = noise(arg_keys[2], (2, D, FF), D ** -0.5, 0.09375, ((2, 256),))
    down_weights = noise_with(arg_keys[3], (2, FF, D), (FF // 16) ** -0.5, 1.0, ((1, 256),), (1, 2, 256, 6.0))
    norm_gain = draw_norm_gain(jax.random.fold_in(arg_keys[14], 71), 0)
    norm_bias = noise(arg_keys[5], (3, D), 0.5, 3.0, ((1, 256),))
    query_weight = noise(arg_keys[6], (D, D), D ** -0.5, 0.09375, ((0, 32), (1, 8)))
    forget_weight = noise(arg_keys[7], (D, D), D ** -0.5, 0.09375, ((0, 32), (1, 8)))
    input_weight = noise(arg_keys[8], (D, D), D ** -0.5, 0.09375, ((0, 32), (1, 8)))
    outgate_weight = noise(arg_keys[9], (D, D), D ** -0.5, 0.09375, ((0, 32), (1, 8)))
    lower_bound = jnp.clip(jnp.exp(math.log(0.9) - 2.8903717 * jax.random.uniform(arg_keys[10], (D,), jnp.float32) ** block_scale(arg_keys[10], (D,), ((0, 8),), -0.2, 0.2)), 0.05, 0.9)
    head_gain = jnp.clip(1.0 + 0.18 * jax.random.normal(arg_keys[11], (D,), jnp.float32), 0.1, 1.9)
    out_weight = noise_with(arg_keys[12], (D, D), (D // 4) ** -0.5, 0.25, ((0, 8),), (0, 1, 8, 2.0))
    state = noise(arg_keys[13], (BATCH, HEADS, HEAD, HEAD), 0.5, 3.0, ((0, 32), (1, 8)), jnp.float32)
    return {"tokens": tokens, "gate_weights": gate_weights, "up_weights": up_weights, "down_weights": down_weights, "norm_gain": norm_gain, "norm_bias": norm_bias, "query_weight": query_weight, "forget_weight": forget_weight, "input_weight": input_weight, "outgate_weight": outgate_weight, "lower_bound": lower_bound, "head_gain": head_gain, "out_weight": out_weight, "state": state}


residual_scale = 8.0 ** 0.25
norm_eps = 1e-05
head_eps = 1e-06

def layer_norm(stream, gain_row, bias_row):
    row_mean = lax.optimization_barrier(jnp.mean(stream, axis=-1, keepdims=True))
    centred = stream - row_mean
    spread = lax.optimization_barrier(jnp.mean(centred * centred, axis=-1, keepdims=True))
    return centred * lax.rsqrt(spread + norm_eps) * gain_row.astype(jnp.float32) + bias_row.astype(jnp.float32)

def half_ffn(row_block, gate_w, up_w, down_w):
    gate_proj = jnp.dot(row_block, gate_w, preferred_element_type=jnp.float32)
    up_proj = jnp.dot(row_block, up_w, preferred_element_type=jnp.float32)
    hidden = (jax.nn.silu(gate_proj) * up_proj).astype(jnp.bfloat16)
    return jnp.dot(hidden, down_w, preferred_element_type=jnp.float32)

def reference(tokens, gate_weights, up_weights, down_weights, norm_gain, norm_bias, query_weight, forget_weight, input_weight, outgate_weight, lower_bound, head_gain, out_weight, state):
    head_count = D // HEAD
    row_count = tokens.shape[0]
    branch_one = half_ffn(tokens, gate_weights[0], up_weights[0], down_weights[0])
    stream = residual_scale * tokens.astype(jnp.float32) + 0.5 * branch_one
    normed = layer_norm(stream, norm_gain[0], norm_bias[0]).astype(jnp.bfloat16)
    projected = [jnp.dot(normed, weight, preferred_element_type=jnp.float32).astype(jnp.bfloat16) for weight in (query_weight, forget_weight, input_weight, outgate_weight)]
    shaped = [piece_pre.astype(jnp.float32).reshape(row_count, head_count, HEAD) for piece_pre in projected[:3]]
    low_bound = lower_bound.reshape(head_count, HEAD)

    def one_sequence(pieces):
        query_pre, forget_pre, input_pre, old_state = pieces
        forget = low_bound + (1.0 - low_bound) * jax.nn.sigmoid(forget_pre)
        key_part = (1.0 - low_bound) * jax.nn.sigmoid(-forget_pre)
        updated = forget[:, :, None] * old_state + key_part[:, :, None] * input_pre[:, None, :]
        readout = jnp.einsum('hd,hde->he', jax.nn.silu(query_pre), updated, precision=lax.Precision.HIGHEST)
        return (readout, updated)
    readout, new_state = lax.map(one_sequence, (shaped[0], shaped[1], shaped[2], state))
    readout = readout * lax.rsqrt(lax.optimization_barrier(jnp.mean(readout * readout, axis=-1, keepdims=True)) + head_eps)
    gated_out = (readout.reshape(row_count, D) * head_gain * jax.nn.silu(projected[3].astype(jnp.float32))).astype(jnp.bfloat16)
    mixed_out = jnp.dot(gated_out, out_weight, preferred_element_type=jnp.float32)
    stream = (residual_scale * normed.astype(jnp.float32) + mixed_out).astype(jnp.bfloat16)
    normed = layer_norm(stream.astype(jnp.float32), norm_gain[1], norm_bias[1]).astype(jnp.bfloat16)
    branch_two = half_ffn(normed, gate_weights[1], up_weights[1], down_weights[1])
    stream = residual_scale * normed.astype(jnp.float32) + 0.5 * branch_two
    mixed = layer_norm(stream, norm_gain[2], norm_bias[2]).astype(jnp.bfloat16)
    return (mixed, new_state)
```

```python
import jax
import jax.numpy as jnp
from jax import lax
from jax.sharding import Mesh
from jax.sharding import PartitionSpec as P

HEAD = 128
LANES = 128
KV_TP = ("kv_0", "kv_1", "tp_0", "tp_1")
KV = ("kv_0", "kv_1")
TP = ("tp_0", "tp_1")
CHIPS = ("kv_0", "kv_1", "tp_0")
CORE = "tp_1"
SWAP = [(0, 1), (1, 0)]

residual_scale = 8.0**0.25
norm_eps = 1e-05
head_eps = 1e-06
bf16 = jnp.bfloat16
f32 = jnp.float32


def exchange(blocks, axes):
    return lax.all_to_all(blocks, axes, split_axis=0, concat_axis=0, tiled=True)


def to_everyone(block, axes, count):
    return exchange(jnp.broadcast_to(block[None], (count, *block.shape)), axes)


def rows_of(lines, count):
    return jnp.pad(lines, ((0, count - lines.shape[0]), (0, LANES - lines.shape[1])))


def ffn_partial(whole_rows, gate_w, up_w, down_w):
    gate_proj = jnp.dot(whole_rows, gate_w, preferred_element_type=f32)
    up_proj = jnp.dot(whole_rows, up_w, preferred_element_type=f32)
    hidden = (jax.nn.silu(gate_proj) * up_proj).astype(bf16)
    return jnp.dot(hidden, down_w, preferred_element_type=f32)


def local(
    tokens,
    gate_weights,
    up_weights,
    down_weights,
    norm_gain,
    norm_bias,
    query_weight,
    forget_weight,
    input_weight,
    outgate_weight,
    lower_bound,
    head_gain,
    out_weight,
    state,
):
    batch, own_cols = tokens.shape
    seqs, heads = state.shape[:2]
    kv_count, tp_count = lax.axis_size(KV), lax.axis_size(TP)
    x_count = tp_count // 2
    chip_count = kv_count * x_count
    half = batch // 2
    width = own_cols * kv_count * tp_count
    kv, tp, core = lax.axis_index(KV), lax.axis_index(TP), lax.axis_index(CORE)

    turned = tokens.reshape(kv_count, 2, own_cols).swapaxes(0, 1).reshape(batch, own_cols)
    lines = jnp.concatenate([turned, norm_gain, norm_bias, jnp.zeros((2, own_cols), bf16)])
    place = (
        lax.broadcasted_iota(jnp.int32, (own_cols, LANES), 1)
        == lax.broadcasted_iota(jnp.int32, (own_cols, LANES), 0) + tp * own_cols
    ).astype(bf16)
    placed = jnp.dot(lines, place, preferred_element_type=f32).astype(bf16)
    block = lax.all_gather(placed, TP, axis=0).astype(f32).sum(axis=0).astype(bf16)
    own_half = lax.dynamic_slice_in_dim(block, core * half, half, 0)
    arrived = to_everyone(jnp.concatenate([own_half, block[batch:]]), KV, kv_count)
    both = lax.all_gather(arrived, CORE, axis=0)
    whole_tokens = both[:, :, :half].swapaxes(1, 2).reshape(batch, width)
    params = both[0, :, half:].astype(f32)

    def sum_over_kv(partial_value, extra):
        pieces = partial_value.astype(bf16).reshape(2, half, kv_count, LANES).swapaxes(1, 2)
        kept = lax.dynamic_index_in_dim(pieces, core, 0, keepdims=False)
        sent = lax.dynamic_index_in_dim(pieces, 1 - core, 0, keepdims=False)
        paired = (kept.astype(f32) + lax.ppermute(sent, CORE, SWAP).astype(f32)).astype(bf16)
        if extra is not None:
            paired = jnp.concatenate([paired, extra], axis=1)
        return exchange(paired, KV).astype(f32).sum(axis=0)

    def over_tp(lines):
        gathered = lax.all_gather(lines, TP, axis=0)
        return gathered.reshape(x_count, 2, *lines.shape)

    partial_one = ffn_partial(whole_tokens, gate_weights[0], up_weights[0], down_weights[0])
    weights = (query_weight, forget_weight, input_weight, outgate_weight)
    all_weights = jnp.concatenate(weights, axis=1)
    chunk_count = all_weights.shape[1] // LANES
    share = kv_count // chunk_count
    gain_one, bias_one = block[batch : batch + 1], block[batch + 3 : batch + 4]
    bias_part = jnp.dot(bias_one, all_weights, preferred_element_type=f32)
    bias_rows = jnp.repeat(bias_part.reshape(chunk_count, 1, LANES), share, axis=0).astype(bf16)
    row_sum = partial_one.sum(axis=1)
    high = row_sum.astype(bf16)
    low = (row_sum - high.astype(f32)).astype(bf16)
    sum_row = jnp.broadcast_to(jnp.concatenate([high, low])[None, None], (kv_count, 1, LANES))
    extra = jnp.concatenate([sum_row, bias_rows, jnp.zeros((kv_count, 6, LANES), bf16)], axis=1)
    arrived = sum_over_kv(partial_one, extra)
    bias_own = arrived[half + 1 : half + 2] / share
    gathered = over_tp(arrived[: half + 8])
    total = gathered[:, :, :half].sum(axis=0).reshape(batch, LANES)
    total_row = gathered[:, :, half].sum(axis=(0, 1))
    stream_one = residual_scale * block[:batch].astype(f32) + 0.5 * total
    row_mean = (
        residual_scale * whole_tokens.astype(f32).sum(axis=1)
        + 0.5 * (total_row[:batch] + total_row[batch:])
    ) / width
    centred = stream_one - row_mean[:, None]

    scaled = (centred * gain_one.astype(f32)).astype(bf16)
    projected = jnp.dot(scaled, all_weights, preferred_element_type=f32).astype(bf16)
    projected = projected.reshape(2, half, chunk_count, LANES).transpose(1, 2, 0, 3)
    blocks = jnp.concatenate(
        [
            projected.reshape(kv_count, 2 * chunk_count, LANES),
            centred.astype(bf16).reshape(2, half, LANES).swapaxes(0, 1),
            jnp.broadcast_to(bias_own.astype(bf16)[None], (kv_count, 1, LANES)),
            jnp.zeros((kv_count, 5, LANES), bf16),
        ],
        axis=1,
    )
    arrived = exchange(blocks, KV).astype(f32)
    proj_sum = arrived[:, : 2 * chunk_count].sum(axis=0).reshape(chunk_count, 2, LANES)
    own_rows = arrived[:, 2 * chunk_count : 2 * chunk_count + 2]
    bias_sum = arrived[:, 2 * chunk_count + 2].reshape(chunk_count, share, LANES).sum(axis=1)
    own_rows = own_rows - jnp.mean(own_rows, axis=(0, 2), keepdims=True)
    row_scale = lax.rsqrt(jnp.mean(own_rows * own_rows, axis=(0, 2), keepdims=True) + norm_eps)
    pre = (proj_sum * row_scale + bias_sum[:, None]).astype(bf16).astype(f32)
    pre = pre.reshape(4, heads, 2, HEAD).swapaxes(1, 2)
    query_pre, forget_pre, input_pre, outgate_pre = pre[0], pre[1], pre[2], pre[3]

    low_bound = lower_bound.reshape(heads, HEAD)
    forget = low_bound + (1.0 - low_bound) * jax.nn.sigmoid(forget_pre)
    key_part = (1.0 - low_bound) * jax.nn.sigmoid(-forget_pre)
    updated = forget[..., None] * state + key_part[..., None] * input_pre[:, :, None, :]
    readout = jnp.einsum(
        "shd,shde->she", jax.nn.silu(query_pre), updated, precision=lax.Precision.HIGHEST
    )
    readout = readout * lax.rsqrt(jnp.mean(readout * readout, axis=-1, keepdims=True) + head_eps)
    gated_out = (readout * head_gain.reshape(heads, HEAD) * jax.nn.silu(outgate_pre)).astype(bf16)
    mixer_part = jnp.dot(
        gated_out.reshape(seqs, heads * HEAD), out_weight, preferred_element_type=f32
    )
    piece_chunks = kv_count // tp_count
    mixer_part = mixer_part.reshape(2, tp_count, piece_chunks, LANES).transpose(1, 2, 0, 3)
    mixer_sum = exchange(mixer_part, TP).reshape(tp_count, piece_chunks, 2, LANES).sum(axis=0)
    at = tp * piece_chunks
    piece = lax.dynamic_slice_in_dim(own_rows, at, piece_chunks, 0)
    piece_gain = lax.dynamic_slice_in_dim(params[:, 0:1], at, piece_chunks, 0)
    piece_bias = lax.dynamic_slice_in_dim(params[:, 3:4], at, piece_chunks, 0)
    piece = (piece * row_scale * piece_gain + piece_bias).astype(bf16).astype(f32)
    stream_own = (residual_scale * piece + mixer_sum).astype(bf16)
    stream_own = stream_own.reshape(2 * piece_chunks, LANES)
    arrived = lax.all_gather(to_everyone(stream_own, CHIPS, chip_count), CORE, axis=0)
    arrived = arrived.reshape(2, kv_count, x_count, piece_chunks, 2, LANES)
    stream_two = arrived.transpose(4, 1, 2, 0, 3, 5).reshape(batch, width).astype(f32)
    row_mean = jnp.mean(stream_two, axis=-1, keepdims=True)
    centred = stream_two - row_mean
    spread = jnp.mean(centred * centred, axis=-1, keepdims=True)
    normed_two = (
        centred * lax.rsqrt(spread + norm_eps) * params[:, 1].reshape(1, width)
        + params[:, 4].reshape(1, width)
    ).astype(bf16)

    partial_two = ffn_partial(normed_two, gate_weights[1], up_weights[1], down_weights[1])
    total = over_tp(sum_over_kv(partial_two, None)).sum(axis=0).reshape(batch, LANES)
    own_normed = lax.dynamic_slice_in_dim(normed_two, kv * LANES, LANES, 1)
    stream_three = residual_scale * own_normed.astype(f32) + 0.5 * total
    block_sum = stream_three.sum(axis=1)
    block_mean = block_sum / LANES
    off = stream_three - block_mean[:, None]
    stats = jnp.concatenate([block_mean, (off * off).sum(axis=1)])[None]
    stats = to_everyone(stats, KV, kv_count)[:, 0]
    means, squares = stats[:, :batch], stats[:, batch:]
    row_mean = means.mean(axis=0)
    spread = (squares.sum(axis=0) + LANES * ((means - row_mean) ** 2).sum(axis=0)) / width
    own = lax.dynamic_slice_in_dim(stream_three, tp * own_cols, own_cols, 1)
    mixed = (own - row_mean[:, None]) * lax.rsqrt(spread + norm_eps)[:, None] * norm_gain[
        2
    ].astype(f32) + norm_bias[2].astype(f32)
    mixed = mixed.reshape(2, half, own_cols).swapaxes(0, 1).reshape(batch, own_cols)
    return (mixed.astype(bf16), updated)


def solution(mesh):
    finer = Mesh(mesh.devices.reshape(8, 4, 4, 2), KV_TP)
    in_specs = (
        P(None, KV_TP),
        P(None, None, KV_TP),
        P(None, None, KV_TP),
        P(None, KV_TP, None),
        P(None, KV_TP),
        P(None, KV_TP),
        P(KV, TP),
        P(KV, TP),
        P(KV, TP),
        P(KV, TP),
        P(TP),
        P(TP),
        P(TP, None),
        P(KV, TP, None, None),
    )
    out_specs = (P(None, KV_TP), P(KV, TP, None, None))
    return jax.shard_map(local, mesh=finer, in_specs=in_specs, out_specs=out_specs, check_vma=False)
```

```python
import jax
import jax.numpy as jnp
from jax import lax
from jax.experimental import pallas as pl
from jax.sharding import Mesh
from jax.sharding import PartitionSpec as P

HEAD = 128
LANES = 128
KV_TP = ("kv_0", "kv_1", "tp_0", "tp_1")
KV = ("kv_0", "kv_1")
TP = ("tp_0", "tp_1")
CHIPS = ("kv_0", "kv_1", "tp_0")
CORE = "tp_1"
SWAP = [(0, 1), (1, 0)]

residual_scale = 8.0**0.25
norm_eps = 1e-05
head_eps = 1e-06
bf16 = jnp.bfloat16
f32 = jnp.float32


def exchange(blocks, axes):
    return lax.all_to_all(blocks, axes, split_axis=0, concat_axis=0, tiled=True)


def to_everyone(block, axes, count):
    return exchange(jnp.broadcast_to(block[None], (count, *block.shape)), axes)


def rows_of(lines, count):
    return jnp.pad(lines, ((0, count - lines.shape[0]), (0, LANES - lines.shape[1])))


def ffn_partial(whole_rows, gate_ws, up_ws, down_ws, layer):
    gate_proj = jnp.einsum("sf,lfh->shl", whole_rows, gate_ws, preferred_element_type=f32)
    up_proj = jnp.einsum("sf,lfh->shl", whole_rows, up_ws, preferred_element_type=f32)
    hidden = (jax.nn.silu(gate_proj) * up_proj).astype(bf16)
    other = lax.broadcasted_iota(jnp.int32, hidden.shape, 2) != layer
    hidden = jnp.where(other, 0, hidden)
    return jnp.einsum("shl,lhf->sf", hidden, down_ws, preferred_element_type=f32)


def out_kernel(gated_ref, weight_ref, result_ref):
    result_ref[...] = jnp.dot(gated_ref[...], weight_ref[...], preferred_element_type=f32)


def out_projection(gated, weight):
    rows, depth = gated.shape
    width = weight.shape[1]
    step = 1024
    return pl.pallas_call(
        out_kernel,
        grid=(width // step,),
        in_specs=[
            pl.BlockSpec((rows, depth), lambda i: (0, 0)),
            pl.BlockSpec((depth, step), lambda i: (0, i)),
        ],
        out_specs=pl.BlockSpec((rows, step), lambda i: (0, i)),
        out_shape=jax.ShapeDtypeStruct((rows, width), f32),
    )(gated, weight)


def local(
    tokens,
    gate_weights,
    up_weights,
    down_weights,
    norm_gain,
    norm_bias,
    query_weight,
    forget_weight,
    input_weight,
    outgate_weight,
    lower_bound,
    head_gain,
    out_weight,
    state,
):
    batch, own_cols = tokens.shape
    seqs, heads = state.shape[:2]
    kv_count, tp_count = lax.axis_size(KV), lax.axis_size(TP)
    x_count = tp_count // 2
    chip_count = kv_count * x_count
    half = batch // 2
    width = own_cols * kv_count * tp_count
    kv, tp, core = lax.axis_index(KV), lax.axis_index(TP), lax.axis_index(CORE)

    turned = tokens.reshape(kv_count, 2, own_cols).swapaxes(0, 1).reshape(batch, own_cols)
    lines = jnp.concatenate([turned, norm_gain, norm_bias, jnp.zeros((2, own_cols), bf16)])
    place = (
        lax.broadcasted_iota(jnp.int32, (own_cols, LANES), 1)
        == lax.broadcasted_iota(jnp.int32, (own_cols, LANES), 0) + tp * own_cols
    ).astype(bf16)
    placed = jnp.dot(lines, place, preferred_element_type=f32).astype(bf16)
    block = to_everyone(placed, TP, tp_count).astype(f32).sum(axis=0).astype(bf16)
    own_half = lax.dynamic_slice_in_dim(block, core * half, half, 0)
    arrived = to_everyone(jnp.concatenate([own_half, block[batch:]]), KV, kv_count)
    both = lax.all_gather(arrived, CORE, axis=0)
    whole_tokens = both[:, :, :half].swapaxes(1, 2).reshape(batch, width)
    params = both[0, :, half:].astype(f32)

    def sum_over_kv(partial_value, extra):
        pieces = partial_value.astype(bf16).reshape(2, half, kv_count, LANES).swapaxes(1, 2)
        kept = lax.dynamic_index_in_dim(pieces, core, 0, keepdims=False)
        sent = lax.dynamic_index_in_dim(pieces, 1 - core, 0, keepdims=False)
        paired = (kept.astype(f32) + lax.ppermute(sent, CORE, SWAP).astype(f32)).astype(bf16)
        if extra is not None:
            paired = jnp.concatenate([paired, extra], axis=1)
        return exchange(paired, KV).astype(f32).sum(axis=0)

    def over_tp(lines):
        gathered = to_everyone(lines, TP, tp_count)
        return gathered.reshape(x_count, 2, *lines.shape)

    partial_one = ffn_partial(whole_tokens, gate_weights, up_weights, down_weights, 0)
    weights = (query_weight, forget_weight, input_weight, outgate_weight)
    chunk_count = 4 * heads

    def project(lines):
        return jnp.concatenate(
            [jnp.dot(lines, w, preferred_element_type=f32) for w in weights], axis=1
        )

    share = kv_count // chunk_count
    gain_one, bias_one = block[batch : batch + 1], block[batch + 3 : batch + 4]
    bias_part = project(bias_one)
    bias_rows = jnp.repeat(bias_part.reshape(chunk_count, 1, LANES), share, axis=0).astype(bf16)
    row_sum = partial_one.sum(axis=1)
    high = row_sum.astype(bf16)
    low = (row_sum - high.astype(f32)).astype(bf16)
    sum_row = jnp.broadcast_to(jnp.concatenate([high, low])[None, None], (kv_count, 1, LANES))
    extra = jnp.concatenate([sum_row, bias_rows, jnp.zeros((kv_count, 6, LANES), bf16)], axis=1)
    arrived = sum_over_kv(partial_one, extra)
    bias_own = arrived[half + 1 : half + 2] / share
    gathered = over_tp(arrived[: half + 8])
    total = gathered[:, :, :half].sum(axis=0).reshape(batch, LANES)
    total_row = gathered[:, :, half].sum(axis=(0, 1))
    stream_one = residual_scale * block[:batch].astype(f32) + 0.5 * total
    row_mean = (
        residual_scale * whole_tokens.astype(f32).sum(axis=1)
        + 0.5 * (total_row[:batch] + total_row[batch:])
    ) / width
    centred = stream_one - row_mean[:, None]

    scaled = (centred * gain_one.astype(f32)).astype(bf16)
    projected = project(scaled).astype(bf16)
    projected = projected.reshape(2, half, chunk_count, LANES).transpose(1, 2, 0, 3)
    blocks = jnp.concatenate(
        [
            projected.reshape(kv_count, 2 * chunk_count, LANES),
            centred.astype(bf16).reshape(2, half, LANES).swapaxes(0, 1),
            jnp.broadcast_to(bias_own.astype(bf16)[None], (kv_count, 1, LANES)),
            jnp.zeros((kv_count, 5, LANES), bf16),
        ],
        axis=1,
    )
    arrived = exchange(blocks, KV).astype(f32)
    proj_sum = arrived[:, : 2 * chunk_count].sum(axis=0).reshape(chunk_count, 2, LANES)
    own_rows = arrived[:, 2 * chunk_count : 2 * chunk_count + 2]
    bias_sum = arrived[:, 2 * chunk_count + 2].reshape(chunk_count, share, LANES).sum(axis=1)
    own_rows = own_rows - jnp.mean(own_rows, axis=(0, 2), keepdims=True)
    row_scale = lax.rsqrt(jnp.mean(own_rows * own_rows, axis=(0, 2), keepdims=True) + norm_eps)
    pre = (proj_sum * row_scale + bias_sum[:, None]).astype(bf16).astype(f32)
    pre = pre.reshape(4, heads, 2, HEAD).swapaxes(1, 2)
    query_pre, forget_pre, input_pre, outgate_pre = pre[0], pre[1], pre[2], pre[3]

    low_bound = lower_bound.reshape(heads, HEAD)
    forget = low_bound + (1.0 - low_bound) * jax.nn.sigmoid(forget_pre)
    key_part = (1.0 - low_bound) * jax.nn.sigmoid(-forget_pre)
    updated = forget[..., None] * state + key_part[..., None] * input_pre[:, :, None, :]
    readout = jnp.einsum(
        "shd,shde->she", jax.nn.silu(query_pre), updated, precision=lax.Precision.HIGHEST
    )
    readout = readout * lax.rsqrt(jnp.mean(readout * readout, axis=-1, keepdims=True) + head_eps)
    gated_out = (readout * head_gain.reshape(heads, HEAD) * jax.nn.silu(outgate_pre)).astype(bf16)
    gated_rows = jnp.pad(gated_out.reshape(seqs, heads * HEAD), ((0, 8 - seqs), (0, 0)))
    mixer_part = out_projection(gated_rows, out_weight)[:seqs]
    piece_chunks = kv_count // tp_count
    mixer_part = mixer_part.reshape(2, tp_count, piece_chunks, LANES).transpose(1, 2, 0, 3)
    mixer_sum = exchange(mixer_part, TP).reshape(tp_count, piece_chunks, 2, LANES).sum(axis=0)
    at = tp * piece_chunks
    piece = lax.dynamic_slice_in_dim(own_rows, at, piece_chunks, 0)
    piece_gain = lax.dynamic_slice_in_dim(params[:, 0:1], at, piece_chunks, 0)
    piece_bias = lax.dynamic_slice_in_dim(params[:, 3:4], at, piece_chunks, 0)
    piece = (piece * row_scale * piece_gain + piece_bias).astype(bf16).astype(f32)
    stream_own = (residual_scale * piece + mixer_sum).astype(bf16)
    stream_own = stream_own.reshape(2 * piece_chunks, LANES)
    arrived = lax.all_gather(to_everyone(stream_own, CHIPS, chip_count), CORE, axis=0)
    arrived = arrived.reshape(2, kv_count, x_count, piece_chunks, 2, LANES)
    stream_two = arrived.transpose(4, 1, 2, 0, 3, 5).reshape(batch, width).astype(f32)
    row_mean = jnp.mean(stream_two, axis=-1, keepdims=True)
    centred = stream_two - row_mean
    spread = jnp.mean(centred * centred, axis=-1, keepdims=True)
    normed_two = (
        centred * lax.rsqrt(spread + norm_eps) * params[:, 1].reshape(1, width)
        + params[:, 4].reshape(1, width)
    ).astype(bf16)

    partial_two = ffn_partial(normed_two, gate_weights, up_weights, down_weights, 1)
    total = over_tp(sum_over_kv(partial_two, None)).sum(axis=0).reshape(batch, LANES)
    own_normed = lax.dynamic_slice_in_dim(normed_two, kv * LANES, LANES, 1)
    stream_three = residual_scale * own_normed.astype(f32) + 0.5 * total
    block_sum = stream_three.sum(axis=1)
    block_mean = block_sum / LANES
    off = stream_three - block_mean[:, None]
    stats = jnp.concatenate([block_mean, (off * off).sum(axis=1)])[None]
    stats = to_everyone(stats, KV, kv_count)[:, 0]
    means, squares = stats[:, :batch], stats[:, batch:]
    row_mean = means.mean(axis=0)
    spread = (squares.sum(axis=0) + LANES * ((means - row_mean) ** 2).sum(axis=0)) / width
    own = lax.dynamic_slice_in_dim(stream_three, tp * own_cols, own_cols, 1)
    mixed = (own - row_mean[:, None]) * lax.rsqrt(spread + norm_eps)[:, None] * norm_gain[
        2
    ].astype(f32) + norm_bias[2].astype(f32)
    mixed = mixed.reshape(2, half, own_cols).swapaxes(0, 1).reshape(batch, own_cols)
    return (mixed.astype(bf16), updated)


def solution(mesh):
    finer = Mesh(mesh.devices.reshape(8, 4, 4, 2), KV_TP)
    in_specs = (
        P(None, KV_TP),
        P(None, None, KV_TP),
        P(None, None, KV_TP),
        P(None, KV_TP, None),
        P(None, KV_TP),
        P(None, KV_TP),
        P(KV, TP),
        P(KV, TP),
        P(KV, TP),
        P(KV, TP),
        P(TP),
        P(TP),
        P(TP, None),
        P(KV, TP, None, None),
    )
    out_specs = (P(None, KV_TP), P(KV, TP, None, None))
    return jax.shard_map(local, mesh=finer, in_specs=in_specs, out_specs=out_specs, check_vma=False)
```

```python
import jax
import jax.numpy as jnp
from jax import lax
from jax.experimental import pallas as pl
from jax.experimental.pallas import tpu as pltpu
from jax.sharding import Mesh
from jax.sharding import PartitionSpec as P

HEAD = 128
LANES = 128
KV_TP = ("kv_0", "kv_1", "tp_0", "tp_1")
KV = ("kv_0", "kv_1")
TP = ("tp_0", "tp_1")
CHIPS = ("kv_0", "kv_1", "tp_0")
CORE = "tp_1"
SWAP = [(0, 1), (1, 0)]

residual_scale = 8.0**0.25
norm_eps = 1e-05
head_eps = 1e-06
bf16 = jnp.bfloat16
f32 = jnp.float32


def exchange(blocks, axes):
    return lax.all_to_all(blocks, axes, split_axis=0, concat_axis=0, tiled=True)


def to_everyone(block, axes, count):
    return exchange(jnp.broadcast_to(block[None], (count, *block.shape)), axes)


def rows_of(lines, count):
    return jnp.pad(lines, ((0, count - lines.shape[0]), (0, LANES - lines.shape[1])))


def ffn_partial(whole_rows, gate_ws, up_ws, down_ws, layer):
    gate_proj = jnp.einsum("sf,lfh->shl", whole_rows, gate_ws, preferred_element_type=f32)
    up_proj = jnp.einsum("sf,lfh->shl", whole_rows, up_ws, preferred_element_type=f32)
    hidden = (jax.nn.silu(gate_proj) * up_proj).astype(bf16)
    other = lax.broadcasted_iota(jnp.int32, hidden.shape, 2) != layer
    hidden = jnp.where(other, 0, hidden)
    return jnp.einsum("shl,lhf->sf", hidden, down_ws, preferred_element_type=f32)


def norm_kernel(arrived_ref, params_ref, result_ref, raw_ref):
    cores, kv_count, x_count, rows, _ = arrived_ref.shape
    pieces = rows // 2
    chunks = cores * x_count * pieces
    for x in range(x_count):
        for core in range(cores):
            tiles = arrived_ref[core, :, x].astype(f32)
            raw_ref[x * cores + core] = tiles.reshape(kv_count * rows, LANES)

    def lines(chunk, seq):
        at = (chunk % pieces) * 2 + seq
        return raw_ref[chunk // pieces, pl.ds(at, kv_count, stride=rows), :]

    width = chunks * LANES
    for seq in range(2):
        total = sum(lines(chunk, seq) for chunk in range(chunks))
        mean = jnp.sum(total, axis=1, keepdims=True) / width
        squares = jnp.zeros((kv_count, LANES), f32)
        for chunk in range(chunks):
            off = lines(chunk, seq) - mean
            squares = squares + off * off
        spread = jnp.sum(squares, axis=1, keepdims=True) / width
        scale = lax.rsqrt(spread + norm_eps)
        for chunk in range(chunks):
            params = params_ref[chunk].astype(f32)
            normed = (lines(chunk, seq) - mean) * scale * params[1:2] + params[4:5]
            result_ref[
                seq * kv_count : (seq + 1) * kv_count, chunk * LANES : (chunk + 1) * LANES
            ] = normed.astype(bf16)


def norm_of_tiles(arrived, params):
    cores, kv_count, x_count, rows, lanes = arrived.shape
    return pl.pallas_call(
        norm_kernel,
        out_shape=jax.ShapeDtypeStruct((2 * kv_count, cores * x_count * rows // 2 * lanes), bf16),
        scratch_shapes=[pltpu.VMEM((cores * x_count, kv_count * rows, lanes), f32)],
        name="norm_two",
    )(arrived, params)


def mixer_kernel(
    tp_ref,
    arrived_ref,
    params_ref,
    low_ref,
    head_gain_ref,
    state_hbm,
    weight_hbm,
    sent_ref,
    piece_ref,
    updated_hbm,
    state_ref,
    weight_ref,
    rows_ref,
    low_rows_ref,
    gain_rows_ref,
    readout_ref,
    gated_ref,
    state_sem,
    weight_sem,
    updated_sem,
):
    seqs, heads = state_ref.shape[:2]
    kv_count = arrived_ref.shape[0]
    chunks = 4 * heads
    share = kv_count // chunks
    parts = weight_ref.shape[0]
    piece_chunks = kv_count // parts

    state_copy = pltpu.make_async_copy(state_hbm, state_ref, state_sem)
    state_copy.start()
    step = weight_ref.shape[2]
    weight_copies = [
        pltpu.make_async_copy(
            weight_hbm.at[:, pl.ds(part * step, step)], weight_ref.at[part], weight_sem.at[part]
        )
        for part in range(parts)
    ]
    for copy in weight_copies:
        copy.start()

    total = arrived_ref[0].astype(f32)
    for block in range(1, kv_count):
        total = total + arrived_ref[block].astype(f32)
    tail = seqs * chunks
    width = kv_count * LANES
    mean = jnp.sum(total[tail : tail + 8], axis=1, keepdims=True) / width
    squares = jnp.zeros((8, LANES), f32)
    for block in range(kv_count):
        off = arrived_ref[block, tail : tail + 8, :].astype(f32) - mean
        squares = squares + off * off
    scale = lax.rsqrt(jnp.sum(squares, axis=1, keepdims=True) / width + norm_eps)
    for chunk in range(chunks):
        bias = arrived_ref[chunk * share, tail : tail + 8, :].astype(f32)
        for other in range(1, share):
            bias = bias + arrived_ref[chunk * share + other, tail : tail + 8, :].astype(f32)
        rows_ref[2 * chunk : 2 * chunk + 2, :] = jnp.broadcast_to(bias[2:3], (2, LANES))
    odd = lax.broadcasted_iota(jnp.int32, (tail, LANES), 0) % 2 == 1
    row_scale = jnp.where(odd, scale[1:2], scale[0:1])
    pre = (total[:tail] * row_scale + rows_ref[...]).astype(bf16).astype(f32)
    size = 2 * heads
    query_pre, forget_pre = pre[:size], pre[size : 2 * size]
    input_pre, outgate_pre = pre[2 * size : 3 * size], pre[3 * size :]

    tp = tp_ref[0]
    for chunk in range(piece_chunks):
        at = tp * piece_chunks + chunk
        rows = arrived_ref[at, tail : tail + 8, :].astype(f32)
        params = params_ref[at].astype(f32)
        rows = ((rows - mean) * scale * params[0:1] + params[3:4]).astype(bf16).astype(f32)
        piece_ref[2 * chunk : 2 * chunk + 2, :] = residual_scale * rows[0:2]

    for head in range(heads):
        at = slice(2 * head, 2 * head + 2)
        low_rows_ref[at, :] = jnp.broadcast_to(low_ref[head : head + 1, :], (2, LANES))
        gain_rows_ref[at, :] = jnp.broadcast_to(head_gain_ref[head : head + 1, :], (2, LANES))
    low = low_rows_ref[...]
    forget = (low + (1.0 - low) * jax.nn.sigmoid(forget_pre)).T
    key = ((1.0 - low) * jax.nn.sigmoid(-forget_pre)).T
    query = jax.nn.silu(query_pre).T
    state_copy.wait()
    updated_copies = []
    for head in range(heads):
        for seq in range(seqs):
            row = head * 2 + seq
            new = (
                forget[:, row : row + 1] * state_ref[seq, head]
                + key[:, row : row + 1] * input_pre[row : row + 1, :]
            )
            state_ref[seq, head] = new
            updated_copies.append(
                pltpu.make_async_copy(
                    state_ref.at[seq, head], updated_hbm.at[seq, head], updated_sem.at[row]
                )
            )
            updated_copies[-1].start()
            readout_ref[row : row + 1, :] = jnp.sum(
                query[:, row : row + 1] * new, axis=0, keepdims=True
            )
    readout = readout_ref[...]
    readout = readout * lax.rsqrt(jnp.mean(readout * readout, axis=1, keepdims=True) + head_eps)
    gated = readout * gain_rows_ref[...] * jax.nn.silu(outgate_pre)
    gated_ref[...] = jnp.zeros(gated_ref.shape, f32)
    for head in range(heads):
        gated_ref[0:2, head * HEAD : (head + 1) * HEAD] = gated[2 * head : 2 * head + 2]
    lhs = gated_ref[...].astype(bf16)
    for part in range(parts):
        weight_copies[part].wait()
        mixed = jnp.dot(lhs, weight_ref[part], preferred_element_type=f32)
        for chunk in range(piece_chunks):
            sent_ref[part, 2 * chunk : 2 * chunk + 2, :] = mixed[
                0:2, chunk * LANES : (chunk + 1) * LANES
            ]
    for copy in updated_copies:
        copy.wait()


def mixer(tp, arrived, params, lower_bound, head_gain, state, weight, parts):
    seqs, heads = state.shape[:2]
    depth, width = weight.shape
    rows = 2 * width // parts // LANES
    vmem, anywhere = pl.BlockSpec(memory_space=pltpu.VMEM), pl.BlockSpec(memory_space=pl.ANY)
    return pl.pallas_call(
        mixer_kernel,
        in_specs=[pl.BlockSpec(memory_space=pltpu.SMEM)] + [vmem] * 4 + [anywhere] * 2,
        out_specs=[vmem, vmem, anywhere],
        out_shape=[
            jax.ShapeDtypeStruct((parts, rows, LANES), f32),
            jax.ShapeDtypeStruct((rows, LANES), f32),
            jax.ShapeDtypeStruct(state.shape, f32),
        ],
        scratch_shapes=[
            pltpu.VMEM(state.shape, f32),
            pltpu.VMEM((parts, depth, width // parts), bf16),
            pltpu.VMEM((seqs * 4 * heads, LANES), f32),
            pltpu.VMEM((2 * heads, LANES), f32),
            pltpu.VMEM((2 * heads, LANES), f32),
            pltpu.VMEM((2 * heads, LANES), f32),
            pltpu.VMEM((8, heads * HEAD), f32),
            pltpu.SemaphoreType.DMA,
            pltpu.SemaphoreType.DMA((parts,)),
            pltpu.SemaphoreType.DMA((seqs * heads,)),
        ],
        name="mixer",
    )(tp.reshape(1), arrived, params, lower_bound, head_gain, state, weight)


def local(
    tokens,
    gate_weights,
    up_weights,
    down_weights,
    norm_gain,
    norm_bias,
    query_weight,
    forget_weight,
    input_weight,
    outgate_weight,
    lower_bound,
    head_gain,
    out_weight,
    state,
):
    batch, own_cols = tokens.shape
    heads = state.shape[1]
    kv_count, tp_count = lax.axis_size(KV), lax.axis_size(TP)
    x_count = tp_count // 2
    chip_count = kv_count * x_count
    half = batch // 2
    width = own_cols * kv_count * tp_count
    kv, tp, core = lax.axis_index(KV), lax.axis_index(TP), lax.axis_index(CORE)

    turned = tokens.reshape(kv_count, 2, own_cols).swapaxes(0, 1).reshape(batch, own_cols)
    lines = jnp.concatenate([turned, norm_gain, norm_bias, jnp.zeros((2, own_cols), bf16)])
    place = (
        lax.broadcasted_iota(jnp.int32, (own_cols, LANES), 1)
        == lax.broadcasted_iota(jnp.int32, (own_cols, LANES), 0) + tp * own_cols
    ).astype(bf16)
    placed = jnp.dot(lines, place, preferred_element_type=f32).astype(bf16)
    block = to_everyone(placed, TP, tp_count).astype(f32).sum(axis=0).astype(bf16)
    own_half = lax.dynamic_slice_in_dim(block, core * half, half, 0)
    arrived = to_everyone(jnp.concatenate([own_half, block[batch:]]), KV, kv_count)
    both = lax.all_gather(arrived, CORE, axis=0)
    whole_tokens = both[:, :, :half].swapaxes(1, 2).reshape(batch, width)
    params = both[0, :, half:]

    def sum_over_kv(partial_value, extra):
        pieces = partial_value.astype(bf16).reshape(2, half, kv_count, LANES).swapaxes(1, 2)
        kept = lax.dynamic_index_in_dim(pieces, core, 0, keepdims=False)
        sent = lax.dynamic_index_in_dim(pieces, 1 - core, 0, keepdims=False)
        paired = (kept.astype(f32) + lax.ppermute(sent, CORE, SWAP).astype(f32)).astype(bf16)
        if extra is not None:
            paired = jnp.concatenate([paired, extra], axis=1)
        return exchange(paired, KV).astype(f32).sum(axis=0)

    def over_tp(lines):
        gathered = to_everyone(lines, TP, tp_count)
        return gathered.reshape(x_count, 2, *lines.shape)

    partial_one = ffn_partial(whole_tokens, gate_weights, up_weights, down_weights, 0)
    weights = (query_weight, forget_weight, input_weight, outgate_weight)
    chunk_count = 4 * heads

    def project(lines):
        return jnp.concatenate(
            [jnp.dot(lines, w, preferred_element_type=f32) for w in weights], axis=1
        )

    share = kv_count // chunk_count
    gain_one, bias_one = block[batch : batch + 1], block[batch + 3 : batch + 4]
    bias_part = project(bias_one)
    bias_rows = jnp.repeat(bias_part.reshape(chunk_count, 1, LANES), share, axis=0).astype(bf16)
    row_sum = partial_one.sum(axis=1)
    high = row_sum.astype(bf16)
    low = (row_sum - high.astype(f32)).astype(bf16)
    sum_row = jnp.broadcast_to(jnp.concatenate([high, low])[None, None], (kv_count, 1, LANES))
    extra = jnp.concatenate([sum_row, bias_rows, jnp.zeros((kv_count, 6, LANES), bf16)], axis=1)
    arrived = sum_over_kv(partial_one, extra)
    bias_own = arrived[half + 1 : half + 2] / share
    gathered = over_tp(arrived[: half + 8])
    total = gathered[:, :, :half].sum(axis=0).reshape(batch, LANES)
    total_row = gathered[:, :, half].sum(axis=(0, 1))
    stream_one = residual_scale * block[:batch].astype(f32) + 0.5 * total
    row_mean = (
        residual_scale * whole_tokens.astype(f32).sum(axis=1)
        + 0.5 * (total_row[:batch] + total_row[batch:])
    ) / width
    centred = stream_one - row_mean[:, None]

    scaled = (centred * gain_one.astype(f32)).astype(bf16)
    projected = project(scaled).astype(bf16)
    projected = projected.reshape(2, half, chunk_count, LANES).transpose(1, 2, 0, 3)
    blocks = jnp.concatenate(
        [
            projected.reshape(kv_count, 2 * chunk_count, LANES),
            centred.astype(bf16).reshape(2, half, LANES).swapaxes(0, 1),
            jnp.broadcast_to(bias_own.astype(bf16)[None], (kv_count, 1, LANES)),
            jnp.zeros((kv_count, 5, LANES), bf16),
        ],
        axis=1,
    )
    arrived = exchange(blocks, KV)
    mixer_part, piece, updated = mixer(
        tp,
        arrived,
        params,
        lower_bound.reshape(heads, HEAD),
        head_gain.reshape(heads, HEAD),
        state,
        out_weight,
        tp_count,
    )
    mixer_sum = exchange(mixer_part, TP).sum(axis=0)
    stream_own = (piece + mixer_sum).astype(bf16)
    arrived = lax.all_gather(to_everyone(stream_own, CHIPS, chip_count), CORE, axis=0)
    arrived = arrived.reshape(2, kv_count, x_count, *stream_own.shape)
    normed_two = norm_of_tiles(arrived, params)

    partial_two = ffn_partial(normed_two, gate_weights, up_weights, down_weights, 1)
    total = over_tp(sum_over_kv(partial_two, None)).sum(axis=0).reshape(batch, LANES)
    own_normed = lax.dynamic_slice_in_dim(normed_two, kv * LANES, LANES, 1)
    stream_three = residual_scale * own_normed.astype(f32) + 0.5 * total
    block_sum = stream_three.sum(axis=1)
    block_mean = block_sum / LANES
    off = stream_three - block_mean[:, None]
    stats = jnp.concatenate([block_mean, (off * off).sum(axis=1)])[None]
    stats = to_everyone(stats, KV, kv_count)[:, 0]
    means, squares = stats[:, :batch], stats[:, batch:]
    row_mean = means.mean(axis=0)
    spread = (squares.sum(axis=0) + LANES * ((means - row_mean) ** 2).sum(axis=0)) / width
    own = lax.dynamic_slice_in_dim(stream_three, tp * own_cols, own_cols, 1)
    mixed = (own - row_mean[:, None]) * lax.rsqrt(spread + norm_eps)[:, None] * norm_gain[
        2
    ].astype(f32) + norm_bias[2].astype(f32)
    mixed = mixed.reshape(2, half, own_cols).swapaxes(0, 1).reshape(batch, own_cols)
    return (mixed.astype(bf16), updated)


def solution(mesh):
    finer = Mesh(mesh.devices.reshape(8, 4, 4, 2), KV_TP)
    in_specs = (
        P(None, KV_TP),
        P(None, None, KV_TP),
        P(None, None, KV_TP),
        P(None, KV_TP, None),
        P(None, KV_TP),
        P(None, KV_TP),
        P(KV, TP),
        P(KV, TP),
        P(KV, TP),
        P(KV, TP),
        P(TP),
        P(TP),
        P(TP, None),
        P(KV, TP, None, None),
    )
    out_specs = (P(None, KV_TP), P(KV, TP, None, None))
    return jax.shard_map(local, mesh=finer, in_specs=in_specs, out_specs=out_specs, check_vma=False)
```

```python
import jax
import jax.numpy as jnp
from jax import lax
from jax.experimental import pallas as pl
from jax.experimental.pallas import tpu as pltpu
from jax.sharding import Mesh
from jax.sharding import PartitionSpec as P

HEAD = 128
LANES = 128
KV_TP = ("kv_0", "kv_1", "tp_0", "tp_1")
KV = ("kv_0", "kv_1")
TP = ("tp_0", "tp_1")
CHIPS = ("kv_0", "kv_1", "tp_0")
CORE = "tp_1"
SWAP = [(0, 1), (1, 0)]

residual_scale = 8.0**0.25
norm_eps = 1e-05
head_eps = 1e-06
bf16 = jnp.bfloat16
f32 = jnp.float32


def exchange(blocks, axes):
    return lax.all_to_all(blocks, axes, split_axis=0, concat_axis=0, tiled=True)


def to_everyone(block, axes, count):
    return exchange(jnp.broadcast_to(block[None], (count, *block.shape)), axes)


def rows_of(lines, count):
    return jnp.pad(lines, ((0, count - lines.shape[0]), (0, LANES - lines.shape[1])))


def ffn_partial(whole_rows, gate_ws, up_ws, down_ws, layer):
    gate_proj = jnp.einsum("sf,lfh->shl", whole_rows, gate_ws, preferred_element_type=f32)
    up_proj = jnp.einsum("sf,lfh->shl", whole_rows, up_ws, preferred_element_type=f32)
    hidden = (jax.nn.silu(gate_proj) * up_proj).astype(bf16)
    other = lax.broadcasted_iota(jnp.int32, hidden.shape, 2) != layer
    hidden = jnp.where(other, 0, hidden)
    return jnp.einsum("shl,lhf->sf", hidden, down_ws, preferred_element_type=f32)


def norm_kernel(arrived_ref, params_ref, result_ref, raw_ref):
    cores, kv_count, x_count, rows, _ = arrived_ref.shape
    pieces = rows // 2
    chunks = cores * x_count * pieces
    for x in range(x_count):
        for core in range(cores):
            tiles = arrived_ref[core, :, x].astype(f32)
            raw_ref[x * cores + core] = tiles.reshape(kv_count * rows, LANES)

    def lines(chunk, seq):
        at = (chunk % pieces) * 2 + seq
        return raw_ref[chunk // pieces, pl.ds(at, kv_count, stride=rows), :]

    width = chunks * LANES
    for seq in range(2):
        total = sum(lines(chunk, seq) for chunk in range(chunks))
        mean = jnp.sum(total, axis=1, keepdims=True) / width
        squares = jnp.zeros((kv_count, LANES), f32)
        for chunk in range(chunks):
            off = lines(chunk, seq) - mean
            squares = squares + off * off
        spread = jnp.sum(squares, axis=1, keepdims=True) / width
        scale = lax.rsqrt(spread + norm_eps)
        for chunk in range(chunks):
            params = params_ref[chunk].astype(f32)
            normed = (lines(chunk, seq) - mean) * scale * params[1:2] + params[4:5]
            result_ref[
                seq * kv_count : (seq + 1) * kv_count, chunk * LANES : (chunk + 1) * LANES
            ] = normed.astype(bf16)


def norm_of_tiles(arrived, params):
    cores, kv_count, x_count, rows, lanes = arrived.shape
    return pl.pallas_call(
        norm_kernel,
        out_shape=jax.ShapeDtypeStruct((2 * kv_count, cores * x_count * rows // 2 * lanes), bf16),
        scratch_shapes=[pltpu.VMEM((cores * x_count, kv_count * rows, lanes), f32)],
        compiler_params=pltpu.CompilerParams(vmem_limit_bytes=8 * 2**20),
        name="norm_two",
    )(arrived, params)


def mixer_kernel(
    tp_ref,
    arrived_ref,
    params_ref,
    low_ref,
    head_gain_ref,
    state_ref,
    weight_ref,
    sent_ref,
    piece_ref,
    updated_hbm,
    updated_ref,
    rows_ref,
    low_rows_ref,
    gain_rows_ref,
    readout_ref,
    gated_ref,
    updated_sem,
):
    seqs, heads = state_ref.shape[:2]
    kv_count = arrived_ref.shape[0]
    chunks = 4 * heads
    share = kv_count // chunks
    parts = sent_ref.shape[0]
    piece_chunks = kv_count // parts
    step = weight_ref.shape[1] // parts

    total = arrived_ref[0].astype(f32)
    for block in range(1, kv_count):
        total = total + arrived_ref[block].astype(f32)
    tail = seqs * chunks
    width = kv_count * LANES
    mean = jnp.sum(total[tail : tail + 8], axis=1, keepdims=True) / width
    squares = jnp.zeros((8, LANES), f32)
    for block in range(kv_count):
        off = arrived_ref[block, tail : tail + 8, :].astype(f32) - mean
        squares = squares + off * off
    scale = lax.rsqrt(jnp.sum(squares, axis=1, keepdims=True) / width + norm_eps)
    for chunk in range(chunks):
        bias = arrived_ref[chunk * share, tail : tail + 8, :].astype(f32)
        for other in range(1, share):
            bias = bias + arrived_ref[chunk * share + other, tail : tail + 8, :].astype(f32)
        rows_ref[2 * chunk : 2 * chunk + 2, :] = jnp.broadcast_to(bias[2:3], (2, LANES))
    odd = lax.broadcasted_iota(jnp.int32, (tail, LANES), 0) % 2 == 1
    row_scale = jnp.where(odd, scale[1:2], scale[0:1])
    pre = (total[:tail] * row_scale + rows_ref[...]).astype(bf16).astype(f32)
    size = 2 * heads
    query_pre, forget_pre = pre[:size], pre[size : 2 * size]
    input_pre, outgate_pre = pre[2 * size : 3 * size], pre[3 * size :]

    tp = tp_ref[0]
    for chunk in range(piece_chunks):
        at = tp * piece_chunks + chunk
        rows = arrived_ref[at, tail : tail + 8, :].astype(f32)
        params = params_ref[at].astype(f32)
        rows = ((rows - mean) * scale * params[0:1] + params[3:4]).astype(bf16).astype(f32)
        piece_ref[2 * chunk : 2 * chunk + 2, :] = residual_scale * rows[0:2]

    for head in range(heads):
        at = slice(2 * head, 2 * head + 2)
        low_rows_ref[at, :] = jnp.broadcast_to(low_ref[head : head + 1, :], (2, LANES))
        gain_rows_ref[at, :] = jnp.broadcast_to(head_gain_ref[head : head + 1, :], (2, LANES))
    low = low_rows_ref[...]
    forget = (low + (1.0 - low) * jax.nn.sigmoid(forget_pre)).T
    key = ((1.0 - low) * jax.nn.sigmoid(-forget_pre)).T
    query = jax.nn.silu(query_pre).T
    updated_copies = []
    for head in range(heads):
        for seq in range(seqs):
            row = head * 2 + seq
            new = (
                forget[:, row : row + 1] * state_ref[seq, head]
                + key[:, row : row + 1] * input_pre[row : row + 1, :]
            )
            updated_ref[seq, head] = new
            updated_copies.append(
                pltpu.make_async_copy(
                    updated_ref.at[seq, head], updated_hbm.at[seq, head], updated_sem.at[row]
                )
            )
            updated_copies[-1].start()
            readout_ref[row : row + 1, :] = jnp.sum(
                query[:, row : row + 1] * new, axis=0, keepdims=True
            )
    readout = readout_ref[...]
    readout = readout * lax.rsqrt(jnp.mean(readout * readout, axis=1, keepdims=True) + head_eps)
    gated = readout * gain_rows_ref[...] * jax.nn.silu(outgate_pre)
    gated_ref[...] = jnp.zeros(gated_ref.shape, f32)
    for head in range(heads):
        gated_ref[0:2, head * HEAD : (head + 1) * HEAD] = gated[2 * head : 2 * head + 2]
    lhs = gated_ref[...].astype(bf16)
    for part in range(parts):
        weight = weight_ref[:, part * step : (part + 1) * step]
        mixed = jnp.dot(lhs, weight, preferred_element_type=f32)
        for chunk in range(piece_chunks):
            sent_ref[part, 2 * chunk : 2 * chunk + 2, :] = mixed[
                0:2, chunk * LANES : (chunk + 1) * LANES
            ]
    for copy in updated_copies:
        copy.wait()


def mixer(tp, arrived, params, lower_bound, head_gain, state, weight, parts):
    seqs, heads = state.shape[:2]
    width = weight.shape[1]
    rows = 2 * width // parts // LANES
    vmem, anywhere = pl.BlockSpec(memory_space=pltpu.VMEM), pl.BlockSpec(memory_space=pl.ANY)
    return pl.pallas_call(
        mixer_kernel,
        in_specs=[pl.BlockSpec(memory_space=pltpu.SMEM)] + [vmem] * 6,
        out_specs=[vmem, vmem, anywhere],
        out_shape=[
            jax.ShapeDtypeStruct((parts, rows, LANES), f32),
            jax.ShapeDtypeStruct((rows, LANES), f32),
            jax.ShapeDtypeStruct(state.shape, f32),
        ],
        scratch_shapes=[
            pltpu.VMEM(state.shape, f32),
            pltpu.VMEM((seqs * 4 * heads, LANES), f32),
            pltpu.VMEM((2 * heads, LANES), f32),
            pltpu.VMEM((2 * heads, LANES), f32),
            pltpu.VMEM((2 * heads, LANES), f32),
            pltpu.VMEM((8, heads * HEAD), f32),
            pltpu.SemaphoreType.DMA((seqs * heads,)),
        ],
        compiler_params=pltpu.CompilerParams(vmem_limit_bytes=8 * 2**20),
        name="mixer",
    )(tp.reshape(1), arrived, params, lower_bound, head_gain, state, weight)


def local(
    tokens,
    gate_weights,
    up_weights,
    down_weights,
    norm_gain,
    norm_bias,
    query_weight,
    forget_weight,
    input_weight,
    outgate_weight,
    lower_bound,
    head_gain,
    out_weight,
    state,
):
    batch, own_cols = tokens.shape
    heads = state.shape[1]
    kv_count, tp_count = lax.axis_size(KV), lax.axis_size(TP)
    x_count = tp_count // 2
    chip_count = kv_count * x_count
    half = batch // 2
    width = own_cols * kv_count * tp_count
    kv, tp, core = lax.axis_index(KV), lax.axis_index(TP), lax.axis_index(CORE)

    turned = tokens.reshape(kv_count, 2, own_cols).swapaxes(0, 1).reshape(batch, own_cols)
    lines = jnp.concatenate([turned, norm_gain, norm_bias, jnp.zeros((2, own_cols), bf16)])
    place = (
        lax.broadcasted_iota(jnp.int32, (own_cols, LANES), 1)
        == lax.broadcasted_iota(jnp.int32, (own_cols, LANES), 0) + tp * own_cols
    ).astype(bf16)
    placed = jnp.dot(lines, place, preferred_element_type=f32).astype(bf16)
    block = to_everyone(placed, TP, tp_count).astype(f32).sum(axis=0).astype(bf16)
    own_half = lax.dynamic_slice_in_dim(block, core * half, half, 0)
    arrived = to_everyone(jnp.concatenate([own_half, block[batch:]]), KV, kv_count)
    both = lax.all_gather(arrived, CORE, axis=0)
    whole_tokens = both[:, :, :half].swapaxes(1, 2).reshape(batch, width)
    params = both[0, :, half:]

    def sum_over_kv(partial_value, extra):
        pieces = partial_value.astype(bf16).reshape(2, half, kv_count, LANES).swapaxes(1, 2)
        kept = lax.dynamic_index_in_dim(pieces, core, 0, keepdims=False)
        sent = lax.dynamic_index_in_dim(pieces, 1 - core, 0, keepdims=False)
        paired = (kept.astype(f32) + lax.ppermute(sent, CORE, SWAP).astype(f32)).astype(bf16)
        if extra is not None:
            paired = jnp.concatenate([paired, extra], axis=1)
        return exchange(paired, KV).astype(f32).sum(axis=0)

    def over_tp(lines):
        gathered = to_everyone(lines, TP, tp_count)
        return gathered.reshape(x_count, 2, *lines.shape)

    partial_one = ffn_partial(whole_tokens, gate_weights, up_weights, down_weights, 0)
    weights = (query_weight, forget_weight, input_weight, outgate_weight)
    chunk_count = 4 * heads

    def project(lines):
        return jnp.concatenate(
            [jnp.dot(lines, w, preferred_element_type=f32) for w in weights], axis=1
        )

    share = kv_count // chunk_count
    gain_one, bias_one = block[batch : batch + 1], block[batch + 3 : batch + 4]
    bias_part = project(bias_one)
    bias_rows = jnp.repeat(bias_part.reshape(chunk_count, 1, LANES), share, axis=0).astype(bf16)
    row_sum = partial_one.sum(axis=1)
    high = row_sum.astype(bf16)
    low = (row_sum - high.astype(f32)).astype(bf16)
    sum_row = jnp.broadcast_to(jnp.concatenate([high, low])[None, None], (kv_count, 1, LANES))
    extra = jnp.concatenate([sum_row, bias_rows, jnp.zeros((kv_count, 6, LANES), bf16)], axis=1)
    arrived = sum_over_kv(partial_one, extra)
    bias_own = arrived[half + 1 : half + 2] / share
    gathered = over_tp(arrived[: half + 8])
    total = gathered[:, :, :half].sum(axis=0).reshape(batch, LANES)
    total_row = gathered[:, :, half].sum(axis=(0, 1))
    stream_one = residual_scale * block[:batch].astype(f32) + 0.5 * total
    row_mean = (
        residual_scale * whole_tokens.astype(f32).sum(axis=1)
        + 0.5 * (total_row[:batch] + total_row[batch:])
    ) / width
    centred = stream_one - row_mean[:, None]

    scaled = (centred * gain_one.astype(f32)).astype(bf16)
    projected = project(scaled).astype(bf16)
    projected = projected.reshape(2, half, chunk_count, LANES).transpose(1, 2, 0, 3)
    blocks = jnp.concatenate(
        [
            projected.reshape(kv_count, 2 * chunk_count, LANES),
            centred.astype(bf16).reshape(2, half, LANES).swapaxes(0, 1),
            jnp.broadcast_to(bias_own.astype(bf16)[None], (kv_count, 1, LANES)),
            jnp.zeros((kv_count, 5, LANES), bf16),
        ],
        axis=1,
    )
    arrived = exchange(blocks, KV)
    mixer_part, piece, updated = mixer(
        tp,
        arrived,
        params,
        lower_bound.reshape(heads, HEAD),
        head_gain.reshape(heads, HEAD),
        state,
        out_weight,
        tp_count,
    )
    mixer_sum = exchange(mixer_part, TP).sum(axis=0)
    stream_own = (piece + mixer_sum).astype(bf16)
    arrived = lax.all_gather(to_everyone(stream_own, CHIPS, chip_count), CORE, axis=0)
    arrived = arrived.reshape(2, kv_count, x_count, *stream_own.shape)
    normed_two = norm_of_tiles(arrived, params)

    partial_two = ffn_partial(normed_two, gate_weights, up_weights, down_weights, 1)
    total = over_tp(sum_over_kv(partial_two, None)).sum(axis=0).reshape(batch, LANES)
    own_normed = lax.dynamic_slice_in_dim(normed_two, kv * LANES, LANES, 1)
    stream_three = residual_scale * own_normed.astype(f32) + 0.5 * total
    block_sum = stream_three.sum(axis=1)
    block_mean = block_sum / LANES
    off = stream_three - block_mean[:, None]
    stats = jnp.concatenate([block_mean, (off * off).sum(axis=1)])[None]
    stats = to_everyone(stats, KV, kv_count)[:, 0]
    means, squares = stats[:, :batch], stats[:, batch:]
    row_mean = means.mean(axis=0)
    spread = (squares.sum(axis=0) + LANES * ((means - row_mean) ** 2).sum(axis=0)) / width
    own = lax.dynamic_slice_in_dim(stream_three, tp * own_cols, own_cols, 1)
    mixed = (own - row_mean[:, None]) * lax.rsqrt(spread + norm_eps)[:, None] * norm_gain[
        2
    ].astype(f32) + norm_bias[2].astype(f32)
    mixed = mixed.reshape(2, half, own_cols).swapaxes(0, 1).reshape(batch, own_cols)
    return (mixed.astype(bf16), updated)


def solution(mesh):
    finer = Mesh(mesh.devices.reshape(8, 4, 4, 2), KV_TP)
    in_specs = (
        P(None, KV_TP),
        P(None, None, KV_TP),
        P(None, None, KV_TP),
        P(None, KV_TP, None),
        P(None, KV_TP),
        P(None, KV_TP),
        P(KV, TP),
        P(KV, TP),
        P(KV, TP),
        P(KV, TP),
        P(TP),
        P(TP),
        P(TP, None),
        P(KV, TP, None, None),
    )
    out_specs = (P(None, KV_TP), P(KV, TP, None, None))
    return jax.shard_map(local, mesh=finer, in_specs=in_specs, out_specs=out_specs, check_vma=False)
```

```python
import jax
import jax.numpy as jnp
from jax import lax
from jax.experimental import pallas as pl
from jax.experimental.pallas import tpu as pltpu
from jax.sharding import Mesh
from jax.sharding import PartitionSpec as P

HEAD = 128
LANES = 128
KV_TP = ("kv_0", "kv_1", "tp_0", "tp_1")
KV = ("kv_0", "kv_1")
TP = ("tp_0", "tp_1")
CHIPS = ("kv_0", "kv_1", "tp_0")
CORE = "tp_1"
SWAP = [(0, 1), (1, 0)]

residual_scale = 8.0**0.25
norm_eps = 1e-05
head_eps = 1e-06
bf16 = jnp.bfloat16
f32 = jnp.float32


def exchange(blocks, axes):
    return lax.all_to_all(blocks, axes, split_axis=0, concat_axis=0, tiled=True)


def to_everyone(block, axes, count):
    return exchange(jnp.broadcast_to(block[None], (count, *block.shape)), axes)


def alone(blocks, axes, *held):
    blocks, *held = lax.optimization_barrier((blocks, *held))
    return lax.optimization_barrier((exchange(blocks, axes), *held))


def copies(block, count):
    return jnp.broadcast_to(block[None], (count, *block.shape))


def ffn_partial(whole_rows, gate_ws, up_ws, down_ws, layer):
    gate_proj = jnp.einsum("sf,lfh->shl", whole_rows, gate_ws, preferred_element_type=f32)
    up_proj = jnp.einsum("sf,lfh->shl", whole_rows, up_ws, preferred_element_type=f32)
    hidden = (jax.nn.silu(gate_proj) * up_proj).astype(bf16)
    own = lax.broadcasted_iota(jnp.int32, hidden.shape, 2) == layer
    hidden = jnp.where(own, hidden, 0)
    return jnp.einsum("shl,lhf->sf", hidden, down_ws, preferred_element_type=f32)


def norm_kernel(arrived_ref, params_ref, result_ref, raw_ref):
    cores, kv_count, x_count, rows, _ = arrived_ref.shape
    pieces = rows // 2
    chunks = cores * x_count * pieces
    for x in range(x_count):
        for core in range(cores):
            tiles = arrived_ref[core, :, x].astype(f32)
            raw_ref[x * cores + core] = tiles.reshape(kv_count * rows, LANES)

    def lines(chunk, seq):
        at = (chunk % pieces) * 2 + seq
        return raw_ref[chunk // pieces, pl.ds(at, kv_count, stride=rows), :]

    width = chunks * LANES
    for seq in range(2):
        total = sum(lines(chunk, seq) for chunk in range(chunks))
        mean = jnp.sum(total, axis=1, keepdims=True) / width
        squares = jnp.zeros((kv_count, LANES), f32)
        for chunk in range(chunks):
            off = lines(chunk, seq) - mean
            squares = squares + off * off
        spread = jnp.sum(squares, axis=1, keepdims=True) / width
        scale = lax.rsqrt(spread + norm_eps)
        for chunk in range(chunks):
            params = params_ref[chunk].astype(f32)
            normed = (lines(chunk, seq) - mean) * scale * params[1:2] + params[4:5]
            result_ref[
                seq * kv_count : (seq + 1) * kv_count, chunk * LANES : (chunk + 1) * LANES
            ] = normed.astype(bf16)


def norm_of_tiles(arrived, params):
    cores, kv_count, x_count, rows, lanes = arrived.shape
    return pl.pallas_call(
        norm_kernel,
        out_shape=jax.ShapeDtypeStruct((2 * kv_count, cores * x_count * rows // 2 * lanes), bf16),
        scratch_shapes=[pltpu.VMEM((cores * x_count, kv_count * rows, lanes), f32)],
        compiler_params=pltpu.CompilerParams(vmem_limit_bytes=8 * 2**20),
        name="norm_two",
    )(arrived, params)


def mixer_kernel(
    tp_ref,
    arrived_ref,
    params_ref,
    low_ref,
    head_gain_ref,
    state_ref,
    weight_hbm,
    sent_ref,
    piece_ref,
    updated_hbm,
    updated_ref,
    weight_ref,
    rows_ref,
    low_rows_ref,
    gain_rows_ref,
    readout_ref,
    gated_ref,
    updated_sem,
    weight_sem,
):
    seqs, heads = state_ref.shape[:2]
    kv_count = arrived_ref.shape[0]
    chunks = 4 * heads
    share = kv_count // chunks
    parts = sent_ref.shape[0]
    piece_chunks = kv_count // parts
    step = weight_ref.shape[2]
    weight_copies = [
        pltpu.make_async_copy(
            weight_hbm.at[:, pl.ds(part * step, step)], weight_ref.at[part], weight_sem.at[part]
        )
        for part in range(parts)
    ]
    for copy in weight_copies:
        copy.start()

    total = arrived_ref[0].astype(f32)
    for block in range(1, kv_count):
        total = total + arrived_ref[block].astype(f32)
    tail = seqs * chunks
    width = kv_count * LANES
    mean = jnp.sum(total[tail : tail + 8], axis=1, keepdims=True) / width
    squares = jnp.zeros((8, LANES), f32)
    for block in range(kv_count):
        off = arrived_ref[block, tail : tail + 8, :].astype(f32) - mean
        squares = squares + off * off
    scale = lax.rsqrt(jnp.sum(squares, axis=1, keepdims=True) / width + norm_eps)
    for chunk in range(chunks):
        bias = arrived_ref[chunk * share, tail : tail + 8, :].astype(f32)
        for other in range(1, share):
            bias = bias + arrived_ref[chunk * share + other, tail : tail + 8, :].astype(f32)
        rows_ref[2 * chunk : 2 * chunk + 2, :] = jnp.broadcast_to(bias[2:3], (2, LANES))
    odd = lax.broadcasted_iota(jnp.int32, (tail, LANES), 0) % 2 == 1
    row_scale = jnp.where(odd, scale[1:2], scale[0:1])
    pre = (total[:tail] * row_scale + rows_ref[...]).astype(bf16).astype(f32)
    size = 2 * heads
    query_pre, forget_pre = pre[:size], pre[size : 2 * size]
    input_pre, outgate_pre = pre[2 * size : 3 * size], pre[3 * size :]

    tp = tp_ref[0]
    for chunk in range(piece_chunks):
        at = tp * piece_chunks + chunk
        rows = arrived_ref[at, tail : tail + 8, :].astype(f32)
        params = params_ref[at].astype(f32)
        rows = ((rows - mean) * scale * params[0:1] + params[3:4]).astype(bf16).astype(f32)
        piece_ref[2 * chunk : 2 * chunk + 2, :] = residual_scale * rows[0:2]

    for head in range(heads):
        at = slice(2 * head, 2 * head + 2)
        low_rows_ref[at, :] = jnp.broadcast_to(low_ref[head : head + 1, :], (2, LANES))
        gain_rows_ref[at, :] = jnp.broadcast_to(head_gain_ref[head : head + 1, :], (2, LANES))
    low = low_rows_ref[...]
    forget = (low + (1.0 - low) * jax.nn.sigmoid(forget_pre)).T
    key = ((1.0 - low) * jax.nn.sigmoid(-forget_pre)).T
    query = jax.nn.silu(query_pre).T
    updated_copies = []
    for head in range(heads):
        for seq in range(seqs):
            row = head * 2 + seq
            new = (
                forget[:, row : row + 1] * state_ref[seq, head]
                + key[:, row : row + 1] * input_pre[row : row + 1, :]
            )
            updated_ref[seq, head] = new
            updated_copies.append(
                pltpu.make_async_copy(
                    updated_ref.at[seq, head], updated_hbm.at[seq, head], updated_sem.at[row]
                )
            )
            updated_copies[-1].start()
            readout_ref[row : row + 1, :] = jnp.sum(
                query[:, row : row + 1] * new, axis=0, keepdims=True
            )
    readout = readout_ref[...]
    readout = readout * lax.rsqrt(jnp.mean(readout * readout, axis=1, keepdims=True) + head_eps)
    gated = readout * gain_rows_ref[...] * jax.nn.silu(outgate_pre)
    gated_ref[...] = jnp.zeros(gated_ref.shape, f32)
    for head in range(heads):
        gated_ref[0:2, head * HEAD : (head + 1) * HEAD] = gated[2 * head : 2 * head + 2]
    lhs = gated_ref[...].astype(bf16)
    for part in range(parts):
        weight_copies[part].wait()
        mixed = jnp.dot(lhs, weight_ref[part], preferred_element_type=f32)
        for chunk in range(piece_chunks):
            sent_ref[part, 2 * chunk : 2 * chunk + 2, :] = mixed[
                0:2, chunk * LANES : (chunk + 1) * LANES
            ]
    for copy in updated_copies:
        copy.wait()


def mixer(tp, arrived, params, lower_bound, head_gain, state, weight, parts):
    seqs, heads = state.shape[:2]
    depth, width = weight.shape
    rows = 2 * width // parts // LANES
    vmem, anywhere = pl.BlockSpec(memory_space=pltpu.VMEM), pl.BlockSpec(memory_space=pl.ANY)
    return pl.pallas_call(
        mixer_kernel,
        in_specs=[pl.BlockSpec(memory_space=pltpu.SMEM)] + [vmem] * 5 + [anywhere],
        out_specs=[vmem, vmem, anywhere],
        out_shape=[
            jax.ShapeDtypeStruct((parts, rows, LANES), f32),
            jax.ShapeDtypeStruct((rows, LANES), f32),
            jax.ShapeDtypeStruct(state.shape, f32),
        ],
        scratch_shapes=[
            pltpu.VMEM(state.shape, f32),
            pltpu.VMEM((parts, depth, width // parts), bf16),
            pltpu.VMEM((seqs * 4 * heads, LANES), f32),
            pltpu.VMEM((2 * heads, LANES), f32),
            pltpu.VMEM((2 * heads, LANES), f32),
            pltpu.VMEM((2 * heads, LANES), f32),
            pltpu.VMEM((8, heads * HEAD), f32),
            pltpu.SemaphoreType.DMA((seqs * heads,)),
            pltpu.SemaphoreType.DMA((parts,)),
        ],
        compiler_params=pltpu.CompilerParams(vmem_limit_bytes=8 * 2**20),
        name="mixer",
    )(
        tp.reshape(1),
        arrived,
        params,
        lower_bound,
        head_gain,
        state,
        pltpu.with_memory_space_constraint(weight, pltpu.HBM),
    )


def local(
    tokens,
    gate_weights,
    up_weights,
    down_weights,
    norm_gain,
    norm_bias,
    query_weight,
    forget_weight,
    input_weight,
    outgate_weight,
    lower_bound,
    head_gain,
    out_weight,
    state,
):
    batch, own_cols = tokens.shape
    heads = state.shape[1]
    kv_count, tp_count = lax.axis_size(KV), lax.axis_size(TP)
    x_count = tp_count // 2
    chip_count = kv_count * x_count
    half = batch // 2
    width = own_cols * kv_count * tp_count
    kv, tp, core = lax.axis_index(KV), lax.axis_index(TP), lax.axis_index(CORE)

    turned = tokens.reshape(kv_count, 2, own_cols).swapaxes(0, 1).reshape(batch, own_cols)
    lines = jnp.concatenate([turned, norm_gain, norm_bias, norm_gain[:2]])
    place = (
        lax.broadcasted_iota(jnp.int32, (own_cols, LANES), 1)
        == lax.broadcasted_iota(jnp.int32, (own_cols, LANES), 0) + tp * own_cols
    ).astype(bf16)
    placed = jnp.dot(lines, place, preferred_element_type=f32).astype(bf16)
    first, second = jnp.int32(0), jnp.int32(1)
    arrived, kv, tp, core, first, second, norm_gain, norm_bias = alone(
        copies(placed, tp_count), TP, kv, tp, core, first, second, norm_gain, norm_bias
    )
    block = arrived.astype(f32).sum(axis=0).astype(bf16)
    own_half = lax.dynamic_slice_in_dim(block, core * half, half, 0)
    arrived = to_everyone(jnp.concatenate([own_half, block[batch:]]), KV, kv_count)
    both = lax.all_gather(arrived, CORE, axis=0)
    whole_tokens = both[:, :, :half].swapaxes(1, 2).reshape(batch, width)
    params = both[0, :, half:]

    def sum_over_kv(partial_value, extra, *held):
        pieces = partial_value.astype(bf16).reshape(2, half, kv_count, LANES).swapaxes(1, 2)
        kept = lax.dynamic_index_in_dim(pieces, core, 0, keepdims=False)
        sent = lax.dynamic_index_in_dim(pieces, 1 - core, 0, keepdims=False)
        paired = (kept.astype(f32) + lax.ppermute(sent, CORE, SWAP).astype(f32)).astype(bf16)
        if extra is not None:
            paired = jnp.concatenate([paired, extra], axis=1)
        arrived, *held = alone(paired, KV, *held)
        return arrived.astype(f32).sum(axis=0), *held

    def over_tp(lines, *held):
        gathered, *held = alone(copies(lines, tp_count), TP, *held)
        return gathered.reshape(x_count, 2, *lines.shape), *held

    partial_one = ffn_partial(whole_tokens, gate_weights, up_weights, down_weights, first)
    weights = (query_weight, forget_weight, input_weight, outgate_weight)
    chunk_count = 4 * heads

    def project(lines):
        return jnp.concatenate(
            [jnp.dot(lines, w, preferred_element_type=f32) for w in weights], axis=1
        )

    share = kv_count // chunk_count
    bias_one = block[batch + 3 : batch + 4]
    bias_part = project(bias_one)
    bias_rows = jnp.repeat(bias_part.reshape(chunk_count, 1, LANES), share, axis=0).astype(bf16)
    row_sum = partial_one.sum(axis=1)
    high = row_sum.astype(bf16)
    low = (row_sum - high.astype(f32)).astype(bf16)
    sum_row = jnp.broadcast_to(jnp.concatenate([high, low])[None, None], (kv_count, 1, LANES))
    extra = jnp.concatenate([sum_row] + [bias_rows] * 7, axis=1)
    token_sum = whole_tokens.astype(f32).sum(axis=1)
    arrived, kv, tp, core, second, norm_gain, norm_bias, block, params, token_sum = sum_over_kv(
        partial_one, extra, kv, tp, core, second, norm_gain, norm_bias, block, params, token_sum
    )
    gathered, kv, tp, core, second, norm_gain, norm_bias, block, params, token_sum, arrived = over_tp(
        arrived, kv, tp, core, second, norm_gain, norm_bias, block, params, token_sum, arrived
    )
    bias_own = (arrived[half + 1 : half + 2] / share).astype(bf16)
    gain_one = block[batch : batch + 1]
    total = gathered[:, :, :half].sum(axis=0).reshape(batch, LANES)
    total_row = gathered[:, :, half].sum(axis=(0, 1))
    stream_one = residual_scale * block[:batch].astype(f32) + 0.5 * total
    row_mean = (
        residual_scale * token_sum
        + 0.5 * (total_row[:batch] + total_row[batch:])
    ) / width
    centred = stream_one - row_mean[:, None]

    scaled = (centred * gain_one.astype(f32)).astype(bf16)
    projected = project(scaled).astype(bf16)
    projected = projected.reshape(2, half, chunk_count, LANES).transpose(1, 2, 0, 3)
    blocks = jnp.concatenate(
        [
            projected.reshape(kv_count, 2 * chunk_count, LANES),
            centred.astype(bf16).reshape(2, half, LANES).swapaxes(0, 1),
            jnp.broadcast_to(bias_own[None], (kv_count, 6, LANES)),
        ],
        axis=1,
    )
    arrived, kv, tp, core, second, norm_gain, norm_bias, params = alone(
        blocks, KV, kv, tp, core, second, norm_gain, norm_bias, params
    )
    mixer_part, piece, updated = mixer(
        tp,
        arrived,
        params,
        lower_bound.reshape(heads, HEAD),
        head_gain.reshape(heads, HEAD),
        state,
        out_weight,
        tp_count,
    )
    arrived, kv, tp, core, second, norm_gain, norm_bias, params, piece = alone(
        mixer_part, TP, kv, tp, core, second, norm_gain, norm_bias, params, piece
    )
    stream_own = (piece + arrived.sum(axis=0)).astype(bf16)
    arrived, kv, tp, core, second, norm_gain, norm_bias, params = alone(
        copies(stream_own, chip_count), CHIPS, kv, tp, core, second, norm_gain, norm_bias, params
    )
    arrived = lax.all_gather(arrived, CORE, axis=0)
    arrived = arrived.reshape(2, kv_count, x_count, *stream_own.shape)
    normed_two = norm_of_tiles(arrived, params)

    partial_two = ffn_partial(normed_two, gate_weights, up_weights, down_weights, second)
    own_normed = normed_two
    arrived, kv, tp, norm_gain, norm_bias, own_normed = sum_over_kv(
        partial_two, None, kv, tp, norm_gain, norm_bias, own_normed
    )
    gathered, kv, tp, norm_gain, norm_bias, own_normed = over_tp(
        arrived, kv, tp, norm_gain, norm_bias, own_normed
    )
    total = gathered.sum(axis=0).reshape(batch, LANES)
    own_normed = lax.dynamic_slice_in_dim(own_normed, kv * LANES, LANES, 1)
    stream_three = residual_scale * own_normed.astype(f32) + 0.5 * total
    block_sum = stream_three.sum(axis=1)
    block_mean = block_sum / LANES
    off = stream_three - block_mean[:, None]
    stats = jnp.concatenate([block_mean, (off * off).sum(axis=1)])[None]
    stats, tp, norm_gain, norm_bias, stream_three = alone(
        copies(stats, kv_count), KV, tp, norm_gain, norm_bias, stream_three
    )
    stats = stats[:, 0]
    means, squares = stats[:, :batch], stats[:, batch:]
    row_mean = means.mean(axis=0)
    spread = (squares.sum(axis=0) + LANES * ((means - row_mean) ** 2).sum(axis=0)) / width
    own = lax.dynamic_slice_in_dim(stream_three, tp * own_cols, own_cols, 1)
    mixed = (own - row_mean[:, None]) * lax.rsqrt(spread + norm_eps)[:, None] * norm_gain[
        2
    ].astype(f32) + norm_bias[2].astype(f32)
    mixed = mixed.reshape(2, half, own_cols).swapaxes(0, 1).reshape(batch, own_cols)
    return (mixed.astype(bf16), updated)


def solution(mesh):
    finer = Mesh(mesh.devices.reshape(8, 4, 4, 2), KV_TP)
    in_specs = (
        P(None, KV_TP),
        P(None, None, KV_TP),
        P(None, None, KV_TP),
        P(None, KV_TP, None),
        P(None, KV_TP),
        P(None, KV_TP),
        P(KV, TP),
        P(KV, TP),
        P(KV, TP),
        P(KV, TP),
        P(TP),
        P(TP),
        P(TP, None),
        P(KV, TP, None, None),
    )
    out_specs = (P(None, KV_TP), P(KV, TP, None, None))
    return jax.shard_map(local, mesh=finer, in_specs=in_specs, out_specs=out_specs, check_vma=False)
```

```python
import jax
import jax.numpy as jnp
from jax import lax
from jax.experimental import pallas as pl
from jax.experimental.pallas import tpu as pltpu
from jax.sharding import Mesh
from jax.sharding import PartitionSpec as P

HEAD = 128
LANES = 128
KV_TP = ("kv_0", "kv_1", "tp_0", "tp_1")
KV = ("kv_0", "kv_1")
TP = ("tp_0", "tp_1")
CHIPS = ("kv_0", "kv_1", "tp_0")
CORE = "tp_1"
SWAP = [(0, 1), (1, 0)]

residual_scale = 8.0**0.25
norm_eps = 1e-05
head_eps = 1e-06
bf16 = jnp.bfloat16
f32 = jnp.float32


def exchange(blocks, axes):
    return lax.all_to_all(blocks, axes, split_axis=0, concat_axis=0, tiled=True)


def to_everyone(block, axes, count):
    return exchange(jnp.broadcast_to(block[None], (count, *block.shape)), axes)


def alone(blocks, axes, *held):
    blocks, *held = lax.optimization_barrier((blocks, *held))
    return lax.optimization_barrier((exchange(blocks, axes), *held))


def copies(block, count):
    return jnp.broadcast_to(block[None], (count, *block.shape))


def small(grant=8):
    return pltpu.CompilerParams(vmem_limit_bytes=grant * 2**20)


VMEM = pl.BlockSpec(memory_space=pltpu.VMEM)
SMEM = pl.BlockSpec(memory_space=pltpu.SMEM)
ANYWHERE = pl.BlockSpec(memory_space=pl.ANY)


def place_kernel(at_ref, tokens_ref, gain_ref, bias_ref, result_ref, lines_ref):
    own_cols, batch = tokens_ref.shape
    half = batch // 2
    shape = (own_cols, LANES)
    spot = lax.broadcasted_iota(jnp.int32, shape, 0) + at_ref[1] * own_cols
    place = (lax.broadcasted_iota(jnp.int32, shape, 1) == spot).astype(f32).astype(bf16)
    row = lax.broadcasted_iota(jnp.int32, (batch, batch), 0)
    source = 2 * (row % half) + row // half
    order = (lax.broadcasted_iota(jnp.int32, (batch, batch), 1) == source).astype(f32)
    turned = lax.dot_general(
        order.astype(bf16), tokens_ref[...], (((1,), (1,)), ((), ())), preferred_element_type=f32
    ).astype(bf16)
    lines_ref[batch:, :] = jnp.zeros((8, LANES), f32)
    lines_ref[:batch, :] = jnp.dot(turned, place, preferred_element_type=f32)
    lines_ref[batch : batch + 3, :] = jnp.dot(gain_ref[...], place, preferred_element_type=f32)
    lines_ref[batch + 3 : batch + 6, :] = jnp.dot(bias_ref[...], place, preferred_element_type=f32)
    lines = lines_ref[...].astype(bf16)
    for copy in range(result_ref.shape[0]):
        result_ref[copy] = lines


def placed_copies(at, tokens, gain, bias, count):
    batch, own_cols = tokens.shape
    return pl.pallas_call(
        place_kernel,
        in_specs=[SMEM, VMEM, VMEM, VMEM],
        out_specs=VMEM,
        out_shape=jax.ShapeDtypeStruct((count, batch + 8, LANES), bf16),
        scratch_shapes=[pltpu.VMEM((batch + 8, LANES), f32)],
        compiler_params=small(),
        name="place",
    )(at, tokens.T, gain, bias)


def prepare_kernel(lines_ref, w0, w1, w2, w3, weight_hbm, bias_ref, weight_ref, weight_sem):
    parts, _, step = weight_ref.shape
    weight_copies = [
        pltpu.make_async_copy(
            weight_hbm.at[:, pl.ds(part * step, step)], weight_ref.at[part], weight_sem.at[part]
        )
        for part in range(parts)
    ]
    for copy in weight_copies:
        copy.start()
    lines = lines_ref[...]
    for index, w_ref in enumerate((w0, w1, w2, w3)):
        sums = jnp.dot(lines, w_ref[...], preferred_element_type=f32)
        heads = sums.shape[1] // LANES
        for head in range(heads):
            chunk = index * heads + head
            bias_ref[chunk : chunk + 1, :] = sums[3:4, head * LANES : (head + 1) * LANES]
    for copy in weight_copies:
        copy.wait()


def prepare(lines, weights, weight, parts):
    depth, width = weight.shape
    return pl.pallas_call(
        prepare_kernel,
        in_specs=[VMEM] * 5 + [ANYWHERE],
        out_specs=[VMEM, VMEM],
        out_shape=[
            jax.ShapeDtypeStruct((4 * weights[0].shape[1] // LANES, LANES), f32),
            jax.ShapeDtypeStruct((parts, depth, width // parts), bf16),
        ],
        scratch_shapes=[pltpu.SemaphoreType.DMA((parts,))],
        compiler_params=small(),
        name="prepare",
    )(lines, *weights, pltpu.with_memory_space_constraint(weight, pltpu.HBM))


def feed_forward(rows, core, layer, gate_ref, up_ref, down_ref):
    def stored(ref):
        return ref[...].reshape(ref.shape[0] * ref.shape[1], ref.shape[2])

    dims = (((1,), (1,)), ((), ()))
    gate = lax.dot_general(rows, stored(gate_ref), dims, preferred_element_type=f32)
    up = lax.dot_general(rows, stored(up_ref), dims, preferred_element_type=f32)
    hidden = jax.nn.silu(gate) * up
    unit = lax.broadcasted_iota(jnp.int32, hidden.shape, 1)
    hidden = jnp.where(unit % 2 == layer, hidden, 0.0)
    half = hidden.shape[0] // 2
    low, high = hidden[:half], hidden[half:]
    first = core == 0
    hidden = jnp.concatenate([jnp.where(first, low, high), jnp.where(first, high, low)])
    return jnp.dot(hidden.astype(bf16), stored(down_ref), preferred_element_type=f32)


def write_halves(part, kept_ref, sent_ref):
    chunks, half, _ = kept_ref.shape
    for chunk in range(chunks):
        at = slice(chunk * LANES, (chunk + 1) * LANES)
        kept_ref[chunk] = part[:half, at].astype(bf16)
        sent_ref[chunk] = part[half:, at].astype(bf16)


def first_kernel(
    at_ref, rows_ref, gate_ref, up_ref, down_ref, kept_ref, sent_ref, tail_ref, total_ref, x_ref
):
    chunks, half, _ = kept_ref.shape
    core = at_ref[2]
    for seq in range(2):
        at = slice(seq * half, (seq + 1) * half)
        total = jnp.zeros((half, LANES), f32)
        for chunk in range(chunks):
            lines = rows_ref[seq, chunk, :half, :]
            x_ref[at, chunk * LANES : (chunk + 1) * LANES] = lines
            total = total + lines.astype(f32)
        total_ref[at, :] = jnp.broadcast_to(jnp.sum(total, axis=1, keepdims=True), (half, LANES))
    part = feed_forward(x_ref[...], core, 0, gate_ref, up_ref, down_ref)
    write_halves(part, kept_ref, sent_ref)
    batch = 2 * half
    sums = jnp.broadcast_to(jnp.sum(part, axis=1, keepdims=True), (batch, LANES))
    row = (lax.broadcasted_iota(jnp.int32, (batch, LANES), 0) + core * half) % batch
    lane = lax.broadcasted_iota(jnp.int32, (batch, LANES), 1)
    line = jnp.sum(jnp.where(lane % batch == row, sums, 0.0), axis=0, keepdims=True)
    high = line.astype(bf16).astype(f32)
    line = jnp.where(lane[:1] < batch, high, line - high)
    tail_ref[...] = jnp.broadcast_to(line, tail_ref.shape)


def stored_order(gate, up, down):
    return gate.transpose(2, 0, 1), up.transpose(2, 0, 1), down.transpose(1, 0, 2)


def first_block(at, rows, gate, up, down, half):
    chunks = rows.shape[1]
    return pl.pallas_call(
        first_kernel,
        in_specs=[SMEM] + [VMEM] * 4,
        out_specs=[VMEM] * 4,
        out_shape=[
            jax.ShapeDtypeStruct((chunks, half, LANES), bf16),
            jax.ShapeDtypeStruct((chunks, half, LANES), bf16),
            jax.ShapeDtypeStruct((8, LANES), f32),
            jax.ShapeDtypeStruct((2 * half, LANES), f32),
        ],
        scratch_shapes=[pltpu.VMEM((2 * half, chunks * LANES), bf16)],
        compiler_params=small(12),
        name="first_block",
    )(at, rows, *stored_order(gate, up, down))


def blocks_kernel(kept_ref, came_ref, tail_ref, bias_ref, result_ref):
    chunks, half, _ = kept_ref.shape
    share = chunks // bias_ref.shape[0]
    top = lax.broadcasted_iota(jnp.int32, (8, LANES), 0) == 0
    for chunk in range(chunks):
        both = kept_ref[chunk].astype(f32) + came_ref[chunk].astype(f32)
        result_ref[chunk, :half, :] = both.astype(bf16)
        bias = bias_ref[chunk // share : chunk // share + 1, :]
        result_ref[chunk, half:, :] = jnp.where(top, tail_ref[...], bias).astype(bf16)


def first_blocks(kept, came, tail, bias):
    chunks, half, lanes = kept.shape
    return pl.pallas_call(
        blocks_kernel,
        in_specs=[VMEM] * 4,
        out_specs=VMEM,
        out_shape=jax.ShapeDtypeStruct((chunks, half + 8, lanes), bf16),
        compiler_params=small(),
        name="first_blocks",
    )(kept, came, tail, bias)


def second_kernel(
    at_ref,
    arrived_ref,
    params_ref,
    gate_ref,
    up_ref,
    down_ref,
    kept_ref,
    sent_ref,
    own_ref,
    raw_ref,
    result_ref,
):
    cores, kv_count, x_count, rows, _ = arrived_ref.shape
    pieces = rows // 2
    chunks = cores * x_count * pieces
    for x in range(x_count):
        for core in range(cores):
            tiles = arrived_ref[core, :, x].astype(f32)
            raw_ref[x * cores + core] = tiles.reshape(kv_count * rows, LANES)

    def lines(chunk, seq):
        at = (chunk % pieces) * 2 + seq
        return raw_ref[chunk // pieces, pl.ds(at, kv_count, stride=rows), :]

    width = chunks * LANES
    for seq in range(2):
        total = sum(lines(chunk, seq) for chunk in range(chunks))
        mean = jnp.sum(total, axis=1, keepdims=True) / width
        squares = jnp.zeros((kv_count, LANES), f32)
        for chunk in range(chunks):
            off = lines(chunk, seq) - mean
            squares = squares + off * off
        spread = jnp.sum(squares, axis=1, keepdims=True) / width
        scale = lax.rsqrt(spread + norm_eps)
        for chunk in range(chunks):
            params = params_ref[chunk].astype(f32)
            normed = (lines(chunk, seq) - mean) * scale * params[1:2] + params[4:5]
            result_ref[
                seq * kv_count : (seq + 1) * kv_count, chunk * LANES : (chunk + 1) * LANES
            ] = normed.astype(bf16)
    own_ref[...] = result_ref[:, pl.ds(pl.multiple_of(at_ref[0] * LANES, LANES), LANES)]
    part = feed_forward(result_ref[...], at_ref[2], 1, gate_ref, up_ref, down_ref)
    write_halves(part, kept_ref, sent_ref)


def second_block(at, arrived, params, gate, up, down):
    cores, kv_count, x_count, rows, lanes = arrived.shape
    chunks = cores * x_count * rows // 2
    return pl.pallas_call(
        second_kernel,
        in_specs=[SMEM] + [VMEM] * 5,
        out_specs=[VMEM] * 3,
        out_shape=[
            jax.ShapeDtypeStruct((chunks, kv_count, lanes), bf16),
            jax.ShapeDtypeStruct((chunks, kv_count, lanes), bf16),
            jax.ShapeDtypeStruct((2 * kv_count, lanes), bf16),
        ],
        scratch_shapes=[
            pltpu.VMEM((cores * x_count, kv_count * rows, lanes), f32),
            pltpu.VMEM((2 * kv_count, chunks * lanes), bf16),
        ],
        compiler_params=small(12),
        name="second_block",
    )(at, arrived, params, *stored_order(gate, up, down))


def mixer_kernel(
    at_ref,
    arrived_ref,
    params_ref,
    low_ref,
    head_gain_ref,
    state_ref,
    weight_ref,
    sent_ref,
    piece_ref,
    updated_hbm,
    updated_ref,
    rows_ref,
    low_rows_ref,
    gain_rows_ref,
    readout_ref,
    gated_ref,
    updated_sem,
):
    seqs, heads = state_ref.shape[:2]
    kv_count = arrived_ref.shape[0]
    chunks = 4 * heads
    share = kv_count // chunks
    parts = sent_ref.shape[0]
    piece_chunks = kv_count // parts
    total = arrived_ref[0].astype(f32)
    for block in range(1, kv_count):
        total = total + arrived_ref[block].astype(f32)
    tail = seqs * chunks
    width = kv_count * LANES
    mean = jnp.sum(total[tail : tail + 8], axis=1, keepdims=True) / width
    squares = jnp.zeros((8, LANES), f32)
    for block in range(kv_count):
        off = arrived_ref[block, tail : tail + 8, :].astype(f32) - mean
        squares = squares + off * off
    scale = lax.rsqrt(jnp.sum(squares, axis=1, keepdims=True) / width + norm_eps)
    for chunk in range(chunks):
        bias = arrived_ref[chunk * share, tail : tail + 8, :].astype(f32)
        for other in range(1, share):
            bias = bias + arrived_ref[chunk * share + other, tail : tail + 8, :].astype(f32)
        rows_ref[2 * chunk : 2 * chunk + 2, :] = jnp.broadcast_to(bias[2:3], (2, LANES))
    odd = lax.broadcasted_iota(jnp.int32, (tail, LANES), 0) % 2 == 1
    row_scale = jnp.where(odd, scale[1:2], scale[0:1])
    pre = (total[:tail] * row_scale + rows_ref[...]).astype(bf16).astype(f32)
    size = 2 * heads
    query_pre, forget_pre = pre[:size], pre[size : 2 * size]
    input_pre, outgate_pre = pre[2 * size : 3 * size], pre[3 * size :]

    tp = at_ref[1]
    for chunk in range(piece_chunks):
        at = tp * piece_chunks + chunk
        rows = arrived_ref[at, tail : tail + 8, :].astype(f32)
        params = params_ref[at].astype(f32)
        rows = ((rows - mean) * scale * params[0:1] + params[3:4]).astype(bf16).astype(f32)
        piece_ref[2 * chunk : 2 * chunk + 2, :] = residual_scale * rows[0:2]

    for head in range(heads):
        at = slice(2 * head, 2 * head + 2)
        low_rows_ref[at, :] = jnp.broadcast_to(low_ref[head : head + 1, :], (2, LANES))
        gain_rows_ref[at, :] = jnp.broadcast_to(head_gain_ref[head : head + 1, :], (2, LANES))
    low = low_rows_ref[...]
    forget = (low + (1.0 - low) * jax.nn.sigmoid(forget_pre)).T
    key = ((1.0 - low) * jax.nn.sigmoid(-forget_pre)).T
    query = jax.nn.silu(query_pre).T
    updated_copies = []
    for head in range(heads):
        for seq in range(seqs):
            row = head * 2 + seq
            new = (
                forget[:, row : row + 1] * state_ref[seq, head]
                + key[:, row : row + 1] * input_pre[row : row + 1, :]
            )
            updated_ref[seq, head] = new
            updated_copies.append(
                pltpu.make_async_copy(
                    updated_ref.at[seq, head], updated_hbm.at[seq, head], updated_sem.at[row]
                )
            )
            updated_copies[-1].start()
            readout_ref[row : row + 1, :] = jnp.sum(
                query[:, row : row + 1] * new, axis=0, keepdims=True
            )
    readout = readout_ref[...]
    readout = readout * lax.rsqrt(jnp.mean(readout * readout, axis=1, keepdims=True) + head_eps)
    gated = readout * gain_rows_ref[...] * jax.nn.silu(outgate_pre)
    gated_ref[...] = jnp.zeros(gated_ref.shape, f32)
    for head in range(heads):
        gated_ref[0:2, head * HEAD : (head + 1) * HEAD] = gated[2 * head : 2 * head + 2]
    lhs = gated_ref[...].astype(bf16)
    for part in range(parts):
        mixed = jnp.dot(lhs, weight_ref[part], preferred_element_type=f32)
        for chunk in range(piece_chunks):
            sent_ref[part, 2 * chunk : 2 * chunk + 2, :] = mixed[
                0:2, chunk * LANES : (chunk + 1) * LANES
            ]
    for copy in updated_copies:
        copy.wait()


def mixer(at, arrived, params, lower_bound, head_gain, state, weight):
    seqs, heads = state.shape[:2]
    parts, _, step = weight.shape
    rows = 2 * step // LANES
    return pl.pallas_call(
        mixer_kernel,
        in_specs=[SMEM] + [VMEM] * 6,
        out_specs=[VMEM, VMEM, ANYWHERE],
        out_shape=[
            jax.ShapeDtypeStruct((parts, rows, LANES), f32),
            jax.ShapeDtypeStruct((rows, LANES), f32),
            jax.ShapeDtypeStruct(state.shape, f32),
        ],
        scratch_shapes=[
            pltpu.VMEM(state.shape, f32),
            pltpu.VMEM((seqs * 4 * heads, LANES), f32),
            pltpu.VMEM((2 * heads, LANES), f32),
            pltpu.VMEM((2 * heads, LANES), f32),
            pltpu.VMEM((2 * heads, LANES), f32),
            pltpu.VMEM((8, heads * HEAD), f32),
            pltpu.SemaphoreType.DMA((seqs * heads,)),
        ],
        compiler_params=small(),
        name="mixer",
    )(at, arrived, params, lower_bound, head_gain, state, weight)


def local(
    tokens,
    gate_weights,
    up_weights,
    down_weights,
    norm_gain,
    norm_bias,
    query_weight,
    forget_weight,
    input_weight,
    outgate_weight,
    lower_bound,
    head_gain,
    out_weight,
    state,
):
    batch, own_cols = tokens.shape
    heads = state.shape[1]
    kv_count, tp_count = lax.axis_size(KV), lax.axis_size(TP)
    x_count = tp_count // 2
    chip_count = kv_count * x_count
    half = batch // 2
    width = own_cols * kv_count * tp_count
    kv, tp, core = lax.axis_index(KV), lax.axis_index(TP), lax.axis_index(CORE)

    at = jnp.stack([kv, tp, core])
    blocks = placed_copies(at, tokens, norm_gain, norm_bias, tp_count)
    arrived, at, kv, tp, core, norm_gain, norm_bias = alone(
        blocks, TP, at, kv, tp, core, norm_gain, norm_bias
    )
    block = arrived.astype(f32).sum(axis=0).astype(bf16)
    own_half = lax.dynamic_slice_in_dim(block, core * half, half, 0)
    arrived = to_everyone(jnp.concatenate([own_half, block[batch:]]), KV, kv_count)
    both = lax.all_gather(arrived, CORE, axis=0)
    params = both[0, :, half:]

    def over_tp(lines, *held):
        gathered, *held = alone(copies(lines, tp_count), TP, *held)
        return gathered.reshape(x_count, 2, *lines.shape), *held

    weights = (query_weight, forget_weight, input_weight, outgate_weight)
    chunk_count = 4 * heads
    share = kv_count // chunk_count
    bias_rows, mixer_weight = prepare(block[batch:], weights, out_weight, tp_count)
    kept, sent, tail, token_sum = first_block(
        at, both, gate_weights, up_weights, down_weights, half
    )
    blocks = first_blocks(kept, lax.ppermute(sent, CORE, SWAP), tail, bias_rows)
    arrived, at, kv, tp, norm_gain, norm_bias, block, params, token_sum = alone(
        blocks, KV, at, kv, tp, norm_gain, norm_bias, block, params, token_sum
    )
    arrived = arrived.astype(f32).sum(axis=0)
    gathered, at, kv, tp, norm_gain, norm_bias, block, params, token_sum, arrived = over_tp(
        arrived, at, kv, tp, norm_gain, norm_bias, block, params, token_sum, arrived
    )
    bias_own = (arrived[half + 1 : half + 2] / share).astype(bf16)
    gain_one = block[batch : batch + 1]
    total = gathered[:, :, :half].sum(axis=0).reshape(batch, LANES)
    total_row = gathered[:, :, half].sum(axis=(0, 1))
    stream_one = residual_scale * block[:batch].astype(f32) + 0.5 * total
    row_mean = (
        residual_scale * token_sum[:, 0]
        + 0.5 * (total_row[:batch] + total_row[batch:])
    ) / width
    centred = stream_one - row_mean[:, None]

    scaled = (centred * gain_one.astype(f32)).astype(bf16)
    projected = jnp.concatenate(
        [jnp.dot(scaled, w, preferred_element_type=f32) for w in weights], axis=1
    ).astype(bf16)
    projected = projected.reshape(2, half, chunk_count, LANES).transpose(1, 2, 0, 3)
    blocks = jnp.concatenate(
        [
            projected.reshape(kv_count, 2 * chunk_count, LANES),
            centred.astype(bf16).reshape(2, half, LANES).swapaxes(0, 1),
            jnp.broadcast_to(bias_own[None], (kv_count, 6, LANES)),
        ],
        axis=1,
    )
    arrived, at, kv, tp, norm_gain, norm_bias, params = alone(
        blocks, KV, at, kv, tp, norm_gain, norm_bias, params
    )
    mixer_part, piece, updated = mixer(
        at,
        arrived,
        params,
        lower_bound.reshape(heads, HEAD),
        head_gain.reshape(heads, HEAD),
        state,
        mixer_weight,
    )
    arrived, at, tp, norm_gain, norm_bias, params, piece = alone(
        mixer_part, TP, at, tp, norm_gain, norm_bias, params, piece
    )
    stream_own = (piece + arrived.sum(axis=0)).astype(bf16)
    arrived, at, tp, norm_gain, norm_bias, params = alone(
        copies(stream_own, chip_count), CHIPS, at, tp, norm_gain, norm_bias, params
    )
    arrived = lax.all_gather(arrived, CORE, axis=0)
    arrived = arrived.reshape(2, kv_count, x_count, *stream_own.shape)

    kept, sent, own_normed = second_block(
        at, arrived, params, gate_weights, up_weights, down_weights
    )
    came = lax.ppermute(sent, CORE, SWAP)
    blocks = (kept.astype(f32) + came.astype(f32)).astype(bf16)
    arrived, tp, norm_gain, norm_bias, own_normed = alone(
        blocks, KV, tp, norm_gain, norm_bias, own_normed
    )
    gathered, tp, norm_gain, norm_bias, own_normed = over_tp(
        arrived.astype(f32).sum(axis=0), tp, norm_gain, norm_bias, own_normed
    )
    total = gathered.sum(axis=0).reshape(batch, LANES)
    stream_three = residual_scale * own_normed.astype(f32) + 0.5 * total
    block_sum = stream_three.sum(axis=1)
    block_mean = block_sum / LANES
    off = stream_three - block_mean[:, None]
    stats = jnp.concatenate([block_mean, (off * off).sum(axis=1)])[None]
    stats, tp, norm_gain, norm_bias, stream_three = alone(
        copies(stats, kv_count), KV, tp, norm_gain, norm_bias, stream_three
    )
    stats = stats[:, 0]
    means, squares = stats[:, :batch], stats[:, batch:]
    row_mean = means.mean(axis=0)
    spread = (squares.sum(axis=0) + LANES * ((means - row_mean) ** 2).sum(axis=0)) / width
    own = lax.dynamic_slice_in_dim(stream_three, tp * own_cols, own_cols, 1)
    mixed = (own - row_mean[:, None]) * lax.rsqrt(spread + norm_eps)[:, None] * norm_gain[
        2
    ].astype(f32) + norm_bias[2].astype(f32)
    mixed = mixed.reshape(2, half, own_cols).swapaxes(0, 1).reshape(batch, own_cols)
    return (mixed.astype(bf16), updated)


def solution(mesh):
    finer = Mesh(mesh.devices.reshape(8, 4, 4, 2), KV_TP)
    in_specs = (
        P(None, KV_TP),
        P(None, None, KV_TP),
        P(None, None, KV_TP),
        P(None, KV_TP, None),
        P(None, KV_TP),
        P(None, KV_TP),
        P(KV, TP),
        P(KV, TP),
        P(KV, TP),
        P(KV, TP),
        P(TP),
        P(TP),
        P(TP, None),
        P(KV, TP, None, None),
    )
    out_specs = (P(None, KV_TP), P(KV, TP, None, None))
    return jax.shard_map(local, mesh=finer, in_specs=in_specs, out_specs=out_specs, check_vma=False)
```

```python
import jax
import jax.numpy as jnp
from jax import lax
from jax.experimental import pallas as pl
from jax.experimental.pallas import tpu as pltpu
from jax.sharding import Mesh
from jax.sharding import PartitionSpec as P

HEAD = 128
LANES = 128
KV_TP = ("kv_0", "kv_1", "tp_0", "tp_1")
KV = ("kv_0", "kv_1")
TP = ("tp_0", "tp_1")
CHIPS = ("kv_0", "kv_1", "tp_0")
CORE = "tp_1"
SWAP = [(0, 1), (1, 0)]

residual_scale = 8.0**0.25
norm_eps = 1e-05
head_eps = 1e-06
bf16 = jnp.bfloat16
f32 = jnp.float32


def exchange(blocks, axes):
    return lax.all_to_all(blocks, axes, split_axis=0, concat_axis=0, tiled=True)


def to_everyone(block, axes, count):
    return exchange(jnp.broadcast_to(block[None], (count, *block.shape)), axes)


def alone(blocks, axes, *held):
    blocks, *held = lax.optimization_barrier((blocks, *held))
    return lax.optimization_barrier((exchange(blocks, axes), *held))


def copies(block, count):
    return jnp.broadcast_to(block[None], (count, *block.shape))


def small(grant=8):
    return pltpu.CompilerParams(vmem_limit_bytes=grant * 2**20)


VMEM = pl.BlockSpec(memory_space=pltpu.VMEM)
SMEM = pl.BlockSpec(memory_space=pltpu.SMEM)
ANYWHERE = pl.BlockSpec(memory_space=pl.ANY)


def off_chip(x):
    return pltpu.with_memory_space_constraint(x, pltpu.HBM)


def place_kernel(
    at_ref,
    tokens_hbm,
    gain_hbm,
    bias_hbm,
    result_ref,
    lines_ref,
    tokens_ref,
    gain_ref,
    bias_ref,
    sem,
):
    pairs = ((tokens_hbm, tokens_ref), (gain_hbm, gain_ref), (bias_hbm, bias_ref))
    fetches = [pltpu.make_async_copy(*pair, sem.at[i]) for i, pair in enumerate(pairs)]
    for fetch in fetches:
        fetch.start()
    own_cols, batch = tokens_ref.shape
    half = batch // 2
    shape = (own_cols, LANES)
    spot = lax.broadcasted_iota(jnp.int32, shape, 0) + at_ref[1] * own_cols
    place = (lax.broadcasted_iota(jnp.int32, shape, 1) == spot).astype(f32).astype(bf16)
    row = lax.broadcasted_iota(jnp.int32, (batch, batch), 0)
    source = 2 * (row % half) + row // half
    order = (lax.broadcasted_iota(jnp.int32, (batch, batch), 1) == source).astype(f32)
    for fetch in fetches:
        fetch.wait()
    turned = lax.dot_general(
        order.astype(bf16), tokens_ref[...], (((1,), (1,)), ((), ())), preferred_element_type=f32
    ).astype(bf16)
    lines_ref[batch:, :] = jnp.zeros((8, LANES), f32)
    lines_ref[:batch, :] = jnp.dot(turned, place, preferred_element_type=f32)
    lines_ref[batch : batch + 3, :] = jnp.dot(gain_ref[...], place, preferred_element_type=f32)
    lines_ref[batch + 3 : batch + 6, :] = jnp.dot(bias_ref[...], place, preferred_element_type=f32)
    lines = lines_ref[...].astype(bf16)
    for copy in range(result_ref.shape[0]):
        result_ref[copy] = lines


def placed_copies(at, tokens, gain, bias, count):
    batch, own_cols = tokens.shape
    return pl.pallas_call(
        place_kernel,
        in_specs=[SMEM] + [ANYWHERE] * 3,
        out_specs=VMEM,
        out_shape=jax.ShapeDtypeStruct((count, batch + 8, LANES), bf16),
        scratch_shapes=[
            pltpu.VMEM((batch + 8, LANES), f32),
            pltpu.VMEM((own_cols, batch), bf16),
            pltpu.VMEM(gain.shape, bf16),
            pltpu.VMEM(bias.shape, bf16),
            pltpu.SemaphoreType.DMA((3,)),
        ],
        compiler_params=small(),
        name="place",
    )(at, off_chip(tokens.T), off_chip(gain), off_chip(bias))


def load_kernel(
    lines_ref,
    hbm_0,
    hbm_1,
    hbm_2,
    hbm_3,
    out_hbm,
    gate_hbm,
    up_hbm,
    down_hbm,
    bias_ref,
    out_ref,
    gate_ref,
    up_ref,
    down_ref,
    project_ref,
    project_sem,
    part_sem,
    sem,
):
    parts, _, step = out_ref.shape
    pairs = ((gate_hbm, gate_ref), (up_hbm, up_ref), (down_hbm, down_ref))
    projections = [
        pltpu.make_async_copy(hbm, project_ref.at[i], project_sem.at[i])
        for i, hbm in enumerate((hbm_0, hbm_1, hbm_2, hbm_3))
    ]
    fetches = [pltpu.make_async_copy(*pair, sem.at[i]) for i, pair in enumerate(pairs)]
    fetches += [
        pltpu.make_async_copy(
            out_hbm.at[:, pl.ds(part * step, step)], out_ref.at[part], part_sem.at[part]
        )
        for part in range(parts)
    ]
    for fetch in projections + fetches:
        fetch.start()
    lines = lines_ref[...]
    for index, projection in enumerate(projections):
        projection.wait()
        sums = jnp.dot(lines, project_ref[index], preferred_element_type=f32)
        heads = sums.shape[1] // LANES
        for head in range(heads):
            chunk = index * heads + head
            bias_ref[chunk : chunk + 1, :] = sums[3:4, head * LANES : (head + 1) * LANES]
    for fetch in fetches:
        fetch.wait()


def load(lines, weights, out_weight, stored, parts):
    depth, width = out_weight.shape
    return pl.pallas_call(
        load_kernel,
        in_specs=[VMEM] + [ANYWHERE] * 8,
        out_specs=[VMEM] * 5,
        out_shape=[
            jax.ShapeDtypeStruct((4 * weights[0].shape[1] // LANES, LANES), f32),
            jax.ShapeDtypeStruct((parts, depth, width // parts), bf16),
        ]
        + [jax.ShapeDtypeStruct(w.shape, bf16) for w in stored],
        scratch_shapes=[
            pltpu.VMEM((4, *weights[0].shape), bf16),
            pltpu.SemaphoreType.DMA((4,)),
            pltpu.SemaphoreType.DMA((parts,)),
            pltpu.SemaphoreType.DMA((3,)),
        ],
        compiler_params=small(12),
        name="load",
    )(lines, *[off_chip(w) for w in (*weights, out_weight, *stored)])


def feed_forward(rows, core, layer, gate_ref, up_ref, down_ref):
    def stored(ref):
        return ref[...].reshape(ref.shape[0] * ref.shape[1], ref.shape[2])

    dims = (((1,), (1,)), ((), ()))
    gate = lax.dot_general(rows, stored(gate_ref), dims, preferred_element_type=f32)
    up = lax.dot_general(rows, stored(up_ref), dims, preferred_element_type=f32)
    hidden = jax.nn.silu(gate) * up
    unit = lax.broadcasted_iota(jnp.int32, hidden.shape, 1)
    hidden = jnp.where(unit % 2 == layer, hidden, 0.0)
    half = hidden.shape[0] // 2
    low, high = hidden[:half], hidden[half:]
    first = core == 0
    hidden = jnp.concatenate([jnp.where(first, low, high), jnp.where(first, high, low)])
    return jnp.dot(hidden.astype(bf16), stored(down_ref), preferred_element_type=f32)


def write_halves(part, kept_ref, sent_ref):
    chunks, half, _ = kept_ref.shape
    for chunk in range(chunks):
        at = slice(chunk * LANES, (chunk + 1) * LANES)
        kept_ref[chunk] = part[:half, at].astype(bf16)
        sent_ref[chunk] = part[half:, at].astype(bf16)


def first_kernel(
    at_ref, rows_ref, gate_ref, up_ref, down_ref, kept_ref, sent_ref, tail_ref, total_ref, x_ref
):
    chunks, half, _ = kept_ref.shape
    core = at_ref[2]
    for seq in range(2):
        at = slice(seq * half, (seq + 1) * half)
        total = jnp.zeros((half, LANES), f32)
        for chunk in range(chunks):
            lines = rows_ref[seq, chunk, :half, :]
            x_ref[at, chunk * LANES : (chunk + 1) * LANES] = lines
            total = total + lines.astype(f32)
        total_ref[at, :] = jnp.broadcast_to(jnp.sum(total, axis=1, keepdims=True), (half, LANES))
    part = feed_forward(x_ref[...], core, 0, gate_ref, up_ref, down_ref)
    write_halves(part, kept_ref, sent_ref)
    batch = 2 * half
    sums = jnp.broadcast_to(jnp.sum(part, axis=1, keepdims=True), (batch, LANES))
    row = (lax.broadcasted_iota(jnp.int32, (batch, LANES), 0) + core * half) % batch
    lane = lax.broadcasted_iota(jnp.int32, (batch, LANES), 1)
    line = jnp.sum(jnp.where(lane % batch == row, sums, 0.0), axis=0, keepdims=True)
    high = line.astype(bf16).astype(f32)
    line = jnp.where(lane[:1] < batch, high, line - high)
    tail_ref[...] = jnp.broadcast_to(line, tail_ref.shape)


def stored_order(gate, up, down):
    return gate.transpose(2, 0, 1), up.transpose(2, 0, 1), down.transpose(1, 0, 2)


def first_block(at, rows, stored, half):
    chunks = rows.shape[1]
    return pl.pallas_call(
        first_kernel,
        in_specs=[SMEM] + [VMEM] * 4,
        out_specs=[VMEM] * 4,
        out_shape=[
            jax.ShapeDtypeStruct((chunks, half, LANES), bf16),
            jax.ShapeDtypeStruct((chunks, half, LANES), bf16),
            jax.ShapeDtypeStruct((8, LANES), f32),
            jax.ShapeDtypeStruct((2 * half, LANES), f32),
        ],
        scratch_shapes=[pltpu.VMEM((2 * half, chunks * LANES), bf16)],
        compiler_params=small(12),
        name="first_block",
    )(at, rows, *stored)


def blocks_kernel(kept_ref, came_ref, tail_ref, bias_ref, result_ref):
    chunks, half, _ = kept_ref.shape
    share = chunks // bias_ref.shape[0]
    top = lax.broadcasted_iota(jnp.int32, (8, LANES), 0) == 0
    for chunk in range(chunks):
        both = kept_ref[chunk].astype(f32) + came_ref[chunk].astype(f32)
        result_ref[chunk, :half, :] = both.astype(bf16)
        bias = bias_ref[chunk // share : chunk // share + 1, :]
        result_ref[chunk, half:, :] = jnp.where(top, tail_ref[...], bias).astype(bf16)


def first_blocks(kept, came, tail, bias):
    chunks, half, lanes = kept.shape
    return pl.pallas_call(
        blocks_kernel,
        in_specs=[VMEM] * 4,
        out_specs=VMEM,
        out_shape=jax.ShapeDtypeStruct((chunks, half + 8, lanes), bf16),
        compiler_params=small(),
        name="first_blocks",
    )(kept, came, tail, bias)


def second_kernel(
    at_ref,
    arrived_ref,
    params_ref,
    gate_ref,
    up_ref,
    down_ref,
    kept_ref,
    sent_ref,
    own_ref,
    raw_ref,
    result_ref,
):
    cores, kv_count, x_count, rows, _ = arrived_ref.shape
    pieces = rows // 2
    chunks = cores * x_count * pieces
    for x in range(x_count):
        for core in range(cores):
            tiles = arrived_ref[core, :, x].astype(f32)
            raw_ref[x * cores + core] = tiles.reshape(kv_count * rows, LANES)

    def lines(chunk, seq):
        at = (chunk % pieces) * 2 + seq
        return raw_ref[chunk // pieces, pl.ds(at, kv_count, stride=rows), :]

    width = chunks * LANES
    for seq in range(2):
        total = sum(lines(chunk, seq) for chunk in range(chunks))
        mean = jnp.sum(total, axis=1, keepdims=True) / width
        squares = jnp.zeros((kv_count, LANES), f32)
        for chunk in range(chunks):
            off = lines(chunk, seq) - mean
            squares = squares + off * off
        spread = jnp.sum(squares, axis=1, keepdims=True) / width
        scale = lax.rsqrt(spread + norm_eps)
        for chunk in range(chunks):
            params = params_ref[chunk].astype(f32)
            normed = (lines(chunk, seq) - mean) * scale * params[1:2] + params[4:5]
            result_ref[
                seq * kv_count : (seq + 1) * kv_count, chunk * LANES : (chunk + 1) * LANES
            ] = normed.astype(bf16)
    own_ref[...] = result_ref[:, pl.ds(pl.multiple_of(at_ref[0] * LANES, LANES), LANES)]
    part = feed_forward(result_ref[...], at_ref[2], 1, gate_ref, up_ref, down_ref)
    write_halves(part, kept_ref, sent_ref)


def second_block(at, arrived, params, stored):
    cores, kv_count, x_count, rows, lanes = arrived.shape
    chunks = cores * x_count * rows // 2
    return pl.pallas_call(
        second_kernel,
        in_specs=[SMEM] + [VMEM] * 5,
        out_specs=[VMEM] * 3,
        out_shape=[
            jax.ShapeDtypeStruct((chunks, kv_count, lanes), bf16),
            jax.ShapeDtypeStruct((chunks, kv_count, lanes), bf16),
            jax.ShapeDtypeStruct((2 * kv_count, lanes), bf16),
        ],
        scratch_shapes=[
            pltpu.VMEM((cores * x_count, kv_count * rows, lanes), f32),
            pltpu.VMEM((2 * kv_count, chunks * lanes), bf16),
        ],
        compiler_params=small(12),
        name="second_block",
    )(at, arrived, params, *stored)


def mixer_kernel(
    at_ref,
    arrived_ref,
    params_ref,
    low_ref,
    head_gain_ref,
    state_ref,
    weight_ref,
    sent_ref,
    piece_ref,
    updated_hbm,
    updated_ref,
    rows_ref,
    low_rows_ref,
    gain_rows_ref,
    readout_ref,
    gated_ref,
    updated_sem,
):
    seqs, heads = state_ref.shape[:2]
    kv_count = arrived_ref.shape[0]
    chunks = 4 * heads
    share = kv_count // chunks
    parts = sent_ref.shape[0]
    piece_chunks = kv_count // parts
    total = arrived_ref[0].astype(f32)
    for block in range(1, kv_count):
        total = total + arrived_ref[block].astype(f32)
    tail = seqs * chunks
    width = kv_count * LANES
    mean = jnp.sum(total[tail : tail + 8], axis=1, keepdims=True) / width
    squares = jnp.zeros((8, LANES), f32)
    for block in range(kv_count):
        off = arrived_ref[block, tail : tail + 8, :].astype(f32) - mean
        squares = squares + off * off
    scale = lax.rsqrt(jnp.sum(squares, axis=1, keepdims=True) / width + norm_eps)
    for chunk in range(chunks):
        bias = arrived_ref[chunk * share, tail : tail + 8, :].astype(f32)
        for other in range(1, share):
            bias = bias + arrived_ref[chunk * share + other, tail : tail + 8, :].astype(f32)
        rows_ref[2 * chunk : 2 * chunk + 2, :] = jnp.broadcast_to(bias[2:3], (2, LANES))
    odd = lax.broadcasted_iota(jnp.int32, (tail, LANES), 0) % 2 == 1
    row_scale = jnp.where(odd, scale[1:2], scale[0:1])
    pre = (total[:tail] * row_scale + rows_ref[...]).astype(bf16).astype(f32)
    size = 2 * heads
    query_pre, forget_pre = pre[:size], pre[size : 2 * size]
    input_pre, outgate_pre = pre[2 * size : 3 * size], pre[3 * size :]

    tp = at_ref[1]
    for chunk in range(piece_chunks):
        at = tp * piece_chunks + chunk
        rows = arrived_ref[at, tail : tail + 8, :].astype(f32)
        params = params_ref[at].astype(f32)
        rows = ((rows - mean) * scale * params[0:1] + params[3:4]).astype(bf16).astype(f32)
        piece_ref[2 * chunk : 2 * chunk + 2, :] = residual_scale * rows[0:2]

    for head in range(heads):
        at = slice(2 * head, 2 * head + 2)
        low_rows_ref[at, :] = jnp.broadcast_to(low_ref[head : head + 1, :], (2, LANES))
        gain_rows_ref[at, :] = jnp.broadcast_to(head_gain_ref[head : head + 1, :], (2, LANES))
    low = low_rows_ref[...]
    forget = (low + (1.0 - low) * jax.nn.sigmoid(forget_pre)).T
    key = ((1.0 - low) * jax.nn.sigmoid(-forget_pre)).T
    query = jax.nn.silu(query_pre).T
    updated_copies = []
    for head in range(heads):
        for seq in range(seqs):
            row = head * 2 + seq
            new = (
                forget[:, row : row + 1] * state_ref[seq, head]
                + key[:, row : row + 1] * input_pre[row : row + 1, :]
            )
            updated_ref[seq, head] = new
            updated_copies.append(
                pltpu.make_async_copy(
                    updated_ref.at[seq, head], updated_hbm.at[seq, head], updated_sem.at[row]
                )
            )
            updated_copies[-1].start()
            readout_ref[row : row + 1, :] = jnp.sum(
                query[:, row : row + 1] * new, axis=0, keepdims=True
            )
    readout = readout_ref[...]
    readout = readout * lax.rsqrt(jnp.mean(readout * readout, axis=1, keepdims=True) + head_eps)
    gated = readout * gain_rows_ref[...] * jax.nn.silu(outgate_pre)
    gated_ref[...] = jnp.zeros(gated_ref.shape, f32)
    for head in range(heads):
        gated_ref[0:2, head * HEAD : (head + 1) * HEAD] = gated[2 * head : 2 * head + 2]
    lhs = gated_ref[...].astype(bf16)
    for part in range(parts):
        mixed = jnp.dot(lhs, weight_ref[part], preferred_element_type=f32)
        for chunk in range(piece_chunks):
            sent_ref[part, 2 * chunk : 2 * chunk + 2, :] = mixed[
                0:2, chunk * LANES : (chunk + 1) * LANES
            ]
    for copy in updated_copies:
        copy.wait()


def mixer(at, arrived, params, lower_bound, head_gain, state, weight):
    seqs, heads = state.shape[:2]
    parts, _, step = weight.shape
    rows = 2 * step // LANES
    return pl.pallas_call(
        mixer_kernel,
        in_specs=[SMEM] + [VMEM] * 6,
        out_specs=[VMEM, VMEM, ANYWHERE],
        out_shape=[
            jax.ShapeDtypeStruct((parts, rows, LANES), f32),
            jax.ShapeDtypeStruct((rows, LANES), f32),
            jax.ShapeDtypeStruct(state.shape, f32),
        ],
        scratch_shapes=[
            pltpu.VMEM(state.shape, f32),
            pltpu.VMEM((seqs * 4 * heads, LANES), f32),
            pltpu.VMEM((2 * heads, LANES), f32),
            pltpu.VMEM((2 * heads, LANES), f32),
            pltpu.VMEM((2 * heads, LANES), f32),
            pltpu.VMEM((8, heads * HEAD), f32),
            pltpu.SemaphoreType.DMA((seqs * heads,)),
        ],
        compiler_params=small(),
        name="mixer",
    )(at, arrived, params, lower_bound, head_gain, state, weight)


def local(
    tokens,
    gate_weights,
    up_weights,
    down_weights,
    norm_gain,
    norm_bias,
    query_weight,
    forget_weight,
    input_weight,
    outgate_weight,
    lower_bound,
    head_gain,
    out_weight,
    state,
):
    batch, own_cols = tokens.shape
    heads = state.shape[1]
    kv_count, tp_count = lax.axis_size(KV), lax.axis_size(TP)
    x_count = tp_count // 2
    chip_count = kv_count * x_count
    half = batch // 2
    width = own_cols * kv_count * tp_count
    kv, tp, core = lax.axis_index(KV), lax.axis_index(TP), lax.axis_index(CORE)

    at = jnp.stack([kv, tp, core])
    blocks = placed_copies(at, tokens, norm_gain, norm_bias, tp_count)
    arrived, at, kv, tp, core, norm_gain, norm_bias = alone(
        blocks, TP, at, kv, tp, core, norm_gain, norm_bias
    )
    block = arrived.astype(f32).sum(axis=0).astype(bf16)
    own_half = lax.dynamic_slice_in_dim(block, core * half, half, 0)
    arrived = to_everyone(jnp.concatenate([own_half, block[batch:]]), KV, kv_count)
    both = lax.all_gather(arrived, CORE, axis=0)
    params = both[0, :, half:]

    def over_tp(lines, *held):
        gathered, *held = alone(copies(lines, tp_count), TP, *held)
        return gathered.reshape(x_count, 2, *lines.shape), *held

    weights = (query_weight, forget_weight, input_weight, outgate_weight)
    chunk_count = 4 * heads
    share = kv_count // chunk_count
    stored = stored_order(gate_weights, up_weights, down_weights)
    bias_rows, mixer_weight, *stored = load(
        block[batch:], weights, out_weight, stored, tp_count
    )
    kept, sent, tail, token_sum = first_block(at, both, stored, half)
    blocks = first_blocks(kept, lax.ppermute(sent, CORE, SWAP), tail, bias_rows)
    arrived, at, kv, tp, norm_gain, norm_bias, block, params, token_sum = alone(
        blocks, KV, at, kv, tp, norm_gain, norm_bias, block, params, token_sum
    )
    arrived = arrived.astype(f32).sum(axis=0)
    gathered, at, kv, tp, norm_gain, norm_bias, block, params, token_sum, arrived = over_tp(
        arrived, at, kv, tp, norm_gain, norm_bias, block, params, token_sum, arrived
    )
    bias_own = (arrived[half + 1 : half + 2] / share).astype(bf16)
    gain_one = block[batch : batch + 1]
    total = gathered[:, :, :half].sum(axis=0).reshape(batch, LANES)
    total_row = gathered[:, :, half].sum(axis=(0, 1))
    stream_one = residual_scale * block[:batch].astype(f32) + 0.5 * total
    row_mean = (
        residual_scale * token_sum[:, 0]
        + 0.5 * (total_row[:batch] + total_row[batch:])
    ) / width
    centred = stream_one - row_mean[:, None]

    scaled = (centred * gain_one.astype(f32)).astype(bf16)
    projected = jnp.concatenate(
        [jnp.dot(scaled, w, preferred_element_type=f32) for w in weights], axis=1
    ).astype(bf16)
    projected = projected.reshape(2, half, chunk_count, LANES).transpose(1, 2, 0, 3)
    blocks = jnp.concatenate(
        [
            projected.reshape(kv_count, 2 * chunk_count, LANES),
            centred.astype(bf16).reshape(2, half, LANES).swapaxes(0, 1),
            jnp.broadcast_to(bias_own[None], (kv_count, 6, LANES)),
        ],
        axis=1,
    )
    arrived, at, kv, tp, norm_gain, norm_bias, params = alone(
        blocks, KV, at, kv, tp, norm_gain, norm_bias, params
    )
    mixer_part, piece, updated = mixer(
        at,
        arrived,
        params,
        lower_bound.reshape(heads, HEAD),
        head_gain.reshape(heads, HEAD),
        state,
        mixer_weight,
    )
    arrived, at, tp, norm_gain, norm_bias, params, piece = alone(
        mixer_part, TP, at, tp, norm_gain, norm_bias, params, piece
    )
    stream_own = (piece + arrived.sum(axis=0)).astype(bf16)
    arrived, at, tp, norm_gain, norm_bias, params = alone(
        copies(stream_own, chip_count), CHIPS, at, tp, norm_gain, norm_bias, params
    )
    arrived = lax.all_gather(arrived, CORE, axis=0)
    arrived = arrived.reshape(2, kv_count, x_count, *stream_own.shape)

    kept, sent, own_normed = second_block(at, arrived, params, stored)
    came = lax.ppermute(sent, CORE, SWAP)
    blocks = (kept.astype(f32) + came.astype(f32)).astype(bf16)
    arrived, tp, norm_gain, norm_bias, own_normed = alone(
        blocks, KV, tp, norm_gain, norm_bias, own_normed
    )
    gathered, tp, norm_gain, norm_bias, own_normed = over_tp(
        arrived.astype(f32).sum(axis=0), tp, norm_gain, norm_bias, own_normed
    )
    total = gathered.sum(axis=0).reshape(batch, LANES)
    stream_three = residual_scale * own_normed.astype(f32) + 0.5 * total
    block_sum = stream_three.sum(axis=1)
    block_mean = block_sum / LANES
    off = stream_three - block_mean[:, None]
    stats = jnp.concatenate([block_mean, (off * off).sum(axis=1)])[None]
    stats, tp, norm_gain, norm_bias, stream_three = alone(
        copies(stats, kv_count), KV, tp, norm_gain, norm_bias, stream_three
    )
    stats = stats[:, 0]
    means, squares = stats[:, :batch], stats[:, batch:]
    row_mean = means.mean(axis=0)
    spread = (squares.sum(axis=0) + LANES * ((means - row_mean) ** 2).sum(axis=0)) / width
    own = lax.dynamic_slice_in_dim(stream_three, tp * own_cols, own_cols, 1)
    mixed = (own - row_mean[:, None]) * lax.rsqrt(spread + norm_eps)[:, None] * norm_gain[
        2
    ].astype(f32) + norm_bias[2].astype(f32)
    mixed = mixed.reshape(2, half, own_cols).swapaxes(0, 1).reshape(batch, own_cols)
    return (mixed.astype(bf16), updated)


def solution(mesh):
    finer = Mesh(mesh.devices.reshape(8, 4, 4, 2), KV_TP)
    in_specs = (
        P(None, KV_TP),
        P(None, None, KV_TP),
        P(None, None, KV_TP),
        P(None, KV_TP, None),
        P(None, KV_TP),
        P(None, KV_TP),
        P(KV, TP),
        P(KV, TP),
        P(KV, TP),
        P(KV, TP),
        P(TP),
        P(TP),
        P(TP, None),
        P(KV, TP, None, None),
    )
    out_specs = (P(None, KV_TP), P(KV, TP, None, None))
    return jax.shard_map(local, mesh=finer, in_specs=in_specs, out_specs=out_specs, check_vma=False)
```

```python
import jax
import jax.numpy as jnp
from jax import lax
from jax.experimental import pallas as pl
from jax.experimental.pallas import tpu as pltpu
from jax.sharding import Mesh
from jax.sharding import PartitionSpec as P

HEAD = 128
LANES = 128
KV_TP = ("kv_0", "kv_1", "tp_0", "tp_1")
KV = ("kv_0", "kv_1")
TP = ("tp_0", "tp_1")
CHIPS = ("kv_0", "kv_1", "tp_0")
CORE = "tp_1"
SWAP = [(0, 1), (1, 0)]

residual_scale = 8.0**0.25
norm_eps = 1e-05
head_eps = 1e-06
bf16 = jnp.bfloat16
f32 = jnp.float32


def exchange(blocks, axes):
    return lax.all_to_all(blocks, axes, split_axis=0, concat_axis=0, tiled=True)


def to_everyone(block, axes, count):
    return exchange(jnp.broadcast_to(block[None], (count, *block.shape)), axes)


def alone(blocks, axes, *held):
    blocks, *held = lax.optimization_barrier((blocks, *held))
    return lax.optimization_barrier((exchange(blocks, axes), *held))


def wide_sum(blocks):
    return lax.optimization_barrier(blocks.astype(f32).sum(axis=0))


def copies(block, count):
    return jnp.broadcast_to(block[None], (count, *block.shape))


def small(grant=8):
    return pltpu.CompilerParams(vmem_limit_bytes=grant * 2**20)


VMEM = pl.BlockSpec(memory_space=pltpu.VMEM)
SMEM = pl.BlockSpec(memory_space=pltpu.SMEM)
ANYWHERE = pl.BlockSpec(memory_space=pl.ANY)


def off_chip(x):
    return pltpu.with_memory_space_constraint(x, pltpu.HBM)


def place_kernel(
    at_ref,
    tokens_hbm,
    gain_hbm,
    bias_hbm,
    result_ref,
    lines_ref,
    tokens_ref,
    gain_ref,
    bias_ref,
    sem,
):
    pairs = ((tokens_hbm, tokens_ref), (gain_hbm, gain_ref), (bias_hbm, bias_ref))
    fetches = [pltpu.make_async_copy(*pair, sem.at[i]) for i, pair in enumerate(pairs)]
    for fetch in fetches:
        fetch.start()
    own_cols, batch = tokens_ref.shape
    half = batch // 2
    shape = (own_cols, LANES)
    spot = lax.broadcasted_iota(jnp.int32, shape, 0) + at_ref[1] * own_cols
    place = (lax.broadcasted_iota(jnp.int32, shape, 1) == spot).astype(f32).astype(bf16)
    row = lax.broadcasted_iota(jnp.int32, (batch, batch), 0)
    source = 2 * (row % half) + row // half
    order = (lax.broadcasted_iota(jnp.int32, (batch, batch), 1) == source).astype(f32)
    for fetch in fetches:
        fetch.wait()
    turned = lax.dot_general(
        order.astype(bf16), tokens_ref[...], (((1,), (1,)), ((), ())), preferred_element_type=f32
    ).astype(bf16)
    lines_ref[batch:, :] = jnp.zeros((8, LANES), f32)
    lines_ref[:batch, :] = jnp.dot(turned, place, preferred_element_type=f32)
    lines_ref[batch : batch + 3, :] = jnp.dot(gain_ref[...], place, preferred_element_type=f32)
    lines_ref[batch + 3 : batch + 6, :] = jnp.dot(bias_ref[...], place, preferred_element_type=f32)
    lines = lines_ref[...].astype(bf16)
    for copy in range(result_ref.shape[0]):
        result_ref[copy] = lines


def placed_copies(at, tokens, gain, bias, count):
    batch, own_cols = tokens.shape
    return pl.pallas_call(
        place_kernel,
        in_specs=[SMEM] + [ANYWHERE] * 3,
        out_specs=VMEM,
        out_shape=jax.ShapeDtypeStruct((count, batch + 8, LANES), bf16),
        scratch_shapes=[
            pltpu.VMEM((batch + 8, LANES), f32),
            pltpu.VMEM((own_cols, batch), bf16),
            pltpu.VMEM(gain.shape, bf16),
            pltpu.VMEM(bias.shape, bf16),
            pltpu.SemaphoreType.DMA((3,)),
        ],
        compiler_params=small(),
        name="place",
    )(at, off_chip(tokens.T), off_chip(gain), off_chip(bias))


def load_kernel(
    lines_ref,
    hbm_0,
    hbm_1,
    hbm_2,
    hbm_3,
    out_hbm,
    gate_hbm,
    up_hbm,
    down_hbm,
    bias_ref,
    out_ref,
    gate_ref,
    up_ref,
    down_ref,
    project_ref,
    project_sem,
    part_sem,
    sem,
):
    parts, _, step = out_ref.shape
    pairs = ((gate_hbm, gate_ref), (up_hbm, up_ref), (down_hbm, down_ref))
    projections = [
        pltpu.make_async_copy(hbm, project_ref.at[i], project_sem.at[i])
        for i, hbm in enumerate((hbm_0, hbm_1, hbm_2, hbm_3))
    ]
    fetches = [pltpu.make_async_copy(*pair, sem.at[i]) for i, pair in enumerate(pairs)]
    fetches += [
        pltpu.make_async_copy(
            out_hbm.at[:, pl.ds(part * step, step)], out_ref.at[part], part_sem.at[part]
        )
        for part in range(parts)
    ]
    for fetch in projections + fetches:
        fetch.start()
    lines = lines_ref[...]
    for index, projection in enumerate(projections):
        projection.wait()
        sums = jnp.dot(lines, project_ref[index], preferred_element_type=f32)
        heads = sums.shape[1] // LANES
        for head in range(heads):
            chunk = index * heads + head
            bias_ref[chunk : chunk + 1, :] = sums[3:4, head * LANES : (head + 1) * LANES]
    for fetch in fetches:
        fetch.wait()


def load(lines, weights, out_weight, stored, parts):
    depth, width = out_weight.shape
    return pl.pallas_call(
        load_kernel,
        in_specs=[VMEM] + [ANYWHERE] * 8,
        out_specs=[VMEM] * 5,
        out_shape=[
            jax.ShapeDtypeStruct((4 * weights[0].shape[1] // LANES, LANES), f32),
            jax.ShapeDtypeStruct((parts, depth, width // parts), bf16),
        ]
        + [jax.ShapeDtypeStruct(w.shape, bf16) for w in stored],
        scratch_shapes=[
            pltpu.VMEM((4, *weights[0].shape), bf16),
            pltpu.SemaphoreType.DMA((4,)),
            pltpu.SemaphoreType.DMA((parts,)),
            pltpu.SemaphoreType.DMA((3,)),
        ],
        compiler_params=small(12),
        name="load",
    )(lines, *[off_chip(w) for w in (*weights, out_weight, *stored)])


def feed_forward(rows, core, layer, gate_ref, up_ref, down_ref):
    def stored(ref):
        return ref[...].reshape(ref.shape[0] * ref.shape[1], ref.shape[2])

    dims = (((1,), (1,)), ((), ()))
    gate = lax.dot_general(rows, stored(gate_ref), dims, preferred_element_type=f32)
    up = lax.dot_general(rows, stored(up_ref), dims, preferred_element_type=f32)
    hidden = jax.nn.silu(gate) * up
    unit = lax.broadcasted_iota(jnp.int32, hidden.shape, 1)
    hidden = jnp.where(unit % 2 == layer, hidden, 0.0)
    half = hidden.shape[0] // 2
    low, high = hidden[:half], hidden[half:]
    first = core == 0
    hidden = jnp.concatenate([jnp.where(first, low, high), jnp.where(first, high, low)])
    return jnp.dot(hidden.astype(bf16), stored(down_ref), preferred_element_type=f32)


def write_halves(part, kept_ref, sent_ref):
    chunks, half, _ = kept_ref.shape
    for chunk in range(chunks):
        at = slice(chunk * LANES, (chunk + 1) * LANES)
        kept_ref[chunk] = part[:half, at].astype(bf16)
        sent_ref[chunk] = part[half:, at].astype(bf16)


def first_kernel(
    at_ref, rows_ref, gate_ref, up_ref, down_ref, kept_ref, sent_ref, tail_ref, total_ref, x_ref
):
    chunks, half, _ = kept_ref.shape
    core = at_ref[2]
    for seq in range(2):
        at = slice(seq * half, (seq + 1) * half)
        total = jnp.zeros((half, LANES), f32)
        for chunk in range(chunks):
            lines = rows_ref[seq, chunk, :half, :]
            x_ref[at, chunk * LANES : (chunk + 1) * LANES] = lines
            total = total + lines.astype(f32)
        total_ref[at, :] = jnp.broadcast_to(jnp.sum(total, axis=1, keepdims=True), (half, LANES))
    part = feed_forward(x_ref[...], core, 0, gate_ref, up_ref, down_ref)
    write_halves(part, kept_ref, sent_ref)
    batch = 2 * half
    sums = jnp.broadcast_to(jnp.sum(part, axis=1, keepdims=True), (batch, LANES))
    row = (lax.broadcasted_iota(jnp.int32, (batch, LANES), 0) + core * half) % batch
    lane = lax.broadcasted_iota(jnp.int32, (batch, LANES), 1)
    line = jnp.sum(jnp.where(lane % batch == row, sums, 0.0), axis=0, keepdims=True)
    high = line.astype(bf16).astype(f32)
    line = jnp.where(lane[:1] < batch, high, line - high)
    tail_ref[...] = jnp.broadcast_to(line, tail_ref.shape)


def stored_order(gate, up, down):
    return gate.transpose(2, 0, 1), up.transpose(2, 0, 1), down.transpose(1, 0, 2)


def first_block(at, rows, stored, half):
    chunks = rows.shape[1]
    return pl.pallas_call(
        first_kernel,
        in_specs=[SMEM] + [VMEM] * 4,
        out_specs=[VMEM] * 4,
        out_shape=[
            jax.ShapeDtypeStruct((chunks, half, LANES), bf16),
            jax.ShapeDtypeStruct((chunks, half, LANES), bf16),
            jax.ShapeDtypeStruct((8, LANES), f32),
            jax.ShapeDtypeStruct((2 * half, LANES), f32),
        ],
        scratch_shapes=[pltpu.VMEM((2 * half, chunks * LANES), bf16)],
        compiler_params=small(12),
        name="first_block",
    )(at, rows, *stored)


def blocks_kernel(kept_ref, came_ref, tail_ref, bias_ref, result_ref):
    chunks, half, _ = kept_ref.shape
    share = chunks // bias_ref.shape[0]
    top = lax.broadcasted_iota(jnp.int32, (8, LANES), 0) == 0
    for chunk in range(chunks):
        both = kept_ref[chunk].astype(f32) + came_ref[chunk].astype(f32)
        bias = bias_ref[chunk // share : chunk // share + 1, :]
        tail = jnp.where(top, tail_ref[...], bias)
        lines = jnp.concatenate([both, tail]).astype(bf16)
        pairs = lines.reshape(lines.shape[0] // 2, 2, LANES)
        result_ref[chunk] = pairs[: result_ref.shape[1]]


def first_blocks(kept, came, tail, bias):
    chunks, half, lanes = kept.shape
    return pl.pallas_call(
        blocks_kernel,
        in_specs=[VMEM] * 4,
        out_specs=VMEM,
        out_shape=jax.ShapeDtypeStruct((chunks, half // 2 + 1, 2, lanes), bf16),
        compiler_params=small(),
        name="first_blocks",
    )(kept, came, tail, bias)


def second_kernel(
    at_ref,
    arrived_ref,
    params_ref,
    gate_ref,
    up_ref,
    down_ref,
    kept_ref,
    sent_ref,
    own_ref,
    raw_ref,
    result_ref,
):
    cores, kv_count, x_count, rows, _ = arrived_ref.shape
    pieces = rows // 2
    chunks = cores * x_count * pieces
    for x in range(x_count):
        for core in range(cores):
            tiles = arrived_ref[core, :, x].astype(f32)
            raw_ref[x * cores + core] = tiles.reshape(kv_count * rows, LANES)

    def lines(chunk, seq):
        at = (chunk % pieces) * 2 + seq
        return raw_ref[chunk // pieces, pl.ds(at, kv_count, stride=rows), :]

    width = chunks * LANES
    for seq in range(2):
        total = sum(lines(chunk, seq) for chunk in range(chunks))
        mean = jnp.sum(total, axis=1, keepdims=True) / width
        squares = jnp.zeros((kv_count, LANES), f32)
        for chunk in range(chunks):
            off = lines(chunk, seq) - mean
            squares = squares + off * off
        spread = jnp.sum(squares, axis=1, keepdims=True) / width
        scale = lax.rsqrt(spread + norm_eps)
        for chunk in range(chunks):
            params = params_ref[chunk].astype(f32)
            normed = (lines(chunk, seq) - mean) * scale * params[1:2] + params[4:5]
            result_ref[
                seq * kv_count : (seq + 1) * kv_count, chunk * LANES : (chunk + 1) * LANES
            ] = normed.astype(bf16)
    own_ref[...] = result_ref[:, pl.ds(pl.multiple_of(at_ref[0] * LANES, LANES), LANES)]
    part = feed_forward(result_ref[...], at_ref[2], 1, gate_ref, up_ref, down_ref)
    write_halves(part, kept_ref, sent_ref)


def second_block(at, arrived, params, stored):
    cores, kv_count, x_count, rows, lanes = arrived.shape
    chunks = cores * x_count * rows // 2
    return pl.pallas_call(
        second_kernel,
        in_specs=[SMEM] + [VMEM] * 5,
        out_specs=[VMEM] * 3,
        out_shape=[
            jax.ShapeDtypeStruct((chunks, kv_count, lanes), bf16),
            jax.ShapeDtypeStruct((chunks, kv_count, lanes), bf16),
            jax.ShapeDtypeStruct((2 * kv_count, lanes), bf16),
        ],
        scratch_shapes=[
            pltpu.VMEM((cores * x_count, kv_count * rows, lanes), f32),
            pltpu.VMEM((2 * kv_count, chunks * lanes), bf16),
        ],
        compiler_params=small(12),
        name="second_block",
    )(at, arrived, params, *stored)


def mixer_kernel(
    at_ref,
    arrived_ref,
    params_ref,
    low_ref,
    head_gain_ref,
    state_ref,
    weight_ref,
    sent_ref,
    piece_ref,
    updated_hbm,
    updated_ref,
    rows_ref,
    low_rows_ref,
    gain_rows_ref,
    readout_ref,
    gated_ref,
    updated_sem,
):
    seqs, heads = state_ref.shape[:2]
    kv_count = arrived_ref.shape[0]
    chunks = 4 * heads
    share = kv_count // chunks
    parts = sent_ref.shape[0]
    piece_chunks = kv_count // parts
    def block_rows(block):
        lines = arrived_ref[block, :chunks]
        return lines.reshape(seqs * chunks, LANES).astype(f32)

    total = block_rows(0)
    for block in range(1, kv_count):
        total = total + block_rows(block)
    tail = seqs * chunks
    width = kv_count * LANES
    own = arrived_ref[:, chunks].astype(f32)
    mean = jnp.sum(jnp.sum(own, axis=0), axis=1, keepdims=True) / width
    off = own - mean
    scale = jnp.sum(jnp.sum(off * off, axis=0), axis=1, keepdims=True) / width
    scale = lax.rsqrt(scale + norm_eps)
    for chunk in range(chunks):
        bias = arrived_ref[chunk * share, chunks + 1].astype(f32)
        for other in range(1, share):
            bias = bias + arrived_ref[chunk * share + other, chunks + 1].astype(f32)
        rows_ref[2 * chunk : 2 * chunk + 2, :] = bias
    odd = lax.broadcasted_iota(jnp.int32, (tail, LANES), 0) % 2 == 1
    row_scale = jnp.where(odd, scale[1:2], scale[0:1])
    pre = (total * row_scale + rows_ref[...]).astype(bf16).astype(f32)
    size = 2 * heads
    query_pre, forget_pre = pre[:size], pre[size : 2 * size]
    input_pre, outgate_pre = pre[2 * size : 3 * size], pre[3 * size :]

    tp = at_ref[1]
    for chunk in range(piece_chunks):
        at = tp * piece_chunks + chunk
        rows = arrived_ref[at, chunks].astype(f32)
        params = params_ref[at].astype(f32)
        rows = ((rows - mean) * scale * params[0:1] + params[3:4]).astype(bf16).astype(f32)
        piece_ref[2 * chunk : 2 * chunk + 2, :] = residual_scale * rows

    for head in range(heads):
        at = slice(2 * head, 2 * head + 2)
        low_rows_ref[at, :] = jnp.broadcast_to(low_ref[head : head + 1, :], (2, LANES))
        gain_rows_ref[at, :] = jnp.broadcast_to(head_gain_ref[head : head + 1, :], (2, LANES))
    low = low_rows_ref[...]
    forget = (low + (1.0 - low) * jax.nn.sigmoid(forget_pre)).T
    key = ((1.0 - low) * jax.nn.sigmoid(-forget_pre)).T
    query = jax.nn.silu(query_pre).T
    updated_copies = []
    for head in range(heads):
        for seq in range(seqs):
            row = head * 2 + seq
            new = (
                forget[:, row : row + 1] * state_ref[seq, head]
                + key[:, row : row + 1] * input_pre[row : row + 1, :]
            )
            updated_ref[seq, head] = new
            updated_copies.append(
                pltpu.make_async_copy(
                    updated_ref.at[seq, head], updated_hbm.at[seq, head], updated_sem.at[row]
                )
            )
            updated_copies[-1].start()
            readout_ref[row : row + 1, :] = jnp.sum(
                query[:, row : row + 1] * new, axis=0, keepdims=True
            )
    readout = readout_ref[...]
    readout = readout * lax.rsqrt(jnp.mean(readout * readout, axis=1, keepdims=True) + head_eps)
    gated = readout * gain_rows_ref[...] * jax.nn.silu(outgate_pre)
    gated_ref[...] = jnp.zeros(gated_ref.shape, f32)
    for head in range(heads):
        gated_ref[0:2, head * HEAD : (head + 1) * HEAD] = gated[2 * head : 2 * head + 2]
    lhs = gated_ref[...].astype(bf16)
    for part in range(parts):
        mixed = jnp.dot(lhs, weight_ref[part], preferred_element_type=f32)
        for chunk in range(piece_chunks):
            sent_ref[part, 2 * chunk : 2 * chunk + 2, :] = mixed[
                0:2, chunk * LANES : (chunk + 1) * LANES
            ]
    for copy in updated_copies:
        copy.wait()


def mixer(at, arrived, params, lower_bound, head_gain, state, weight):
    seqs, heads = state.shape[:2]
    parts, _, step = weight.shape
    rows = 2 * step // LANES
    return pl.pallas_call(
        mixer_kernel,
        in_specs=[SMEM] + [VMEM] * 6,
        out_specs=[VMEM, VMEM, ANYWHERE],
        out_shape=[
            jax.ShapeDtypeStruct((parts, rows, LANES), f32),
            jax.ShapeDtypeStruct((rows, LANES), f32),
            jax.ShapeDtypeStruct(state.shape, f32),
        ],
        scratch_shapes=[
            pltpu.VMEM(state.shape, f32),
            pltpu.VMEM((seqs * 4 * heads, LANES), f32),
            pltpu.VMEM((2 * heads, LANES), f32),
            pltpu.VMEM((2 * heads, LANES), f32),
            pltpu.VMEM((2 * heads, LANES), f32),
            pltpu.VMEM((8, heads * HEAD), f32),
            pltpu.SemaphoreType.DMA((seqs * heads,)),
        ],
        compiler_params=small(),
        name="mixer",
    )(at, arrived, params, lower_bound, head_gain, state, weight)


def local(
    tokens,
    gate_weights,
    up_weights,
    down_weights,
    norm_gain,
    norm_bias,
    query_weight,
    forget_weight,
    input_weight,
    outgate_weight,
    lower_bound,
    head_gain,
    out_weight,
    state,
):
    batch, own_cols = tokens.shape
    heads = state.shape[1]
    kv_count, tp_count = lax.axis_size(KV), lax.axis_size(TP)
    x_count = tp_count // 2
    chip_count = kv_count * x_count
    half = batch // 2
    width = own_cols * kv_count * tp_count
    kv, tp, core = lax.axis_index(KV), lax.axis_index(TP), lax.axis_index(CORE)

    at = jnp.stack([kv, tp, core])
    blocks = placed_copies(at, tokens, norm_gain, norm_bias, tp_count)
    arrived, at, kv, tp, core, norm_gain, norm_bias = alone(
        blocks, TP, at, kv, tp, core, norm_gain, norm_bias
    )
    block = arrived.astype(f32).sum(axis=0).astype(bf16)
    own_half = lax.dynamic_slice_in_dim(block, core * half, half, 0)
    arrived = to_everyone(jnp.concatenate([own_half, block[batch:]]), KV, kv_count)
    both = lax.all_gather(arrived, CORE, axis=0)
    params = both[0, :, half:]

    def over_tp(lines, *held):
        gathered, *held = alone(copies(lines, tp_count), TP, *held)
        return gathered.reshape(x_count, 2, *lines.shape), *held

    weights = (query_weight, forget_weight, input_weight, outgate_weight)
    chunk_count = 4 * heads
    share = kv_count // chunk_count
    stored = stored_order(gate_weights, up_weights, down_weights)
    bias_rows, mixer_weight, *stored = load(
        block[batch:], weights, out_weight, stored, tp_count
    )
    kept, sent, tail, token_sum = first_block(at, both, stored, half)
    blocks = first_blocks(kept, lax.ppermute(sent, CORE, SWAP), tail, bias_rows)
    arrived, at, kv, tp, norm_gain, norm_bias, block, params, token_sum = alone(
        blocks, KV, at, kv, tp, norm_gain, norm_bias, block, params, token_sum
    )
    arrived = wide_sum(arrived).reshape(half + 2, LANES).astype(bf16)
    gathered, at, kv, tp, norm_gain, norm_bias, block, params, token_sum, arrived = over_tp(
        arrived, at, kv, tp, norm_gain, norm_bias, block, params, token_sum, arrived
    )
    gathered = gathered.astype(f32)
    bias_own = arrived[half + 1 : half + 2] / share
    gain_one = block[batch : batch + 1]
    total = gathered[:, :, :half].sum(axis=0).reshape(batch, LANES)
    total_row = gathered[:, :, half].sum(axis=(0, 1))
    stream_one = residual_scale * block[:batch].astype(f32) + 0.5 * total
    row_mean = (
        residual_scale * token_sum[:, 0]
        + 0.5 * (total_row[:batch] + total_row[batch:])
    ) / width
    centred = stream_one - row_mean[:, None]

    scaled = (centred * gain_one.astype(f32)).astype(bf16)
    projected = jnp.concatenate(
        [jnp.dot(scaled, w, preferred_element_type=f32) for w in weights], axis=1
    ).astype(bf16)
    projected = projected.reshape(2, half, chunk_count, LANES).transpose(1, 2, 0, 3)
    blocks = jnp.concatenate(
        [
            projected,
            centred.astype(bf16).reshape(2, half, LANES).swapaxes(0, 1)[:, None],
            jnp.broadcast_to(bias_own.astype(bf16)[None, None], (kv_count, 1, 2, LANES)),
        ],
        axis=1,
    )
    arrived, at, kv, tp, norm_gain, norm_bias, params = alone(
        blocks, KV, at, kv, tp, norm_gain, norm_bias, params
    )
    mixer_part, piece, updated = mixer(
        at,
        arrived,
        params,
        lower_bound.reshape(heads, HEAD),
        head_gain.reshape(heads, HEAD),
        state,
        mixer_weight,
    )
    arrived, at, tp, norm_gain, norm_bias, params, piece = alone(
        mixer_part, TP, at, tp, norm_gain, norm_bias, params, piece
    )
    stream_own = (piece + arrived.sum(axis=0)).astype(bf16)
    arrived, at, tp, norm_gain, norm_bias, params = alone(
        copies(stream_own, chip_count), CHIPS, at, tp, norm_gain, norm_bias, params
    )
    arrived = lax.all_gather(arrived, CORE, axis=0)
    arrived = arrived.reshape(2, kv_count, x_count, *stream_own.shape)

    kept, sent, own_normed = second_block(at, arrived, params, stored)
    came = lax.ppermute(sent, CORE, SWAP)
    blocks = (kept.astype(f32) + came.astype(f32)).astype(bf16)
    arrived, tp, norm_gain, norm_bias, own_normed = alone(
        blocks, KV, tp, norm_gain, norm_bias, own_normed
    )
    gathered, tp, norm_gain, norm_bias, own_normed = over_tp(
        wide_sum(arrived).astype(bf16), tp, norm_gain, norm_bias, own_normed
    )
    gathered = gathered.astype(f32)
    total = gathered.sum(axis=0).reshape(batch, LANES)
    stream_three = residual_scale * own_normed.astype(f32) + 0.5 * total
    block_sum = stream_three.sum(axis=1)
    block_mean = block_sum / LANES
    off = stream_three - block_mean[:, None]
    stats = jnp.concatenate([block_mean, (off * off).sum(axis=1)])[None]
    stats, tp, norm_gain, norm_bias, stream_three = alone(
        copies(stats, kv_count), KV, tp, norm_gain, norm_bias, stream_three
    )
    stats = stats[:, 0]
    means, squares = stats[:, :batch], stats[:, batch:]
    row_mean = means.mean(axis=0)
    spread = (squares.sum(axis=0) + LANES * ((means - row_mean) ** 2).sum(axis=0)) / width
    own = lax.dynamic_slice_in_dim(stream_three, tp * own_cols, own_cols, 1)
    mixed = (own - row_mean[:, None]) * lax.rsqrt(spread + norm_eps)[:, None] * norm_gain[
        2
    ].astype(f32) + norm_bias[2].astype(f32)
    mixed = mixed.reshape(2, half, own_cols).swapaxes(0, 1).reshape(batch, own_cols)
    return (mixed.astype(bf16), updated)


def solution(mesh):
    finer = Mesh(mesh.devices.reshape(8, 4, 4, 2), KV_TP)
    in_specs = (
        P(None, KV_TP),
        P(None, None, KV_TP),
        P(None, None, KV_TP),
        P(None, KV_TP, None),
        P(None, KV_TP),
        P(None, KV_TP),
        P(KV, TP),
        P(KV, TP),
        P(KV, TP),
        P(KV, TP),
        P(TP),
        P(TP),
        P(TP, None),
        P(KV, TP, None, None),
    )
    out_specs = (P(None, KV_TP), P(KV, TP, None, None))
    return jax.shard_map(local, mesh=finer, in_specs=in_specs, out_specs=out_specs, check_vma=False)
```

```python
import jax
import jax.numpy as jnp
from jax import lax
from jax.experimental import pallas as pl
from jax.experimental.pallas import tpu as pltpu
from jax.sharding import Mesh
from jax.sharding import PartitionSpec as P

HEAD = 128
LANES = 128
KV_TP = ("kv_0", "kv_1", "tp_0", "tp_1")
KV = ("kv_0", "kv_1")
TP = ("tp_0", "tp_1")
CHIPS = ("kv_0", "kv_1", "tp_0")
CORE = "tp_1"
SWAP = [(0, 1), (1, 0)]

residual_scale = 8.0**0.25
norm_eps = 1e-05
head_eps = 1e-06
bf16 = jnp.bfloat16
f32 = jnp.float32


def exchange(blocks, axes):
    return lax.all_to_all(blocks, axes, split_axis=0, concat_axis=0, tiled=True)


def to_everyone(block, axes, count):
    return exchange(jnp.broadcast_to(block[None], (count, *block.shape)), axes)


def alone(blocks, axes, *held):
    blocks, *held = lax.optimization_barrier((blocks, *held))
    return lax.optimization_barrier((exchange(blocks, axes), *held))


def wide_sum(blocks):
    return lax.optimization_barrier(blocks.astype(f32).sum(axis=0))


def copies(block, count):
    return jnp.broadcast_to(block[None], (count, *block.shape))


def small(grant=8):
    return pltpu.CompilerParams(vmem_limit_bytes=grant * 2**20)


VMEM = pl.BlockSpec(memory_space=pltpu.VMEM)
SMEM = pl.BlockSpec(memory_space=pltpu.SMEM)
ANYWHERE = pl.BlockSpec(memory_space=pl.ANY)


def off_chip(x):
    return pltpu.with_memory_space_constraint(x, pltpu.HBM)


def place_kernel(
    at_ref,
    tokens_hbm,
    gain_hbm,
    bias_hbm,
    result_ref,
    lines_ref,
    tokens_ref,
    gain_ref,
    bias_ref,
    sem,
):
    pairs = ((tokens_hbm, tokens_ref), (gain_hbm, gain_ref), (bias_hbm, bias_ref))
    fetches = [pltpu.make_async_copy(*pair, sem.at[i]) for i, pair in enumerate(pairs)]
    for fetch in fetches:
        fetch.start()
    own_cols, batch = tokens_ref.shape
    half = batch // 2
    lane = lax.broadcasted_iota(jnp.int32, (batch, LANES), 1)
    row = lane % batch
    taken = lax.broadcasted_iota(jnp.int32, (batch, LANES), 0) == 2 * (row % half) + row // half
    first = jnp.where(taken & (lane < batch), 1.0, 0.0).astype(bf16)
    second = jnp.where(taken & (lane >= batch), 1.0, 0.0).astype(bf16)
    groups = LANES // own_cols
    spot = lax.broadcasted_iota(jnp.int32, (own_cols, LANES), 0)
    own_lane = lax.broadcasted_iota(jnp.int32, (own_cols, LANES), 1)
    for fetch in fetches:
        fetch.wait()
    top = jnp.dot(tokens_ref[...], first, preferred_element_type=f32)
    low = jnp.dot(tokens_ref[...], second, preferred_element_type=f32)
    line = jnp.zeros((1, LANES), f32)
    for index in range(6):
        at = (index + at_ref[1]) % groups * own_cols
        place = jnp.where(own_lane == spot + at, 1.0, 0.0).astype(bf16)
        source = gain_ref if index < 3 else bias_ref
        moved = jnp.dot(source[...], place, preferred_element_type=f32)
        line = line + moved[index % 3 : index % 3 + 1]
    count = own_cols // 2
    lines_ref[...] = jnp.zeros(lines_ref.shape, f32)
    lines_ref[:count, :] = top[:count] + low[count:]
    lines_ref[count : count + 1, :] = line
    lines = lines_ref[...].astype(bf16).reshape(count, 2, LANES)[: result_ref.shape[1]]
    for copy in range(result_ref.shape[0]):
        result_ref[copy] = lines


def placed_copies(at, tokens, gain, bias, count):
    batch, own_cols = tokens.shape
    return pl.pallas_call(
        place_kernel,
        in_specs=[SMEM] + [ANYWHERE] * 3,
        out_specs=VMEM,
        out_shape=jax.ShapeDtypeStruct((count, own_cols // 4 + 1, 2, LANES), bf16),
        scratch_shapes=[
            pltpu.VMEM((own_cols, LANES), f32),
            pltpu.VMEM((own_cols, batch), bf16),
            pltpu.VMEM(gain.shape, bf16),
            pltpu.VMEM(bias.shape, bf16),
            pltpu.SemaphoreType.DMA((3,)),
        ],
        compiler_params=small(),
        name="place",
    )(at, off_chip(tokens.T), off_chip(gain), off_chip(bias))


def load_kernel(
    out_hbm, gate_hbm, up_hbm, down_hbm, out_ref, gate_ref, up_ref, down_ref, part_sem, sem
):
    parts, _, step = out_ref.shape
    pairs = ((gate_hbm, gate_ref), (up_hbm, up_ref), (down_hbm, down_ref))
    fetches = [pltpu.make_async_copy(*pair, sem.at[i]) for i, pair in enumerate(pairs)]
    fetches += [
        pltpu.make_async_copy(
            out_hbm.at[:, pl.ds(part * step, step)], out_ref.at[part], part_sem.at[part]
        )
        for part in range(parts)
    ]
    for fetch in fetches:
        fetch.start()
    for fetch in fetches:
        fetch.wait()


def load(out_weight, stored, parts):
    depth, width = out_weight.shape
    return pl.pallas_call(
        load_kernel,
        in_specs=[ANYWHERE] * 4,
        out_specs=[VMEM] * 4,
        out_shape=[jax.ShapeDtypeStruct((parts, depth, width // parts), bf16)]
        + [jax.ShapeDtypeStruct(w.shape, bf16) for w in stored],
        scratch_shapes=[pltpu.SemaphoreType.DMA((parts,)), pltpu.SemaphoreType.DMA((3,))],
        compiler_params=small(12),
        name="load",
    )(*[off_chip(w) for w in (out_weight, *stored)])


def order_kernel(at_ref, rows_ref, w0, w1, w2, w3, params_ref, bias_ref):
    cores, kv_count, x_count = rows_ref.shape[:3]
    last = rows_ref.shape[3] - 1
    groups = cores * x_count
    own_cols = LANES // groups
    lines = [
        rows_ref[group % cores, :, group // cores, last].astype(f32)[:, 0, :]
        for group in range(groups)
    ]
    place = lax.broadcasted_iota(jnp.int32, (kv_count, LANES), 1) // own_cols
    params_ref[...] = jnp.zeros(params_ref.shape, f32)
    for index in range(6):
        total = jnp.zeros((kv_count, LANES), f32)
        for group in range(groups):
            total = jnp.where(place == (index + group) % groups, lines[group], total)
        if index:
            total = pltpu.roll(total, LANES - index * own_cols, 1)
        params_ref[pl.ds(index, kv_count, stride=8), :] = total
    own = params_ref[pl.ds(pl.multiple_of(at_ref[0] * 8, 8), 8), :].astype(bf16)
    for index, w_ref in enumerate((w0, w1, w2, w3)):
        sums = jnp.dot(own, w_ref[...], preferred_element_type=f32)
        heads = sums.shape[1] // LANES
        for head in range(heads):
            chunk = index * heads + head
            bias_ref[chunk : chunk + 1, :] = sums[3:4, head * LANES : (head + 1) * LANES]


def in_order(at, rows, weights):
    kv_count = rows.shape[1]
    return pl.pallas_call(
        order_kernel,
        in_specs=[SMEM] + [VMEM] * 5,
        out_specs=[VMEM] * 2,
        out_shape=[
            jax.ShapeDtypeStruct((kv_count * 8, LANES), f32),
            jax.ShapeDtypeStruct((4 * weights[0].shape[1] // LANES, LANES), f32),
        ],
        compiler_params=small(),
        name="in_order",
    )(at, rows, *weights)


def stored(ref):
    return ref[...].reshape(ref.shape[0] * ref.shape[1], ref.shape[2])


def feed_forward(gate, up, core, layer, down_ref):
    hidden = jax.nn.silu(gate) * up
    unit = lax.broadcasted_iota(jnp.int32, hidden.shape, 1)
    hidden = jnp.where(unit % 2 == layer, hidden, 0.0)
    half = hidden.shape[0] // 2
    low, high = hidden[:half], hidden[half:]
    first = core == 0
    hidden = jnp.concatenate([jnp.where(first, low, high), jnp.where(first, high, low)])
    return jnp.dot(hidden.astype(bf16), stored(down_ref), preferred_element_type=f32)


def write_halves(part, kept_ref, sent_ref):
    chunks, half, _ = kept_ref.shape
    for chunk in range(chunks):
        at = slice(chunk * LANES, (chunk + 1) * LANES)
        kept_ref[chunk] = part[:half, at].astype(bf16)
        sent_ref[chunk] = part[half:, at].astype(bf16)


def first_kernel(
    at_ref,
    rows_ref,
    gate_ref,
    up_ref,
    down_ref,
    kept_ref,
    sent_ref,
    tail_ref,
    total_ref,
    block_ref,
    x_ref,
):
    half = kept_ref.shape[1]
    batch = 2 * half
    cores, kv_count, x_count = rows_ref.shape[:3]
    pairs = rows_ref.shape[3] - 1
    core = at_ref[2]
    total = jnp.zeros((8, LANES), f32)
    for index in range(cores):
        for x in range(x_count):
            lines = rows_ref[index, :, x, :pairs].reshape(kv_count * 8, LANES).astype(f32)
            other = pltpu.roll(lines, LANES - batch, 1)
            lines = lines.reshape(kv_count, 8, LANES)
            total = total + lines.sum(axis=0)
            lines = jnp.concatenate([lines, other.reshape(kv_count, 8, LANES)], axis=1)
            x_ref[:, x * cores + index] = lines.astype(bf16)
    total = jnp.sum(total, axis=0, keepdims=True)
    total = total + pltpu.roll(total, LANES - batch, 1)
    total_ref[...] = jnp.broadcast_to(total, total_ref.shape)
    own = x_ref[at_ref[0]].reshape(LANES, LANES).astype(f32)
    block_ref[...] = own.T[:batch]
    rows = x_ref[...].reshape(kv_count * LANES, LANES)
    gate = jnp.dot(stored(gate_ref), rows, preferred_element_type=f32).T[:batch]
    up = jnp.dot(stored(up_ref), rows, preferred_element_type=f32).T[:batch]
    part = feed_forward(gate, up, core, 0, down_ref)
    write_halves(part, kept_ref, sent_ref)
    sums = jnp.broadcast_to(jnp.sum(part, axis=1, keepdims=True), (batch, LANES))
    row = (lax.broadcasted_iota(jnp.int32, (batch, LANES), 0) + core * half) % batch
    lane = lax.broadcasted_iota(jnp.int32, (batch, LANES), 1)
    line = jnp.sum(jnp.where(lane % batch == row, sums, 0.0), axis=0, keepdims=True)
    high = line.astype(bf16).astype(f32)
    line = jnp.where(lane[:1] < batch, high, line - high)
    tail_ref[...] = jnp.broadcast_to(line, tail_ref.shape)


def stored_order(gate, up, down):
    return gate.transpose(2, 0, 1), up.transpose(2, 0, 1), down.transpose(1, 0, 2)


def first_block(at, rows, stored, half):
    chunks = rows.shape[1]
    groups = rows.shape[0] * rows.shape[2]
    return pl.pallas_call(
        first_kernel,
        in_specs=[SMEM] + [VMEM] * 4,
        out_specs=[VMEM] * 5,
        out_shape=[
            jax.ShapeDtypeStruct((chunks, half, LANES), bf16),
            jax.ShapeDtypeStruct((chunks, half, LANES), bf16),
            jax.ShapeDtypeStruct((8, LANES), f32),
            jax.ShapeDtypeStruct((8, LANES), f32),
            jax.ShapeDtypeStruct((2 * half, LANES), f32),
        ],
        scratch_shapes=[pltpu.VMEM((chunks, groups, LANES // groups, LANES), bf16)],
        compiler_params=small(12),
        name="first_block",
    )(at, rows, *stored)


def blocks_kernel(kept_ref, came_ref, tail_ref, bias_ref, result_ref):
    chunks, half, _ = kept_ref.shape
    share = chunks // bias_ref.shape[0]
    top = lax.broadcasted_iota(jnp.int32, (8, LANES), 0) == 0
    for chunk in range(chunks):
        both = kept_ref[chunk].astype(f32) + came_ref[chunk].astype(f32)
        bias = bias_ref[chunk // share : chunk // share + 1, :]
        tail = jnp.where(top, tail_ref[...], bias)
        lines = jnp.concatenate([both, tail]).astype(bf16)
        pairs = lines.reshape(lines.shape[0] // 2, 2, LANES)
        result_ref[chunk] = pairs[: result_ref.shape[1]]


def first_blocks(kept, came, tail, bias):
    chunks, half, lanes = kept.shape
    return pl.pallas_call(
        blocks_kernel,
        in_specs=[VMEM] * 4,
        out_specs=VMEM,
        out_shape=jax.ShapeDtypeStruct((chunks, half // 2 + 1, 2, lanes), bf16),
        compiler_params=small(),
        name="first_blocks",
    )(kept, came, tail, bias)


def second_kernel(
    at_ref,
    arrived_ref,
    params_ref,
    gate_ref,
    up_ref,
    down_ref,
    kept_ref,
    sent_ref,
    own_ref,
    raw_ref,
    result_ref,
):
    cores, kv_count, x_count, rows, _ = arrived_ref.shape
    pieces = rows // 2
    chunks = cores * x_count * pieces
    for x in range(x_count):
        for core in range(cores):
            tiles = arrived_ref[core, :, x].astype(f32)
            raw_ref[x * cores + core] = tiles.reshape(kv_count * rows, LANES)

    def lines(chunk, seq):
        at = (chunk % pieces) * 2 + seq
        return raw_ref[chunk // pieces, pl.ds(at, kv_count, stride=rows), :]

    width = chunks * LANES
    for seq in range(2):
        total = sum(lines(chunk, seq) for chunk in range(chunks))
        mean = jnp.sum(total, axis=1, keepdims=True) / width
        squares = jnp.zeros((kv_count, LANES), f32)
        for chunk in range(chunks):
            off = lines(chunk, seq) - mean
            squares = squares + off * off
        spread = jnp.sum(squares, axis=1, keepdims=True) / width
        scale = lax.rsqrt(spread + norm_eps)
        for chunk in range(chunks):
            params = params_ref[chunk].astype(f32)
            normed = (lines(chunk, seq) - mean) * scale * params[1:2] + params[4:5]
            result_ref[
                seq * kv_count : (seq + 1) * kv_count, chunk * LANES : (chunk + 1) * LANES
            ] = normed.astype(bf16)
    own_ref[...] = result_ref[:, pl.ds(pl.multiple_of(at_ref[0] * LANES, LANES), LANES)]
    dims = (((1,), (1,)), ((), ()))
    rows = result_ref[...]
    gate = lax.dot_general(rows, stored(gate_ref), dims, preferred_element_type=f32)
    up = lax.dot_general(rows, stored(up_ref), dims, preferred_element_type=f32)
    part = feed_forward(gate, up, at_ref[2], 1, down_ref)
    write_halves(part, kept_ref, sent_ref)


def second_block(at, arrived, params, stored):
    cores, kv_count, x_count, rows, lanes = arrived.shape
    chunks = cores * x_count * rows // 2
    return pl.pallas_call(
        second_kernel,
        in_specs=[SMEM] + [VMEM] * 5,
        out_specs=[VMEM] * 3,
        out_shape=[
            jax.ShapeDtypeStruct((chunks, kv_count, lanes), bf16),
            jax.ShapeDtypeStruct((chunks, kv_count, lanes), bf16),
            jax.ShapeDtypeStruct((2 * kv_count, lanes), bf16),
        ],
        scratch_shapes=[
            pltpu.VMEM((cores * x_count, kv_count * rows, lanes), f32),
            pltpu.VMEM((2 * kv_count, chunks * lanes), bf16),
        ],
        compiler_params=small(12),
        name="second_block",
    )(at, arrived, params, *stored)


def mixer_kernel(
    at_ref,
    arrived_ref,
    params_ref,
    low_ref,
    head_gain_ref,
    state_ref,
    weight_ref,
    sent_ref,
    piece_ref,
    updated_hbm,
    updated_ref,
    rows_ref,
    low_rows_ref,
    gain_rows_ref,
    readout_ref,
    gated_ref,
    updated_sem,
):
    seqs, heads = state_ref.shape[:2]
    kv_count = arrived_ref.shape[0]
    chunks = 4 * heads
    share = kv_count // chunks
    parts = sent_ref.shape[0]
    piece_chunks = kv_count // parts
    def block_rows(block):
        lines = arrived_ref[block, :chunks]
        return lines.reshape(seqs * chunks, LANES).astype(f32)

    total = block_rows(0)
    for block in range(1, kv_count):
        total = total + block_rows(block)
    tail = seqs * chunks
    width = kv_count * LANES
    own = arrived_ref[:, chunks].astype(f32)
    mean = jnp.sum(jnp.sum(own, axis=0), axis=1, keepdims=True) / width
    off = own - mean
    scale = jnp.sum(jnp.sum(off * off, axis=0), axis=1, keepdims=True) / width
    scale = lax.rsqrt(scale + norm_eps)
    for chunk in range(chunks):
        bias = arrived_ref[chunk * share, chunks + 1].astype(f32)
        for other in range(1, share):
            bias = bias + arrived_ref[chunk * share + other, chunks + 1].astype(f32)
        rows_ref[2 * chunk : 2 * chunk + 2, :] = bias
    odd = lax.broadcasted_iota(jnp.int32, (tail, LANES), 0) % 2 == 1
    row_scale = jnp.where(odd, scale[1:2], scale[0:1])
    pre = (total * row_scale + rows_ref[...]).astype(bf16).astype(f32)
    size = 2 * heads
    query_pre, forget_pre = pre[:size], pre[size : 2 * size]
    input_pre, outgate_pre = pre[2 * size : 3 * size], pre[3 * size :]

    tp = at_ref[1]
    for chunk in range(piece_chunks):
        at = tp * piece_chunks + chunk
        rows = arrived_ref[at, chunks].astype(f32)
        params = params_ref[at].astype(f32)
        rows = ((rows - mean) * scale * params[0:1] + params[3:4]).astype(bf16).astype(f32)
        piece_ref[2 * chunk : 2 * chunk + 2, :] = residual_scale * rows

    for head in range(heads):
        at = slice(2 * head, 2 * head + 2)
        low_rows_ref[at, :] = jnp.broadcast_to(low_ref[head : head + 1, :], (2, LANES))
        gain_rows_ref[at, :] = jnp.broadcast_to(head_gain_ref[head : head + 1, :], (2, LANES))
    low = low_rows_ref[...]
    forget = (low + (1.0 - low) * jax.nn.sigmoid(forget_pre)).T
    key = ((1.0 - low) * jax.nn.sigmoid(-forget_pre)).T
    query = jax.nn.silu(query_pre).T
    updated_copies = []
    for head in range(heads):
        for seq in range(seqs):
            row = head * 2 + seq
            new = (
                forget[:, row : row + 1] * state_ref[seq, head]
                + key[:, row : row + 1] * input_pre[row : row + 1, :]
            )
            updated_ref[seq, head] = new
            updated_copies.append(
                pltpu.make_async_copy(
                    updated_ref.at[seq, head], updated_hbm.at[seq, head], updated_sem.at[row]
                )
            )
            updated_copies[-1].start()
            readout_ref[row : row + 1, :] = jnp.sum(
                query[:, row : row + 1] * new, axis=0, keepdims=True
            )
    readout = readout_ref[...]
    readout = readout * lax.rsqrt(jnp.mean(readout * readout, axis=1, keepdims=True) + head_eps)
    gated = readout * gain_rows_ref[...] * jax.nn.silu(outgate_pre)
    gated_ref[...] = jnp.zeros(gated_ref.shape, f32)
    for head in range(heads):
        gated_ref[0:2, head * HEAD : (head + 1) * HEAD] = gated[2 * head : 2 * head + 2]
    lhs = gated_ref[...].astype(bf16)
    for part in range(parts):
        mixed = jnp.dot(lhs, weight_ref[part], preferred_element_type=f32)
        for chunk in range(piece_chunks):
            sent_ref[part, 2 * chunk : 2 * chunk + 2, :] = mixed[
                0:2, chunk * LANES : (chunk + 1) * LANES
            ]
    for copy in updated_copies:
        copy.wait()


def mixer(at, arrived, params, lower_bound, head_gain, state, weight):
    seqs, heads = state.shape[:2]
    parts, _, step = weight.shape
    rows = 2 * step // LANES
    return pl.pallas_call(
        mixer_kernel,
        in_specs=[SMEM] + [VMEM] * 6,
        out_specs=[VMEM, VMEM, ANYWHERE],
        out_shape=[
            jax.ShapeDtypeStruct((parts, rows, LANES), f32),
            jax.ShapeDtypeStruct((rows, LANES), f32),
            jax.ShapeDtypeStruct(state.shape, f32),
        ],
        scratch_shapes=[
            pltpu.VMEM(state.shape, f32),
            pltpu.VMEM((seqs * 4 * heads, LANES), f32),
            pltpu.VMEM((2 * heads, LANES), f32),
            pltpu.VMEM((2 * heads, LANES), f32),
            pltpu.VMEM((2 * heads, LANES), f32),
            pltpu.VMEM((8, heads * HEAD), f32),
            pltpu.SemaphoreType.DMA((seqs * heads,)),
        ],
        compiler_params=small(),
        name="mixer",
    )(at, arrived, params, lower_bound, head_gain, state, weight)


def local(
    tokens,
    gate_weights,
    up_weights,
    down_weights,
    norm_gain,
    norm_bias,
    query_weight,
    forget_weight,
    input_weight,
    outgate_weight,
    lower_bound,
    head_gain,
    out_weight,
    state,
):
    batch, own_cols = tokens.shape
    heads = state.shape[1]
    kv_count, tp_count = lax.axis_size(KV), lax.axis_size(TP)
    x_count = tp_count // 2
    chip_count = kv_count * x_count
    half = batch // 2
    width = own_cols * kv_count * tp_count
    kv, tp, core = lax.axis_index(KV), lax.axis_index(TP), lax.axis_index(CORE)

    at = jnp.stack([kv, tp, core])
    blocks = placed_copies(at, tokens, norm_gain, norm_bias, chip_count)
    arrived = exchange(blocks, CHIPS)
    rows = lax.all_gather(arrived, CORE, axis=0)
    rows = rows.reshape(2, kv_count, x_count, *rows.shape[2:])

    def over_tp(lines, *held):
        gathered, *held = alone(copies(lines, tp_count), TP, *held)
        return gathered.reshape(x_count, 2, *lines.shape), *held

    weights = (query_weight, forget_weight, input_weight, outgate_weight)
    chunk_count = 4 * heads
    share = kv_count // chunk_count
    stored = stored_order(gate_weights, up_weights, down_weights)
    mixer_weight, *stored = load(out_weight, stored, tp_count)
    kept, sent, tail, token_sum, block = first_block(at, rows, stored, half)
    params, bias_rows = in_order(at, rows, weights)
    params = params.reshape(kv_count, 8, LANES)
    blocks = first_blocks(kept, lax.ppermute(sent, CORE, SWAP), tail, bias_rows)
    arrived, at, kv, tp, norm_gain, norm_bias, block, params, token_sum = alone(
        blocks, KV, at, kv, tp, norm_gain, norm_bias, block, params, token_sum
    )
    arrived = wide_sum(arrived).reshape(half + 2, LANES).astype(bf16)
    gathered, at, kv, tp, norm_gain, norm_bias, block, params, token_sum, arrived = over_tp(
        arrived, at, kv, tp, norm_gain, norm_bias, block, params, token_sum, arrived
    )
    gathered = gathered.astype(f32)
    bias_own = arrived[half + 1 : half + 2] / share
    gain_one = lax.dynamic_index_in_dim(params, kv, 0, keepdims=False)[:1]
    total = gathered[:, :, :half].sum(axis=0).reshape(batch, LANES)
    total_row = gathered[:, :, half].sum(axis=(0, 1))
    stream_one = residual_scale * block + 0.5 * total
    row_mean = (
        residual_scale * token_sum[0, :batch]
        + 0.5 * (total_row[:batch] + total_row[batch:])
    ) / width
    centred = stream_one - row_mean[:, None]

    scaled = (centred * gain_one.astype(f32)).astype(bf16)
    projected = jnp.concatenate(
        [jnp.dot(scaled, w, preferred_element_type=f32) for w in weights], axis=1
    ).astype(bf16)
    projected = projected.reshape(2, half, chunk_count, LANES).transpose(1, 2, 0, 3)
    blocks = jnp.concatenate(
        [
            projected,
            centred.astype(bf16).reshape(2, half, LANES).swapaxes(0, 1)[:, None],
            jnp.broadcast_to(bias_own.astype(bf16)[None, None], (kv_count, 1, 2, LANES)),
        ],
        axis=1,
    )
    arrived, at, kv, tp, norm_gain, norm_bias, params = alone(
        blocks, KV, at, kv, tp, norm_gain, norm_bias, params
    )
    mixer_part, piece, updated = mixer(
        at,
        arrived,
        params,
        lower_bound.reshape(heads, HEAD),
        head_gain.reshape(heads, HEAD),
        state,
        mixer_weight,
    )
    arrived, at, tp, norm_gain, norm_bias, params, piece = alone(
        mixer_part, TP, at, tp, norm_gain, norm_bias, params, piece
    )
    stream_own = (piece + arrived.sum(axis=0)).astype(bf16)
    arrived, at, tp, norm_gain, norm_bias, params = alone(
        copies(stream_own, chip_count), CHIPS, at, tp, norm_gain, norm_bias, params
    )
    arrived = lax.all_gather(arrived, CORE, axis=0)
    arrived = arrived.reshape(2, kv_count, x_count, *stream_own.shape)

    kept, sent, own_normed = second_block(at, arrived, params, stored)
    came = lax.ppermute(sent, CORE, SWAP)
    blocks = (kept.astype(f32) + came.astype(f32)).astype(bf16)
    arrived, tp, norm_gain, norm_bias, own_normed = alone(
        blocks, KV, tp, norm_gain, norm_bias, own_normed
    )
    gathered, tp, norm_gain, norm_bias, own_normed = over_tp(
        wide_sum(arrived).astype(bf16), tp, norm_gain, norm_bias, own_normed
    )
    gathered = gathered.astype(f32)
    total = gathered.sum(axis=0).reshape(batch, LANES)
    stream_three = residual_scale * own_normed.astype(f32) + 0.5 * total
    block_sum = stream_three.sum(axis=1)
    block_mean = block_sum / LANES
    off = stream_three - block_mean[:, None]
    stats = jnp.concatenate([block_mean, (off * off).sum(axis=1)])[None]
    stats, tp, norm_gain, norm_bias, stream_three = alone(
        copies(stats, kv_count), KV, tp, norm_gain, norm_bias, stream_three
    )
    stats = stats[:, 0]
    means, squares = stats[:, :batch], stats[:, batch:]
    row_mean = means.mean(axis=0)
    spread = (squares.sum(axis=0) + LANES * ((means - row_mean) ** 2).sum(axis=0)) / width
    own = lax.dynamic_slice_in_dim(stream_three, tp * own_cols, own_cols, 1)
    mixed = (own - row_mean[:, None]) * lax.rsqrt(spread + norm_eps)[:, None] * norm_gain[
        2
    ].astype(f32) + norm_bias[2].astype(f32)
    mixed = mixed.reshape(2, half, own_cols).swapaxes(0, 1).reshape(batch, own_cols)
    return (mixed.astype(bf16), updated)


def solution(mesh):
    finer = Mesh(mesh.devices.reshape(8, 4, 4, 2), KV_TP)
    in_specs = (
        P(None, KV_TP),
        P(None, None, KV_TP),
        P(None, None, KV_TP),
        P(None, KV_TP, None),
        P(None, KV_TP),
        P(None, KV_TP),
        P(KV, TP),
        P(KV, TP),
        P(KV, TP),
        P(KV, TP),
        P(TP),
        P(TP),
        P(TP, None),
        P(KV, TP, None, None),
    )
    out_specs = (P(None, KV_TP), P(KV, TP, None, None))
    return jax.shard_map(local, mesh=finer, in_specs=in_specs, out_specs=out_specs, check_vma=False)
```

```python
import jax
import jax.numpy as jnp
from jax import lax
from jax.experimental import pallas as pl
from jax.experimental.pallas import tpu as pltpu
from jax.sharding import Mesh
from jax.sharding import PartitionSpec as P

HEAD = 128
LANES = 128
KV_TP = ("kv_0", "kv_1", "tp_0", "tp_1")
KV = ("kv_0", "kv_1")
TP = ("tp_0", "tp_1")
CHIPS = ("kv_0", "kv_1", "tp_0")
CORE = "tp_1"
SWAP = [(0, 1), (1, 0)]

residual_scale = 8.0**0.25
norm_eps = 1e-05
head_eps = 1e-06
bf16 = jnp.bfloat16
f32 = jnp.float32


def exchange(blocks, axes):
    return lax.all_to_all(blocks, axes, split_axis=0, concat_axis=0, tiled=True)


def to_everyone(block, axes, count):
    return exchange(jnp.broadcast_to(block[None], (count, *block.shape)), axes)


def alone(blocks, axes, *held):
    blocks, *held = lax.optimization_barrier((blocks, *held))
    return lax.optimization_barrier((exchange(blocks, axes), *held))


def wide_sum(blocks):
    return lax.optimization_barrier(blocks.astype(f32).sum(axis=0))


def copies(block, count):
    return jnp.broadcast_to(block[None], (count, *block.shape))


def small(grant=8):
    return pltpu.CompilerParams(vmem_limit_bytes=grant * 2**20)


VMEM = pl.BlockSpec(memory_space=pltpu.VMEM)
SMEM = pl.BlockSpec(memory_space=pltpu.SMEM)
ANYWHERE = pl.BlockSpec(memory_space=pl.ANY)


def off_chip(x):
    return pltpu.with_memory_space_constraint(x, pltpu.HBM)


def place_kernel(
    at_ref,
    tokens_hbm,
    gain_hbm,
    bias_hbm,
    result_ref,
    lines_ref,
    tokens_ref,
    gain_ref,
    bias_ref,
    sem,
):
    pairs = ((tokens_hbm, tokens_ref), (gain_hbm, gain_ref), (bias_hbm, bias_ref))
    fetches = [pltpu.make_async_copy(*pair, sem.at[i]) for i, pair in enumerate(pairs)]
    for fetch in fetches:
        fetch.start()
    own_cols, batch = tokens_ref.shape
    half = batch // 2
    lane = lax.broadcasted_iota(jnp.int32, (batch, LANES), 1)
    row = lane % batch
    taken = lax.broadcasted_iota(jnp.int32, (batch, LANES), 0) == 2 * (row % half) + row // half
    first = jnp.where(taken & (lane < batch), 1.0, 0.0).astype(bf16)
    second = jnp.where(taken & (lane >= batch), 1.0, 0.0).astype(bf16)
    groups = LANES // own_cols
    spot = lax.broadcasted_iota(jnp.int32, (own_cols, LANES), 0)
    own_lane = lax.broadcasted_iota(jnp.int32, (own_cols, LANES), 1)
    for fetch in fetches:
        fetch.wait()
    top = jnp.dot(tokens_ref[...], first, preferred_element_type=f32)
    low = jnp.dot(tokens_ref[...], second, preferred_element_type=f32)
    line = jnp.zeros((1, LANES), f32)
    for index in range(6):
        at = (index + at_ref[1]) % groups * own_cols
        place = jnp.where(own_lane == spot + at, 1.0, 0.0).astype(bf16)
        source = gain_ref if index < 3 else bias_ref
        moved = jnp.dot(source[...], place, preferred_element_type=f32)
        line = line + moved[index % 3 : index % 3 + 1]
    count = own_cols // 2
    lines_ref[...] = jnp.zeros(lines_ref.shape, f32)
    lines_ref[:count, :] = top[:count] + low[count:]
    lines_ref[count : count + 1, :] = line
    lines = lines_ref[...].astype(bf16).reshape(count, 2, LANES)[: result_ref.shape[1]]
    for copy in range(result_ref.shape[0]):
        result_ref[copy] = lines


def placed_copies(at, tokens, gain, bias, count):
    batch, own_cols = tokens.shape
    return pl.pallas_call(
        place_kernel,
        in_specs=[SMEM] + [ANYWHERE] * 3,
        out_specs=VMEM,
        out_shape=jax.ShapeDtypeStruct((count, own_cols // 4 + 1, 2, LANES), bf16),
        scratch_shapes=[
            pltpu.VMEM((own_cols, LANES), f32),
            pltpu.VMEM((own_cols, batch), bf16),
            pltpu.VMEM(gain.shape, bf16),
            pltpu.VMEM(bias.shape, bf16),
            pltpu.SemaphoreType.DMA((3,)),
        ],
        compiler_params=small(),
        name="place",
    )(at, off_chip(tokens.T), off_chip(gain), off_chip(bias))


def load_kernel(gate_hbm, up_hbm, down_hbm, gate_ref, up_ref, down_ref, sem):
    pairs = ((gate_hbm, gate_ref), (up_hbm, up_ref), (down_hbm, down_ref))
    fetches = [pltpu.make_async_copy(*pair, sem.at[i]) for i, pair in enumerate(pairs)]
    for fetch in fetches:
        fetch.start()
    for fetch in fetches:
        fetch.wait()


def load(stored):
    return pl.pallas_call(
        load_kernel,
        in_specs=[ANYWHERE] * 3,
        out_specs=[VMEM] * 3,
        out_shape=[jax.ShapeDtypeStruct(w.shape, bf16) for w in stored],
        scratch_shapes=[pltpu.SemaphoreType.DMA((3,))],
        compiler_params=small(),
        name="load",
    )(*[off_chip(w) for w in stored])


def order_kernel(at_ref, rows_ref, w0, w1, w2, w3, params_ref, bias_ref):
    cores, kv_count, x_count = rows_ref.shape[:3]
    last = rows_ref.shape[3] - 1
    groups = cores * x_count
    own_cols = LANES // groups
    lines = [
        rows_ref[group % cores, :, group // cores, last].astype(f32)[:, 0, :]
        for group in range(groups)
    ]
    place = lax.broadcasted_iota(jnp.int32, (kv_count, LANES), 1) // own_cols
    params_ref[...] = jnp.zeros(params_ref.shape, f32)
    for index in range(6):
        total = jnp.zeros((kv_count, LANES), f32)
        for group in range(groups):
            total = jnp.where(place == (index + group) % groups, lines[group], total)
        if index:
            total = pltpu.roll(total, LANES - index * own_cols, 1)
        params_ref[pl.ds(index, kv_count, stride=8), :] = total
    own = params_ref[pl.ds(pl.multiple_of(at_ref[0] * 8, 8), 8), :].astype(bf16)
    for index, w_ref in enumerate((w0, w1, w2, w3)):
        sums = jnp.dot(own, w_ref[...], preferred_element_type=f32)
        heads = sums.shape[1] // LANES
        for head in range(heads):
            chunk = index * heads + head
            bias_ref[chunk : chunk + 1, :] = sums[3:4, head * LANES : (head + 1) * LANES]


def in_order(at, rows, weights):
    kv_count = rows.shape[1]
    return pl.pallas_call(
        order_kernel,
        in_specs=[SMEM] + [VMEM] * 5,
        out_specs=[VMEM] * 2,
        out_shape=[
            jax.ShapeDtypeStruct((kv_count * 8, LANES), f32),
            jax.ShapeDtypeStruct((4 * weights[0].shape[1] // LANES, LANES), f32),
        ],
        compiler_params=small(),
        name="in_order",
    )(at, rows, *weights)


def stored(ref):
    return ref[...].reshape(ref.shape[0] * ref.shape[1], ref.shape[2])


def feed_forward(gate, up, core, layer, down_ref):
    hidden = jax.nn.silu(gate) * up
    unit = lax.broadcasted_iota(jnp.int32, hidden.shape, 1)
    hidden = jnp.where(unit % 2 == layer, hidden, 0.0)
    half = hidden.shape[0] // 2
    low, high = hidden[:half], hidden[half:]
    first = core == 0
    hidden = jnp.concatenate([jnp.where(first, low, high), jnp.where(first, high, low)])
    return jnp.dot(hidden.astype(bf16), stored(down_ref), preferred_element_type=f32)


def write_halves(part, kept_ref, sent_ref):
    chunks, half, _ = kept_ref.shape
    for chunk in range(chunks):
        at = slice(chunk * LANES, (chunk + 1) * LANES)
        kept_ref[chunk] = part[:half, at].astype(bf16)
        sent_ref[chunk] = part[half:, at].astype(bf16)


def first_kernel(
    at_ref,
    rows_ref,
    gate_ref,
    up_ref,
    down_ref,
    kept_ref,
    sent_ref,
    tail_ref,
    total_ref,
    block_ref,
    x_ref,
):
    half = kept_ref.shape[1]
    batch = 2 * half
    cores, kv_count, x_count = rows_ref.shape[:3]
    pairs = rows_ref.shape[3] - 1
    core = at_ref[2]
    total = jnp.zeros((8, LANES), f32)
    for index in range(cores):
        for x in range(x_count):
            lines = rows_ref[index, :, x, :pairs].reshape(kv_count * 8, LANES).astype(f32)
            other = pltpu.roll(lines, LANES - batch, 1)
            lines = lines.reshape(kv_count, 8, LANES)
            total = total + lines.sum(axis=0)
            lines = jnp.concatenate([lines, other.reshape(kv_count, 8, LANES)], axis=1)
            x_ref[:, x * cores + index] = lines.astype(bf16)
    total = jnp.sum(total, axis=0, keepdims=True)
    total = total + pltpu.roll(total, LANES - batch, 1)
    total_ref[...] = jnp.broadcast_to(total, total_ref.shape)
    own = x_ref[at_ref[0]].reshape(LANES, LANES).astype(f32)
    block_ref[...] = own.T[:batch]
    rows = x_ref[...].reshape(kv_count * LANES, LANES)
    gate = jnp.dot(stored(gate_ref), rows, preferred_element_type=f32).T[:batch]
    up = jnp.dot(stored(up_ref), rows, preferred_element_type=f32).T[:batch]
    part = feed_forward(gate, up, core, 0, down_ref)
    write_halves(part, kept_ref, sent_ref)
    sums = jnp.broadcast_to(jnp.sum(part, axis=1, keepdims=True), (batch, LANES))
    row = (lax.broadcasted_iota(jnp.int32, (batch, LANES), 0) + core * half) % batch
    lane = lax.broadcasted_iota(jnp.int32, (batch, LANES), 1)
    line = jnp.sum(jnp.where(lane % batch == row, sums, 0.0), axis=0, keepdims=True)
    high = line.astype(bf16).astype(f32)
    line = jnp.where(lane[:1] < batch, high, line - high)
    tail_ref[...] = jnp.broadcast_to(line, tail_ref.shape)


def stored_order(gate, up, down):
    return gate.transpose(2, 0, 1), up.transpose(2, 0, 1), down.transpose(1, 0, 2)


def first_block(at, rows, stored, half):
    chunks = rows.shape[1]
    groups = rows.shape[0] * rows.shape[2]
    return pl.pallas_call(
        first_kernel,
        in_specs=[SMEM] + [VMEM] * 4,
        out_specs=[VMEM] * 5,
        out_shape=[
            jax.ShapeDtypeStruct((chunks, half, LANES), bf16),
            jax.ShapeDtypeStruct((chunks, half, LANES), bf16),
            jax.ShapeDtypeStruct((8, LANES), f32),
            jax.ShapeDtypeStruct((8, LANES), f32),
            jax.ShapeDtypeStruct((2 * half, LANES), f32),
        ],
        scratch_shapes=[pltpu.VMEM((chunks, groups, LANES // groups, LANES), bf16)],
        compiler_params=small(12),
        name="first_block",
    )(at, rows, *stored)


def blocks_kernel(kept_ref, came_ref, tail_ref, bias_ref, result_ref):
    chunks, half, _ = kept_ref.shape
    share = chunks // bias_ref.shape[0]
    top = lax.broadcasted_iota(jnp.int32, (8, LANES), 0) == 0
    for chunk in range(chunks):
        both = kept_ref[chunk].astype(f32) + came_ref[chunk].astype(f32)
        bias = bias_ref[chunk // share : chunk // share + 1, :]
        tail = jnp.where(top, tail_ref[...], bias)
        lines = jnp.concatenate([both, tail]).astype(bf16)
        pairs = lines.reshape(lines.shape[0] // 2, 2, LANES)
        result_ref[chunk] = pairs[: result_ref.shape[1]]


def first_blocks(kept, came, tail, bias):
    chunks, half, lanes = kept.shape
    return pl.pallas_call(
        blocks_kernel,
        in_specs=[VMEM] * 4,
        out_specs=VMEM,
        out_shape=jax.ShapeDtypeStruct((chunks, half // 2 + 1, 2, lanes), bf16),
        compiler_params=small(),
        name="first_blocks",
    )(kept, came, tail, bias)


def second_kernel(
    at_ref,
    arrived_ref,
    params_ref,
    gate_ref,
    up_ref,
    down_ref,
    kept_ref,
    sent_ref,
    own_ref,
    raw_ref,
    result_ref,
):
    cores, kv_count, x_count, rows, _ = arrived_ref.shape
    pieces = rows // 2
    chunks = cores * x_count * pieces
    for x in range(x_count):
        for core in range(cores):
            tiles = arrived_ref[core, :, x].astype(f32)
            raw_ref[x * cores + core] = tiles.reshape(kv_count * rows, LANES)

    def lines(chunk, seq):
        at = (chunk % pieces) * 2 + seq
        return raw_ref[chunk // pieces, pl.ds(at, kv_count, stride=rows), :]

    width = chunks * LANES
    for seq in range(2):
        total = sum(lines(chunk, seq) for chunk in range(chunks))
        mean = jnp.sum(total, axis=1, keepdims=True) / width
        squares = jnp.zeros((kv_count, LANES), f32)
        for chunk in range(chunks):
            off = lines(chunk, seq) - mean
            squares = squares + off * off
        spread = jnp.sum(squares, axis=1, keepdims=True) / width
        scale = lax.rsqrt(spread + norm_eps)
        for chunk in range(chunks):
            params = params_ref[chunk].astype(f32)
            normed = (lines(chunk, seq) - mean) * scale * params[1:2] + params[4:5]
            result_ref[
                seq * kv_count : (seq + 1) * kv_count, chunk * LANES : (chunk + 1) * LANES
            ] = normed.astype(bf16)
    own_ref[...] = result_ref[:, pl.ds(pl.multiple_of(at_ref[0] * LANES, LANES), LANES)]
    dims = (((1,), (1,)), ((), ()))
    rows = result_ref[...]
    gate = lax.dot_general(rows, stored(gate_ref), dims, preferred_element_type=f32)
    up = lax.dot_general(rows, stored(up_ref), dims, preferred_element_type=f32)
    part = feed_forward(gate, up, at_ref[2], 1, down_ref)
    write_halves(part, kept_ref, sent_ref)


def second_block(at, arrived, params, stored):
    cores, kv_count, x_count, rows, lanes = arrived.shape
    chunks = cores * x_count * rows // 2
    return pl.pallas_call(
        second_kernel,
        in_specs=[SMEM] + [VMEM] * 5,
        out_specs=[VMEM] * 3,
        out_shape=[
            jax.ShapeDtypeStruct((chunks, kv_count, lanes), bf16),
            jax.ShapeDtypeStruct((chunks, kv_count, lanes), bf16),
            jax.ShapeDtypeStruct((2 * kv_count, lanes), bf16),
        ],
        scratch_shapes=[
            pltpu.VMEM((cores * x_count, kv_count * rows, lanes), f32),
            pltpu.VMEM((2 * kv_count, chunks * lanes), bf16),
        ],
        compiler_params=small(12),
        name="second_block",
    )(at, arrived, params, *stored)


def mixer_kernel(
    at_ref,
    arrived_ref,
    params_ref,
    low_ref,
    head_gain_ref,
    state_ref,
    weight_hbm,
    sent_ref,
    piece_ref,
    updated_hbm,
    updated_ref,
    weight_ref,
    rows_ref,
    low_rows_ref,
    gain_rows_ref,
    readout_ref,
    gated_ref,
    updated_sem,
    weight_sem,
):
    seqs, heads = state_ref.shape[:2]
    kv_count = arrived_ref.shape[0]
    chunks = 4 * heads
    share = kv_count // chunks
    parts = sent_ref.shape[0]
    piece_chunks = kv_count // parts
    step = weight_ref.shape[2]
    fetches = [
        pltpu.make_async_copy(
            weight_hbm.at[:, pl.ds(part * step, step)], weight_ref.at[part], weight_sem.at[part]
        )
        for part in range(parts)
    ]
    for fetch in fetches:
        fetch.start()

    def block_rows(block):
        lines = arrived_ref[block, :chunks]
        return lines.reshape(seqs * chunks, LANES).astype(f32)

    total = block_rows(0)
    for block in range(1, kv_count):
        total = total + block_rows(block)
    tail = seqs * chunks
    width = kv_count * LANES
    own = arrived_ref[:, chunks].astype(f32)
    mean = jnp.sum(jnp.sum(own, axis=0), axis=1, keepdims=True) / width
    off = own - mean
    scale = jnp.sum(jnp.sum(off * off, axis=0), axis=1, keepdims=True) / width
    scale = lax.rsqrt(scale + norm_eps)
    for chunk in range(chunks):
        bias = arrived_ref[chunk * share, chunks + 1].astype(f32)
        for other in range(1, share):
            bias = bias + arrived_ref[chunk * share + other, chunks + 1].astype(f32)
        rows_ref[2 * chunk : 2 * chunk + 2, :] = bias
    odd = lax.broadcasted_iota(jnp.int32, (tail, LANES), 0) % 2 == 1
    row_scale = jnp.where(odd, scale[1:2], scale[0:1])
    pre = (total * row_scale + rows_ref[...]).astype(bf16).astype(f32)
    size = 2 * heads
    query_pre, forget_pre = pre[:size], pre[size : 2 * size]
    input_pre, outgate_pre = pre[2 * size : 3 * size], pre[3 * size :]

    tp = at_ref[1]
    for chunk in range(piece_chunks):
        at = tp * piece_chunks + chunk
        rows = arrived_ref[at, chunks].astype(f32)
        params = params_ref[at].astype(f32)
        rows = ((rows - mean) * scale * params[0:1] + params[3:4]).astype(bf16).astype(f32)
        piece_ref[2 * chunk : 2 * chunk + 2, :] = residual_scale * rows

    for head in range(heads):
        at = slice(2 * head, 2 * head + 2)
        low_rows_ref[at, :] = jnp.broadcast_to(low_ref[head : head + 1, :], (2, LANES))
        gain_rows_ref[at, :] = jnp.broadcast_to(head_gain_ref[head : head + 1, :], (2, LANES))
    low = low_rows_ref[...]
    forget = (low + (1.0 - low) * jax.nn.sigmoid(forget_pre)).T
    key = ((1.0 - low) * jax.nn.sigmoid(-forget_pre)).T
    query = jax.nn.silu(query_pre).T
    updated_copies = []
    for head in range(heads):
        for seq in range(seqs):
            row = head * 2 + seq
            new = (
                forget[:, row : row + 1] * state_ref[seq, head]
                + key[:, row : row + 1] * input_pre[row : row + 1, :]
            )
            updated_ref[seq, head] = new
            updated_copies.append(
                pltpu.make_async_copy(
                    updated_ref.at[seq, head], updated_hbm.at[seq, head], updated_sem.at[row]
                )
            )
            updated_copies[-1].start()
            readout_ref[row : row + 1, :] = jnp.sum(
                query[:, row : row + 1] * new, axis=0, keepdims=True
            )
    readout = readout_ref[...]
    readout = readout * lax.rsqrt(jnp.mean(readout * readout, axis=1, keepdims=True) + head_eps)
    gated = readout * gain_rows_ref[...] * jax.nn.silu(outgate_pre)
    gated_ref[...] = jnp.zeros(gated_ref.shape, f32)
    for head in range(heads):
        gated_ref[0:2, head * HEAD : (head + 1) * HEAD] = gated[2 * head : 2 * head + 2]
    lhs = gated_ref[...].astype(bf16)
    for part in range(parts):
        fetches[part].wait()
        mixed = jnp.dot(lhs, weight_ref[part], preferred_element_type=f32)
        for chunk in range(piece_chunks):
            sent_ref[part, 2 * chunk : 2 * chunk + 2, :] = mixed[
                0:2, chunk * LANES : (chunk + 1) * LANES
            ]
    for copy in updated_copies:
        copy.wait()


def mixer(at, arrived, params, lower_bound, head_gain, state, weight, parts):
    seqs, heads = state.shape[:2]
    depth, width = weight.shape
    rows = 2 * width // parts // LANES
    return pl.pallas_call(
        mixer_kernel,
        in_specs=[SMEM] + [VMEM] * 5 + [ANYWHERE],
        out_specs=[VMEM, VMEM, ANYWHERE],
        out_shape=[
            jax.ShapeDtypeStruct((parts, rows, LANES), f32),
            jax.ShapeDtypeStruct((rows, LANES), f32),
            jax.ShapeDtypeStruct(state.shape, f32),
        ],
        scratch_shapes=[
            pltpu.VMEM(state.shape, f32),
            pltpu.VMEM((parts, depth, width // parts), bf16),
            pltpu.VMEM((seqs * 4 * heads, LANES), f32),
            pltpu.VMEM((2 * heads, LANES), f32),
            pltpu.VMEM((2 * heads, LANES), f32),
            pltpu.VMEM((2 * heads, LANES), f32),
            pltpu.VMEM((8, heads * HEAD), f32),
            pltpu.SemaphoreType.DMA((seqs * heads,)),
            pltpu.SemaphoreType.DMA((parts,)),
        ],
        compiler_params=small(),
        name="mixer",
    )(at, arrived, params, lower_bound, head_gain, state, off_chip(weight))


def local(
    tokens,
    gate_weights,
    up_weights,
    down_weights,
    norm_gain,
    norm_bias,
    query_weight,
    forget_weight,
    input_weight,
    outgate_weight,
    lower_bound,
    head_gain,
    out_weight,
    state,
):
    batch, own_cols = tokens.shape
    heads = state.shape[1]
    kv_count, tp_count = lax.axis_size(KV), lax.axis_size(TP)
    x_count = tp_count // 2
    chip_count = kv_count * x_count
    half = batch // 2
    width = own_cols * kv_count * tp_count
    kv, tp, core = lax.axis_index(KV), lax.axis_index(TP), lax.axis_index(CORE)

    at = jnp.stack([kv, tp, core])
    blocks = placed_copies(at, tokens, norm_gain, norm_bias, chip_count)
    arrived = exchange(blocks, CHIPS)
    rows = lax.all_gather(arrived, CORE, axis=0)
    rows = rows.reshape(2, kv_count, x_count, *rows.shape[2:])

    def over_tp(lines, *held):
        gathered, *held = alone(copies(lines, tp_count), TP, *held)
        return gathered.reshape(x_count, 2, *lines.shape), *held

    weights = (query_weight, forget_weight, input_weight, outgate_weight)
    chunk_count = 4 * heads
    share = kv_count // chunk_count
    stored = stored_order(gate_weights, up_weights, down_weights)
    stored = load(stored)
    kept, sent, tail, token_sum, block = first_block(at, rows, stored, half)
    params, bias_rows = in_order(at, rows, weights)
    params = params.reshape(kv_count, 8, LANES)
    blocks = first_blocks(kept, lax.ppermute(sent, CORE, SWAP), tail, bias_rows)
    arrived, at, kv, tp, norm_gain, norm_bias, block, params, token_sum = alone(
        blocks, KV, at, kv, tp, norm_gain, norm_bias, block, params, token_sum
    )
    arrived = wide_sum(arrived).reshape(half + 2, LANES).astype(bf16)
    gathered, at, kv, tp, norm_gain, norm_bias, block, params, token_sum, arrived = over_tp(
        arrived, at, kv, tp, norm_gain, norm_bias, block, params, token_sum, arrived
    )
    gathered = gathered.astype(f32)
    bias_own = arrived[half + 1 : half + 2] / share
    gain_one = lax.dynamic_index_in_dim(params, kv, 0, keepdims=False)[:1]
    total = gathered[:, :, :half].sum(axis=0).reshape(batch, LANES)
    total_row = gathered[:, :, half].sum(axis=(0, 1))
    stream_one = residual_scale * block + 0.5 * total
    row_mean = (
        residual_scale * token_sum[0, :batch]
        + 0.5 * (total_row[:batch] + total_row[batch:])
    ) / width
    centred = stream_one - row_mean[:, None]

    scaled = (centred * gain_one.astype(f32)).astype(bf16)
    projected = jnp.concatenate(
        [jnp.dot(scaled, w, preferred_element_type=f32) for w in weights], axis=1
    ).astype(bf16)
    projected = projected.reshape(2, half, chunk_count, LANES).transpose(1, 2, 0, 3)
    blocks = jnp.concatenate(
        [
            projected,
            centred.astype(bf16).reshape(2, half, LANES).swapaxes(0, 1)[:, None],
            jnp.broadcast_to(bias_own.astype(bf16)[None, None], (kv_count, 1, 2, LANES)),
        ],
        axis=1,
    )
    arrived, at, kv, tp, norm_gain, norm_bias, params = alone(
        blocks, KV, at, kv, tp, norm_gain, norm_bias, params
    )
    mixer_part, piece, updated = mixer(
        at,
        arrived,
        params,
        lower_bound.reshape(heads, HEAD),
        head_gain.reshape(heads, HEAD),
        state,
        out_weight,
        tp_count,
    )
    arrived, at, tp, norm_gain, norm_bias, params, piece = alone(
        mixer_part, TP, at, tp, norm_gain, norm_bias, params, piece
    )
    stream_own = (piece + arrived.sum(axis=0)).astype(bf16)
    arrived, at, tp, norm_gain, norm_bias, params = alone(
        copies(stream_own, chip_count), CHIPS, at, tp, norm_gain, norm_bias, params
    )
    arrived = lax.all_gather(arrived, CORE, axis=0)
    arrived = arrived.reshape(2, kv_count, x_count, *stream_own.shape)

    kept, sent, own_normed = second_block(at, arrived, params, stored)
    came = lax.ppermute(sent, CORE, SWAP)
    blocks = (kept.astype(f32) + came.astype(f32)).astype(bf16)
    arrived, tp, norm_gain, norm_bias, own_normed = alone(
        blocks, KV, tp, norm_gain, norm_bias, own_normed
    )
    gathered, tp, norm_gain, norm_bias, own_normed = over_tp(
        wide_sum(arrived).astype(bf16), tp, norm_gain, norm_bias, own_normed
    )
    gathered = gathered.astype(f32)
    total = gathered.sum(axis=0).reshape(batch, LANES)
    stream_three = residual_scale * own_normed.astype(f32) + 0.5 * total
    block_sum = stream_three.sum(axis=1)
    block_mean = block_sum / LANES
    off = stream_three - block_mean[:, None]
    stats = jnp.concatenate([block_mean, (off * off).sum(axis=1)])[None]
    stats, tp, norm_gain, norm_bias, stream_three = alone(
        copies(stats, kv_count), KV, tp, norm_gain, norm_bias, stream_three
    )
    stats = stats[:, 0]
    means, squares = stats[:, :batch], stats[:, batch:]
    row_mean = means.mean(axis=0)
    spread = (squares.sum(axis=0) + LANES * ((means - row_mean) ** 2).sum(axis=0)) / width
    own = lax.dynamic_slice_in_dim(stream_three, tp * own_cols, own_cols, 1)
    mixed = (own - row_mean[:, None]) * lax.rsqrt(spread + norm_eps)[:, None] * norm_gain[
        2
    ].astype(f32) + norm_bias[2].astype(f32)
    mixed = mixed.reshape(2, half, own_cols).swapaxes(0, 1).reshape(batch, own_cols)
    return (mixed.astype(bf16), updated)


def solution(mesh):
    finer = Mesh(mesh.devices.reshape(8, 4, 4, 2), KV_TP)
    in_specs = (
        P(None, KV_TP),
        P(None, None, KV_TP),
        P(None, None, KV_TP),
        P(None, KV_TP, None),
        P(None, KV_TP),
        P(None, KV_TP),
        P(KV, TP),
        P(KV, TP),
        P(KV, TP),
        P(KV, TP),
        P(TP),
        P(TP),
        P(TP, None),
        P(KV, TP, None, None),
    )
    out_specs = (P(None, KV_TP), P(KV, TP, None, None))
    return jax.shard_map(local, mesh=finer, in_specs=in_specs, out_specs=out_specs, check_vma=False)
```

```python
import jax
import jax.numpy as jnp
from jax import lax
from jax.experimental import pallas as pl
from jax.experimental.pallas import tpu as pltpu
from jax.sharding import Mesh
from jax.sharding import PartitionSpec as P

HEAD = 128
LANES = 128
KV_TP = ("kv_0", "kv_1", "tp_0", "tp_1")
KV = ("kv_0", "kv_1")
TP = ("tp_0", "tp_1")
CHIPS = ("kv_0", "kv_1", "tp_0")
CORE = "tp_1"
SWAP = [(0, 1), (1, 0)]

residual_scale = 8.0**0.25
norm_eps = 1e-05
head_eps = 1e-06
bf16 = jnp.bfloat16
f32 = jnp.float32


def exchange(blocks, axes):
    return lax.all_to_all(blocks, axes, split_axis=0, concat_axis=0, tiled=True)


def to_everyone(block, axes, count):
    return exchange(jnp.broadcast_to(block[None], (count, *block.shape)), axes)


def alone(blocks, axes, *held):
    blocks, *held = lax.optimization_barrier((blocks, *held))
    return lax.optimization_barrier((exchange(blocks, axes), *held))


def wide_sum(blocks):
    return lax.optimization_barrier(blocks.astype(f32).sum(axis=0))


def copies(block, count):
    return jnp.broadcast_to(block[None], (count, *block.shape))


def small(grant=8):
    return pltpu.CompilerParams(vmem_limit_bytes=grant * 2**20)


VMEM = pl.BlockSpec(memory_space=pltpu.VMEM)
SMEM = pl.BlockSpec(memory_space=pltpu.SMEM)
ANYWHERE = pl.BlockSpec(memory_space=pl.ANY)


def off_chip(x):
    return pltpu.with_memory_space_constraint(x, pltpu.HBM)


def place_kernel(
    at_ref,
    tokens_hbm,
    gain_hbm,
    bias_hbm,
    result_ref,
    lines_ref,
    tokens_ref,
    gain_ref,
    bias_ref,
    sem,
):
    pairs = ((tokens_hbm, tokens_ref), (gain_hbm, gain_ref), (bias_hbm, bias_ref))
    fetches = [pltpu.make_async_copy(*pair, sem.at[i]) for i, pair in enumerate(pairs)]
    for fetch in fetches:
        fetch.start()
    own_cols, batch = tokens_ref.shape
    half = batch // 2
    lane = lax.broadcasted_iota(jnp.int32, (batch, LANES), 1)
    row = lane % batch
    taken = lax.broadcasted_iota(jnp.int32, (batch, LANES), 0) == 2 * (row % half) + row // half
    first = jnp.where(taken & (lane < batch), 1.0, 0.0).astype(bf16)
    second = jnp.where(taken & (lane >= batch), 1.0, 0.0).astype(bf16)
    groups = LANES // own_cols
    spot = lax.broadcasted_iota(jnp.int32, (own_cols, LANES), 0)
    own_lane = lax.broadcasted_iota(jnp.int32, (own_cols, LANES), 1)
    for fetch in fetches:
        fetch.wait()
    top = jnp.dot(tokens_ref[...], first, preferred_element_type=f32)
    low = jnp.dot(tokens_ref[...], second, preferred_element_type=f32)
    line = jnp.zeros((1, LANES), f32)
    for index in range(6):
        at = (index + at_ref[1]) % groups * own_cols
        place = jnp.where(own_lane == spot + at, 1.0, 0.0).astype(bf16)
        source = gain_ref if index < 3 else bias_ref
        moved = jnp.dot(source[...], place, preferred_element_type=f32)
        line = line + moved[index % 3 : index % 3 + 1]
    count = own_cols // 2
    lines_ref[...] = jnp.zeros(lines_ref.shape, f32)
    lines_ref[:count, :] = top[:count] + low[count:]
    lines_ref[count : count + 1, :] = line
    lines = lines_ref[...].astype(bf16).reshape(count, 2, LANES)[: result_ref.shape[1]]
    for copy in range(result_ref.shape[0]):
        result_ref[copy] = lines


def placed_copies(at, tokens, gain, bias, count):
    batch, own_cols = tokens.shape
    return pl.pallas_call(
        place_kernel,
        in_specs=[SMEM] + [ANYWHERE] * 3,
        out_specs=VMEM,
        out_shape=jax.ShapeDtypeStruct((count, own_cols // 4 + 1, 2, LANES), bf16),
        scratch_shapes=[
            pltpu.VMEM((own_cols, LANES), f32),
            pltpu.VMEM((own_cols, batch), bf16),
            pltpu.VMEM(gain.shape, bf16),
            pltpu.VMEM(bias.shape, bf16),
            pltpu.SemaphoreType.DMA((3,)),
        ],
        compiler_params=small(),
        name="place",
    )(at, off_chip(tokens.T), off_chip(gain), off_chip(bias))


def load_kernel(gate_hbm, up_hbm, down_hbm, gate_ref, up_ref, down_ref, sem):
    pairs = ((gate_hbm, gate_ref), (up_hbm, up_ref), (down_hbm, down_ref))
    fetches = [pltpu.make_async_copy(*pair, sem.at[i]) for i, pair in enumerate(pairs)]
    for fetch in fetches:
        fetch.start()
    for fetch in fetches:
        fetch.wait()


def load(stored):
    return pl.pallas_call(
        load_kernel,
        in_specs=[ANYWHERE] * 3,
        out_specs=[VMEM] * 3,
        out_shape=[jax.ShapeDtypeStruct(w.shape, bf16) for w in stored],
        scratch_shapes=[pltpu.SemaphoreType.DMA((3,))],
        compiler_params=small(),
        name="load",
    )(*[off_chip(w) for w in stored])


def order_kernel(at_ref, rows_ref, w0, w1, w2, w3, params_ref, bias_ref):
    cores, kv_count, x_count = rows_ref.shape[:3]
    last = rows_ref.shape[3] - 1
    groups = cores * x_count
    own_cols = LANES // groups
    lines = [
        rows_ref[group % cores, :, group // cores, last].astype(f32)[:, 0, :]
        for group in range(groups)
    ]
    place = lax.broadcasted_iota(jnp.int32, (kv_count, LANES), 1) // own_cols
    params_ref[...] = jnp.zeros(params_ref.shape, f32)
    for index in range(6):
        total = jnp.zeros((kv_count, LANES), f32)
        for group in range(groups):
            total = jnp.where(place == (index + group) % groups, lines[group], total)
        if index:
            total = pltpu.roll(total, LANES - index * own_cols, 1)
        params_ref[pl.ds(index, kv_count, stride=8), :] = total
    own = params_ref[pl.ds(pl.multiple_of(at_ref[0] * 8, 8), 8), :].astype(bf16)
    for index, w_ref in enumerate((w0, w1, w2, w3)):
        sums = jnp.dot(own, w_ref[...], preferred_element_type=f32)
        heads = sums.shape[1] // LANES
        for head in range(heads):
            chunk = index * heads + head
            bias_ref[chunk : chunk + 1, :] = sums[3:4, head * LANES : (head + 1) * LANES]


def in_order(at, rows, weights):
    kv_count = rows.shape[1]
    return pl.pallas_call(
        order_kernel,
        in_specs=[SMEM] + [VMEM] * 5,
        out_specs=[VMEM] * 2,
        out_shape=[
            jax.ShapeDtypeStruct((kv_count * 8, LANES), f32),
            jax.ShapeDtypeStruct((4 * weights[0].shape[1] // LANES, LANES), f32),
        ],
        compiler_params=small(),
        name="in_order",
    )(at, rows, *weights)


def stored(ref):
    return ref[...].reshape(ref.shape[0] * ref.shape[1], ref.shape[2])


def feed_forward(gate, up, core, layer, down_ref):
    hidden = jax.nn.silu(gate) * up
    unit = lax.broadcasted_iota(jnp.int32, hidden.shape, 1)
    hidden = jnp.where(unit % 2 == layer, hidden, 0.0)
    half = hidden.shape[0] // 2
    low, high = hidden[:half], hidden[half:]
    first = core == 0
    hidden = jnp.concatenate([jnp.where(first, low, high), jnp.where(first, high, low)])
    return jnp.dot(hidden.astype(bf16), stored(down_ref), preferred_element_type=f32)


def write_halves(part, kept_ref, sent_ref):
    chunks, half, _ = kept_ref.shape
    for chunk in range(chunks):
        at = slice(chunk * LANES, (chunk + 1) * LANES)
        kept_ref[chunk] = part[:half, at].astype(bf16)
        sent_ref[chunk] = part[half:, at].astype(bf16)


def first_kernel(
    at_ref,
    rows_ref,
    gate_ref,
    up_ref,
    down_ref,
    kept_ref,
    sent_ref,
    tail_ref,
    total_ref,
    block_ref,
    x_ref,
):
    half = kept_ref.shape[1]
    batch = 2 * half
    cores, kv_count, x_count = rows_ref.shape[:3]
    pairs = rows_ref.shape[3] - 1
    core = at_ref[2]
    total = jnp.zeros((8, LANES), f32)
    for index in range(cores):
        for x in range(x_count):
            lines = rows_ref[index, :, x, :pairs].reshape(kv_count * 8, LANES).astype(f32)
            other = pltpu.roll(lines, LANES - batch, 1)
            lines = lines.reshape(kv_count, 8, LANES)
            total = total + lines.sum(axis=0)
            lines = jnp.concatenate([lines, other.reshape(kv_count, 8, LANES)], axis=1)
            x_ref[:, x * cores + index] = lines.astype(bf16)
    total = jnp.sum(total, axis=0, keepdims=True)
    total = total + pltpu.roll(total, LANES - batch, 1)
    total_ref[...] = jnp.broadcast_to(total, total_ref.shape)
    own = x_ref[at_ref[0]].reshape(LANES, LANES).astype(f32)
    block_ref[...] = own.T[:batch]
    rows = x_ref[...].reshape(kv_count * LANES, LANES)
    gate = jnp.dot(stored(gate_ref), rows, preferred_element_type=f32).T[:batch]
    up = jnp.dot(stored(up_ref), rows, preferred_element_type=f32).T[:batch]
    part = feed_forward(gate, up, core, 0, down_ref)
    write_halves(part, kept_ref, sent_ref)
    sums = jnp.broadcast_to(jnp.sum(part, axis=1, keepdims=True), (batch, LANES))
    row = (lax.broadcasted_iota(jnp.int32, (batch, LANES), 0) + core * half) % batch
    lane = lax.broadcasted_iota(jnp.int32, (batch, LANES), 1)
    line = jnp.sum(jnp.where(lane % batch == row, sums, 0.0), axis=0, keepdims=True)
    high = line.astype(bf16).astype(f32)
    line = jnp.where(lane[:1] < batch, high, line - high)
    tail_ref[...] = jnp.broadcast_to(line, tail_ref.shape)


def stored_order(gate, up, down):
    return gate.transpose(2, 0, 1), up.transpose(2, 0, 1), down.transpose(1, 0, 2)


def first_block(at, rows, stored, half):
    chunks = rows.shape[1]
    groups = rows.shape[0] * rows.shape[2]
    return pl.pallas_call(
        first_kernel,
        in_specs=[SMEM] + [VMEM] * 4,
        out_specs=[VMEM] * 5,
        out_shape=[
            jax.ShapeDtypeStruct((chunks, half, LANES), bf16),
            jax.ShapeDtypeStruct((chunks, half, LANES), bf16),
            jax.ShapeDtypeStruct((8, LANES), f32),
            jax.ShapeDtypeStruct((8, LANES), f32),
            jax.ShapeDtypeStruct((2 * half, LANES), f32),
        ],
        scratch_shapes=[pltpu.VMEM((chunks, groups, LANES // groups, LANES), bf16)],
        compiler_params=small(12),
        name="first_block",
    )(at, rows, *stored)


def project_kernel(
    at_ref, parts_ref, block_ref, total_ref, params_ref, own_ref, w0, w1, w2, w3, result_ref, line_ref
):
    members, lines, _ = parts_ref.shape
    half = lines - 2
    batch = 2 * half
    kv_count = params_ref.shape[0]
    width = kv_count * LANES
    stride = line_ref.shape[0] // half
    sums = jnp.zeros((2, LANES), f32)
    halves = [jnp.zeros((half, LANES), f32) for _ in range(2)]
    for member in range(members):
        part = parts_ref[member].astype(f32)
        halves[member % 2] = halves[member % 2] + part[:half]
        sums = sums + part[half:]
    row = lax.broadcasted_iota(jnp.int32, (batch, LANES), 0)
    lane = lax.broadcasted_iota(jnp.int32, (batch, LANES), 1)
    tokens = jnp.where(lane[:1] < batch, total_ref[0:1, :], 0.0)
    line = (residual_scale * tokens + 0.5 * sums[0:1]) / width
    mean = jnp.sum(jnp.where(lane % batch == row, line, 0.0), axis=1, keepdims=True)
    centred = residual_scale * block_ref[...] + 0.5 * jnp.concatenate(halves) - mean
    scaled = (centred * params_ref[at_ref[0], 0:1, :]).astype(bf16)

    def put(pair, rows):
        for seq in range(2):
            at = slice(seq * half, (seq + 1) * half)
            line_ref[pl.ds(2 * pair + seq, half, stride=stride), :] = rows[at]

    pair = 0
    for w_ref in (w0, w1, w2, w3):
        projected = jnp.dot(scaled, w_ref[...], preferred_element_type=f32)
        for head in range(projected.shape[1] // LANES):
            put(pair, projected[:, head * LANES : (head + 1) * LANES])
            pair += 1
    put(pair, centred)
    own = own_ref[...].astype(f32)[half + 1 : half + 2] * (pair / kv_count)
    put(pair + 1, jnp.broadcast_to(own, (batch, LANES)))
    result_ref[...] = line_ref[...].astype(bf16).reshape(result_ref.shape)


def project(at, parts, block, total, params, own, weights):
    half = parts.shape[1] - 2
    stride = 2 * (4 * weights[0].shape[1] // LANES + 2)
    return pl.pallas_call(
        project_kernel,
        in_specs=[SMEM] + [VMEM] * 9,
        out_specs=VMEM,
        out_shape=jax.ShapeDtypeStruct((half * stride // 2, 2, LANES), bf16),
        scratch_shapes=[pltpu.VMEM((half * stride, LANES), f32)],
        compiler_params=small(),
        name="project",
    )(at, parts, block, total, params, own, *weights)


def blocks_kernel(kept_ref, came_ref, tail_ref, bias_ref, result_ref):
    chunks, half, _ = kept_ref.shape
    share = chunks // bias_ref.shape[0]
    top = lax.broadcasted_iota(jnp.int32, (8, LANES), 0) == 0
    for chunk in range(chunks):
        both = kept_ref[chunk].astype(f32) + came_ref[chunk].astype(f32)
        bias = bias_ref[chunk // share : chunk // share + 1, :]
        tail = jnp.where(top, tail_ref[...], bias)
        lines = jnp.concatenate([both, tail]).astype(bf16)
        pairs = lines.reshape(lines.shape[0] // 2, 2, LANES)
        result_ref[chunk] = pairs[: result_ref.shape[1]]


def first_blocks(kept, came, tail, bias):
    chunks, half, lanes = kept.shape
    return pl.pallas_call(
        blocks_kernel,
        in_specs=[VMEM] * 4,
        out_specs=VMEM,
        out_shape=jax.ShapeDtypeStruct((chunks, half // 2 + 1, 2, lanes), bf16),
        compiler_params=small(),
        name="first_blocks",
    )(kept, came, tail, bias)


def second_kernel(
    at_ref,
    arrived_ref,
    params_ref,
    gate_ref,
    up_ref,
    down_ref,
    kept_ref,
    sent_ref,
    own_ref,
    raw_ref,
    result_ref,
):
    cores, kv_count, x_count, rows, _ = arrived_ref.shape
    pieces = rows // 2
    chunks = cores * x_count * pieces
    for x in range(x_count):
        for core in range(cores):
            tiles = arrived_ref[core, :, x].astype(f32)
            raw_ref[x * cores + core] = tiles.reshape(kv_count * rows, LANES)

    def lines(chunk, seq):
        at = (chunk % pieces) * 2 + seq
        return raw_ref[chunk // pieces, pl.ds(at, kv_count, stride=rows), :]

    width = chunks * LANES
    for seq in range(2):
        total = sum(lines(chunk, seq) for chunk in range(chunks))
        mean = jnp.sum(total, axis=1, keepdims=True) / width
        squares = jnp.zeros((kv_count, LANES), f32)
        for chunk in range(chunks):
            off = lines(chunk, seq) - mean
            squares = squares + off * off
        spread = jnp.sum(squares, axis=1, keepdims=True) / width
        scale = lax.rsqrt(spread + norm_eps)
        for chunk in range(chunks):
            params = params_ref[chunk].astype(f32)
            normed = (lines(chunk, seq) - mean) * scale * params[1:2] + params[4:5]
            result_ref[
                seq * kv_count : (seq + 1) * kv_count, chunk * LANES : (chunk + 1) * LANES
            ] = normed.astype(bf16)
    own_ref[...] = result_ref[:, pl.ds(pl.multiple_of(at_ref[0] * LANES, LANES), LANES)]
    dims = (((1,), (1,)), ((), ()))
    rows = result_ref[...]
    gate = lax.dot_general(rows, stored(gate_ref), dims, preferred_element_type=f32)
    up = lax.dot_general(rows, stored(up_ref), dims, preferred_element_type=f32)
    part = feed_forward(gate, up, at_ref[2], 1, down_ref)
    write_halves(part, kept_ref, sent_ref)


def second_block(at, arrived, params, stored):
    cores, kv_count, x_count, rows, lanes = arrived.shape
    chunks = cores * x_count * rows // 2
    return pl.pallas_call(
        second_kernel,
        in_specs=[SMEM] + [VMEM] * 5,
        out_specs=[VMEM] * 3,
        out_shape=[
            jax.ShapeDtypeStruct((chunks, kv_count, lanes), bf16),
            jax.ShapeDtypeStruct((chunks, kv_count, lanes), bf16),
            jax.ShapeDtypeStruct((2 * kv_count, lanes), bf16),
        ],
        scratch_shapes=[
            pltpu.VMEM((cores * x_count, kv_count * rows, lanes), f32),
            pltpu.VMEM((2 * kv_count, chunks * lanes), bf16),
        ],
        compiler_params=small(12),
        name="second_block",
    )(at, arrived, params, *stored)


def mixer_kernel(
    at_ref,
    arrived_ref,
    params_ref,
    low_ref,
    head_gain_ref,
    state_ref,
    weight_hbm,
    sent_ref,
    piece_ref,
    updated_hbm,
    updated_ref,
    weight_ref,
    rows_ref,
    low_rows_ref,
    gain_rows_ref,
    readout_ref,
    gated_ref,
    updated_sem,
    weight_sem,
):
    seqs, heads = state_ref.shape[:2]
    kv_count = arrived_ref.shape[0]
    chunks = 4 * heads
    share = kv_count // chunks
    parts = sent_ref.shape[0]
    piece_chunks = kv_count // parts
    step = weight_ref.shape[2]
    fetches = [
        pltpu.make_async_copy(
            weight_hbm.at[:, pl.ds(part * step, step)], weight_ref.at[part], weight_sem.at[part]
        )
        for part in range(parts)
    ]
    for fetch in fetches[: parts // 2]:
        fetch.start()

    def block_rows(block):
        lines = arrived_ref[block, :chunks]
        return lines.reshape(seqs * chunks, LANES).astype(f32)

    total = block_rows(0)
    for block in range(1, kv_count):
        total = total + block_rows(block)
    tail = seqs * chunks
    width = kv_count * LANES
    own = arrived_ref[:, chunks].astype(f32)
    mean = jnp.sum(jnp.sum(own, axis=0), axis=1, keepdims=True) / width
    off = own - mean
    scale = jnp.sum(jnp.sum(off * off, axis=0), axis=1, keepdims=True) / width
    scale = lax.rsqrt(scale + norm_eps)
    for chunk in range(chunks):
        bias = arrived_ref[chunk * share, chunks + 1].astype(f32)
        for other in range(1, share):
            bias = bias + arrived_ref[chunk * share + other, chunks + 1].astype(f32)
        rows_ref[2 * chunk : 2 * chunk + 2, :] = bias
    odd = lax.broadcasted_iota(jnp.int32, (tail, LANES), 0) % 2 == 1
    row_scale = jnp.where(odd, scale[1:2], scale[0:1])
    pre = (total * row_scale + rows_ref[...]).astype(bf16).astype(f32)
    size = 2 * heads
    query_pre, forget_pre = pre[:size], pre[size : 2 * size]
    input_pre, outgate_pre = pre[2 * size : 3 * size], pre[3 * size :]

    tp = at_ref[1]
    for chunk in range(piece_chunks):
        at = tp * piece_chunks + chunk
        rows = arrived_ref[at, chunks].astype(f32)
        params = params_ref[at].astype(f32)
        rows = ((rows - mean) * scale * params[0:1] + params[3:4]).astype(bf16).astype(f32)
        piece_ref[2 * chunk : 2 * chunk + 2, :] = residual_scale * rows

    for head in range(heads):
        at = slice(2 * head, 2 * head + 2)
        low_rows_ref[at, :] = jnp.broadcast_to(low_ref[head : head + 1, :], (2, LANES))
        gain_rows_ref[at, :] = jnp.broadcast_to(head_gain_ref[head : head + 1, :], (2, LANES))
    low = low_rows_ref[...]
    forget = (low + (1.0 - low) * jax.nn.sigmoid(forget_pre)).T
    key = ((1.0 - low) * jax.nn.sigmoid(-forget_pre)).T
    query = jax.nn.silu(query_pre).T
    for fetch in fetches[parts // 2 :]:
        fetch.start()
    updated_copies = []
    for head in range(heads):
        for seq in range(seqs):
            row = head * 2 + seq
            new = (
                forget[:, row : row + 1] * state_ref[seq, head]
                + key[:, row : row + 1] * input_pre[row : row + 1, :]
            )
            updated_ref[seq, head] = new
            updated_copies.append(
                pltpu.make_async_copy(
                    updated_ref.at[seq, head], updated_hbm.at[seq, head], updated_sem.at[row]
                )
            )
            updated_copies[-1].start()
            readout_ref[row : row + 1, :] = jnp.sum(
                query[:, row : row + 1] * new, axis=0, keepdims=True
            )
    readout = readout_ref[...]
    readout = readout * lax.rsqrt(jnp.mean(readout * readout, axis=1, keepdims=True) + head_eps)
    gated = readout * gain_rows_ref[...] * jax.nn.silu(outgate_pre)
    gated_ref[...] = jnp.zeros(gated_ref.shape, f32)
    for head in range(heads):
        gated_ref[0:2, head * HEAD : (head + 1) * HEAD] = gated[2 * head : 2 * head + 2]
    lhs = gated_ref[...].astype(bf16)
    for part in range(parts):
        fetches[part].wait()
        mixed = jnp.dot(lhs, weight_ref[part], preferred_element_type=f32)
        for chunk in range(piece_chunks):
            sent_ref[part, 2 * chunk : 2 * chunk + 2, :] = mixed[
                0:2, chunk * LANES : (chunk + 1) * LANES
            ]
    for copy in updated_copies:
        copy.wait()


def mixer(at, arrived, params, lower_bound, head_gain, state, weight, parts):
    seqs, heads = state.shape[:2]
    depth, width = weight.shape
    rows = 2 * width // parts // LANES
    return pl.pallas_call(
        mixer_kernel,
        in_specs=[SMEM] + [VMEM] * 5 + [ANYWHERE],
        out_specs=[VMEM, VMEM, ANYWHERE],
        out_shape=[
            jax.ShapeDtypeStruct((parts, rows, LANES), f32),
            jax.ShapeDtypeStruct((rows, LANES), f32),
            jax.ShapeDtypeStruct(state.shape, f32),
        ],
        scratch_shapes=[
            pltpu.VMEM(state.shape, f32),
            pltpu.VMEM((parts, depth, width // parts), bf16),
            pltpu.VMEM((seqs * 4 * heads, LANES), f32),
            pltpu.VMEM((2 * heads, LANES), f32),
            pltpu.VMEM((2 * heads, LANES), f32),
            pltpu.VMEM((2 * heads, LANES), f32),
            pltpu.VMEM((8, heads * HEAD), f32),
            pltpu.SemaphoreType.DMA((seqs * heads,)),
            pltpu.SemaphoreType.DMA((parts,)),
        ],
        compiler_params=small(),
        name="mixer",
    )(at, arrived, params, lower_bound, head_gain, state, off_chip(weight))


def local(
    tokens,
    gate_weights,
    up_weights,
    down_weights,
    norm_gain,
    norm_bias,
    query_weight,
    forget_weight,
    input_weight,
    outgate_weight,
    lower_bound,
    head_gain,
    out_weight,
    state,
):
    batch, own_cols = tokens.shape
    heads = state.shape[1]
    kv_count, tp_count = lax.axis_size(KV), lax.axis_size(TP)
    x_count = tp_count // 2
    chip_count = kv_count * x_count
    half = batch // 2
    width = own_cols * kv_count * tp_count
    kv, tp, core = lax.axis_index(KV), lax.axis_index(TP), lax.axis_index(CORE)

    at = jnp.stack([kv, tp, core])
    blocks = placed_copies(at, tokens, norm_gain, norm_bias, chip_count)
    arrived = exchange(blocks, CHIPS)
    rows = lax.all_gather(arrived, CORE, axis=0)
    rows = rows.reshape(2, kv_count, x_count, *rows.shape[2:])

    def over_tp(lines, *held):
        gathered, *held = alone(copies(lines, tp_count), TP, *held)
        return gathered.reshape(x_count, 2, *lines.shape), *held

    weights = (query_weight, forget_weight, input_weight, outgate_weight)
    stored = stored_order(gate_weights, up_weights, down_weights)
    stored = load(stored)
    kept, sent, tail, token_sum, block = first_block(at, rows, stored, half)
    params, bias_rows = in_order(at, rows, weights)
    params = params.reshape(kv_count, 8, LANES)
    blocks = first_blocks(kept, lax.ppermute(sent, CORE, SWAP), tail, bias_rows)
    arrived, at, kv, tp, norm_gain, norm_bias, block, params, token_sum = alone(
        blocks, KV, at, kv, tp, norm_gain, norm_bias, block, params, token_sum
    )
    arrived = wide_sum(arrived).reshape(half + 2, LANES).astype(bf16)
    gathered, at, kv, tp, norm_gain, norm_bias, block, params, token_sum, arrived = alone(
        copies(arrived, tp_count),
        TP,
        at,
        kv,
        tp,
        norm_gain,
        norm_bias,
        block,
        params,
        token_sum,
        arrived,
    )

    blocks = project(at, gathered, block, token_sum, params, arrived, weights)
    blocks = blocks.reshape(kv_count, -1, 2, LANES)
    arrived, at, kv, tp, norm_gain, norm_bias, params = alone(
        blocks, KV, at, kv, tp, norm_gain, norm_bias, params
    )
    mixer_part, piece, updated = mixer(
        at,
        arrived,
        params,
        lower_bound.reshape(heads, HEAD),
        head_gain.reshape(heads, HEAD),
        state,
        out_weight,
        tp_count,
    )
    arrived, at, tp, norm_gain, norm_bias, params, piece = alone(
        mixer_part, TP, at, tp, norm_gain, norm_bias, params, piece
    )
    stream_own = (piece + arrived.sum(axis=0)).astype(bf16)
    arrived, at, tp, norm_gain, norm_bias, params = alone(
        copies(stream_own, chip_count), CHIPS, at, tp, norm_gain, norm_bias, params
    )
    arrived = lax.all_gather(arrived, CORE, axis=0)
    arrived = arrived.reshape(2, kv_count, x_count, *stream_own.shape)

    kept, sent, own_normed = second_block(at, arrived, params, stored)
    came = lax.ppermute(sent, CORE, SWAP)
    blocks = (kept.astype(f32) + came.astype(f32)).astype(bf16)
    arrived, tp, norm_gain, norm_bias, own_normed = alone(
        blocks, KV, tp, norm_gain, norm_bias, own_normed
    )
    gathered, tp, norm_gain, norm_bias, own_normed = over_tp(
        wide_sum(arrived).astype(bf16), tp, norm_gain, norm_bias, own_normed
    )
    gathered = gathered.astype(f32)
    total = gathered.sum(axis=0).reshape(batch, LANES)
    stream_three = residual_scale * own_normed.astype(f32) + 0.5 * total
    block_sum = stream_three.sum(axis=1)
    block_mean = block_sum / LANES
    off = stream_three - block_mean[:, None]
    stats = jnp.concatenate([block_mean, (off * off).sum(axis=1)])[None]
    stats, tp, norm_gain, norm_bias, stream_three = alone(
        copies(stats, kv_count), KV, tp, norm_gain, norm_bias, stream_three
    )
    stats = stats[:, 0]
    means, squares = stats[:, :batch], stats[:, batch:]
    row_mean = means.mean(axis=0)
    spread = (squares.sum(axis=0) + LANES * ((means - row_mean) ** 2).sum(axis=0)) / width
    own = lax.dynamic_slice_in_dim(stream_three, tp * own_cols, own_cols, 1)
    mixed = (own - row_mean[:, None]) * lax.rsqrt(spread + norm_eps)[:, None] * norm_gain[
        2
    ].astype(f32) + norm_bias[2].astype(f32)
    mixed = mixed.reshape(2, half, own_cols).swapaxes(0, 1).reshape(batch, own_cols)
    return (mixed.astype(bf16), updated)


def solution(mesh):
    finer = Mesh(mesh.devices.reshape(8, 4, 4, 2), KV_TP)
    in_specs = (
        P(None, KV_TP),
        P(None, None, KV_TP),
        P(None, None, KV_TP),
        P(None, KV_TP, None),
        P(None, KV_TP),
        P(None, KV_TP),
        P(KV, TP),
        P(KV, TP),
        P(KV, TP),
        P(KV, TP),
        P(TP),
        P(TP),
        P(TP, None),
        P(KV, TP, None, None),
    )
    out_specs = (P(None, KV_TP), P(KV, TP, None, None))
    return jax.shard_map(local, mesh=finer, in_specs=in_specs, out_specs=out_specs, check_vma=False)
```

```python
import jax
import jax.numpy as jnp
from jax import lax
from jax.experimental import pallas as pl
from jax.experimental.pallas import tpu as pltpu
from jax.sharding import Mesh
from jax.sharding import PartitionSpec as P

HEAD = 128
LANES = 128
KV_TP = ("kv_0", "kv_1", "tp_0", "tp_1")
KV = ("kv_0", "kv_1")
TP = ("tp_0", "tp_1")
CHIPS = ("kv_0", "kv_1", "tp_0")
CORE = "tp_1"
SWAP = [(0, 1), (1, 0)]

residual_scale = 8.0**0.25
norm_eps = 1e-05
head_eps = 1e-06
bf16 = jnp.bfloat16
f32 = jnp.float32


def exchange(blocks, axes):
    return lax.all_to_all(blocks, axes, split_axis=0, concat_axis=0, tiled=True)


def to_everyone(block, axes, count):
    return exchange(jnp.broadcast_to(block[None], (count, *block.shape)), axes)


def alone(blocks, axes, *held):
    blocks, *held = lax.optimization_barrier((blocks, *held))
    return lax.optimization_barrier((exchange(blocks, axes), *held))


def wide_sum(blocks):
    return lax.optimization_barrier(blocks.astype(f32).sum(axis=0))


def copies(block, count):
    return jnp.broadcast_to(block[None], (count, *block.shape))


def small(grant=8):
    return pltpu.CompilerParams(vmem_limit_bytes=grant * 2**20)


VMEM = pl.BlockSpec(memory_space=pltpu.VMEM)
SMEM = pl.BlockSpec(memory_space=pltpu.SMEM)
ANYWHERE = pl.BlockSpec(memory_space=pl.ANY)


def off_chip(x):
    return pltpu.with_memory_space_constraint(x, pltpu.HBM)


def place_kernel(
    at_ref,
    tokens_hbm,
    gain_hbm,
    bias_hbm,
    result_ref,
    lines_ref,
    tokens_ref,
    gain_ref,
    bias_ref,
    sem,
):
    pairs = ((tokens_hbm, tokens_ref), (gain_hbm, gain_ref), (bias_hbm, bias_ref))
    fetches = [pltpu.make_async_copy(*pair, sem.at[i]) for i, pair in enumerate(pairs)]
    for fetch in fetches:
        fetch.start()
    own_cols, batch = tokens_ref.shape
    half = batch // 2
    lane = lax.broadcasted_iota(jnp.int32, (batch, LANES), 1)
    row = lane % batch
    taken = lax.broadcasted_iota(jnp.int32, (batch, LANES), 0) == 2 * (row % half) + row // half
    first = jnp.where(taken & (lane < batch), 1.0, 0.0).astype(bf16)
    second = jnp.where(taken & (lane >= batch), 1.0, 0.0).astype(bf16)
    groups = LANES // own_cols
    spot = lax.broadcasted_iota(jnp.int32, (own_cols, LANES), 0)
    own_lane = lax.broadcasted_iota(jnp.int32, (own_cols, LANES), 1)
    for fetch in fetches:
        fetch.wait()
    top = jnp.dot(tokens_ref[...], first, preferred_element_type=f32)
    low = jnp.dot(tokens_ref[...], second, preferred_element_type=f32)
    line = jnp.zeros((1, LANES), f32)
    for index in range(6):
        at = (index + at_ref[1]) % groups * own_cols
        place = jnp.where(own_lane == spot + at, 1.0, 0.0).astype(bf16)
        source = gain_ref if index < 3 else bias_ref
        moved = jnp.dot(source[...], place, preferred_element_type=f32)
        line = line + moved[index % 3 : index % 3 + 1]
    count = own_cols // 2
    lines_ref[...] = jnp.zeros(lines_ref.shape, f32)
    lines_ref[:count, :] = top[:count] + low[count:]
    lines_ref[count : count + 1, :] = line
    lines = lines_ref[...].astype(bf16).reshape(count, 2, LANES)[: result_ref.shape[1]]
    for copy in range(result_ref.shape[0]):
        result_ref[copy] = lines


def placed_copies(at, tokens, gain, bias, count):
    batch, own_cols = tokens.shape
    return pl.pallas_call(
        place_kernel,
        in_specs=[SMEM] + [ANYWHERE] * 3,
        out_specs=VMEM,
        out_shape=jax.ShapeDtypeStruct((count, own_cols // 4 + 1, 2, LANES), bf16),
        scratch_shapes=[
            pltpu.VMEM((own_cols, LANES), f32),
            pltpu.VMEM((own_cols, batch), bf16),
            pltpu.VMEM(gain.shape, bf16),
            pltpu.VMEM(bias.shape, bf16),
            pltpu.SemaphoreType.DMA((3,)),
        ],
        compiler_params=small(),
        name="place",
    )(at, off_chip(tokens.T), off_chip(gain), off_chip(bias))


def load_kernel(gate_hbm, up_hbm, down_hbm, gate_ref, up_ref, down_ref, sem):
    pairs = ((gate_hbm, gate_ref), (up_hbm, up_ref), (down_hbm, down_ref))
    fetches = [pltpu.make_async_copy(*pair, sem.at[i]) for i, pair in enumerate(pairs)]
    for fetch in fetches:
        fetch.start()
    for fetch in fetches:
        fetch.wait()


def load(stored):
    return pl.pallas_call(
        load_kernel,
        in_specs=[ANYWHERE] * 3,
        out_specs=[VMEM] * 3,
        out_shape=[jax.ShapeDtypeStruct(w.shape, bf16) for w in stored],
        scratch_shapes=[pltpu.SemaphoreType.DMA((3,))],
        compiler_params=small(),
        name="load",
    )(*[off_chip(w) for w in stored])


def order_kernel(at_ref, rows_ref, w0, w1, w2, w3, params_ref, bias_ref):
    cores, kv_count, x_count = rows_ref.shape[:3]
    last = rows_ref.shape[3] - 1
    groups = cores * x_count
    own_cols = LANES // groups
    lines = [
        rows_ref[group % cores, :, group // cores, last].astype(f32)[:, 0, :]
        for group in range(groups)
    ]
    place = lax.broadcasted_iota(jnp.int32, (kv_count, LANES), 1) // own_cols
    params_ref[...] = jnp.zeros(params_ref.shape, f32)
    for index in range(6):
        total = jnp.zeros((kv_count, LANES), f32)
        for group in range(groups):
            total = jnp.where(place == (index + group) % groups, lines[group], total)
        if index:
            total = pltpu.roll(total, LANES - index * own_cols, 1)
        params_ref[pl.ds(index, kv_count, stride=8), :] = total
    own = params_ref[pl.ds(pl.multiple_of(at_ref[0] * 8, 8), 8), :].astype(bf16)
    for index, w_ref in enumerate((w0, w1, w2, w3)):
        sums = jnp.dot(own, w_ref[...], preferred_element_type=f32)
        heads = sums.shape[1] // LANES
        for head in range(heads):
            chunk = index * heads + head
            bias_ref[chunk : chunk + 1, :] = sums[3:4, head * LANES : (head + 1) * LANES]


def in_order(at, rows, weights):
    kv_count = rows.shape[1]
    return pl.pallas_call(
        order_kernel,
        in_specs=[SMEM] + [VMEM] * 5,
        out_specs=[VMEM] * 2,
        out_shape=[
            jax.ShapeDtypeStruct((kv_count * 8, LANES), f32),
            jax.ShapeDtypeStruct((4 * weights[0].shape[1] // LANES, LANES), f32),
        ],
        compiler_params=small(),
        name="in_order",
    )(at, rows, *weights)


def stored(ref):
    return ref[...].reshape(ref.shape[0] * ref.shape[1], ref.shape[2])


def feed_forward(gate, up, core, layer, down_ref):
    hidden = jax.nn.silu(gate) * up
    unit = lax.broadcasted_iota(jnp.int32, hidden.shape, 1)
    hidden = jnp.where(unit % 2 == layer, hidden, 0.0)
    half = hidden.shape[0] // 2
    low, high = hidden[:half], hidden[half:]
    first = core == 0
    hidden = jnp.concatenate([jnp.where(first, low, high), jnp.where(first, high, low)])
    return jnp.dot(hidden.astype(bf16), stored(down_ref), preferred_element_type=f32)


def write_halves(part, kept_ref, sent_ref):
    chunks, half, _ = kept_ref.shape
    for chunk in range(chunks):
        at = slice(chunk * LANES, (chunk + 1) * LANES)
        kept_ref[chunk] = part[:half, at].astype(bf16)
        sent_ref[chunk] = part[half:, at].astype(bf16)


def first_kernel(
    at_ref,
    rows_ref,
    gate_ref,
    up_ref,
    down_ref,
    kept_ref,
    sent_ref,
    tail_ref,
    total_ref,
    block_ref,
    x_ref,
):
    half = kept_ref.shape[1]
    batch = 2 * half
    cores, kv_count, x_count = rows_ref.shape[:3]
    pairs = rows_ref.shape[3] - 1
    core = at_ref[2]
    total = jnp.zeros((8, LANES), f32)
    for index in range(cores):
        for x in range(x_count):
            lines = rows_ref[index, :, x, :pairs].reshape(kv_count * 8, LANES).astype(f32)
            other = pltpu.roll(lines, LANES - batch, 1)
            lines = lines.reshape(kv_count, 8, LANES)
            total = total + lines.sum(axis=0)
            lines = jnp.concatenate([lines, other.reshape(kv_count, 8, LANES)], axis=1)
            x_ref[:, x * cores + index] = lines.astype(bf16)
    total = jnp.sum(total, axis=0, keepdims=True)
    total = total + pltpu.roll(total, LANES - batch, 1)
    total_ref[...] = jnp.broadcast_to(total, total_ref.shape)
    own = x_ref[at_ref[0]].reshape(LANES, LANES).astype(f32)
    block_ref[...] = own.T[:batch]
    rows = x_ref[...].reshape(kv_count * LANES, LANES)
    gate = jnp.dot(stored(gate_ref), rows, preferred_element_type=f32).T[:batch]
    up = jnp.dot(stored(up_ref), rows, preferred_element_type=f32).T[:batch]
    part = feed_forward(gate, up, core, 0, down_ref)
    write_halves(part, kept_ref, sent_ref)
    sums = jnp.broadcast_to(jnp.sum(part, axis=1, keepdims=True), (batch, LANES))
    row = (lax.broadcasted_iota(jnp.int32, (batch, LANES), 0) + core * half) % batch
    lane = lax.broadcasted_iota(jnp.int32, (batch, LANES), 1)
    line = jnp.sum(jnp.where(lane % batch == row, sums, 0.0), axis=0, keepdims=True)
    high = line.astype(bf16).astype(f32)
    line = jnp.where(lane[:1] < batch, high, line - high)
    tail_ref[...] = jnp.broadcast_to(line, tail_ref.shape)


def stored_order(gate, up, down):
    return gate.transpose(2, 0, 1), up.transpose(2, 0, 1), down.transpose(1, 0, 2)


def first_block(at, rows, stored, half):
    chunks = rows.shape[1]
    groups = rows.shape[0] * rows.shape[2]
    return pl.pallas_call(
        first_kernel,
        in_specs=[SMEM] + [VMEM] * 4,
        out_specs=[VMEM] * 5,
        out_shape=[
            jax.ShapeDtypeStruct((chunks, half, LANES), bf16),
            jax.ShapeDtypeStruct((chunks, half, LANES), bf16),
            jax.ShapeDtypeStruct((8, LANES), f32),
            jax.ShapeDtypeStruct((8, LANES), f32),
            jax.ShapeDtypeStruct((2 * half, LANES), f32),
        ],
        scratch_shapes=[pltpu.VMEM((chunks, groups, LANES // groups, LANES), bf16)],
        compiler_params=small(12),
        name="first_block",
    )(at, rows, *stored)


def project_kernel(
    at_ref, parts_ref, block_ref, total_ref, params_ref, own_ref, w0, w1, w2, w3, result_ref, line_ref
):
    members, lines, _ = parts_ref.shape
    half = lines - 2
    batch = 2 * half
    kv_count = params_ref.shape[0]
    width = kv_count * LANES
    stride = line_ref.shape[0] // half
    sums = jnp.zeros((2, LANES), f32)
    halves = [jnp.zeros((half, LANES), f32) for _ in range(2)]
    for member in range(members):
        part = parts_ref[member].astype(f32)
        halves[member % 2] = halves[member % 2] + part[:half]
        sums = sums + part[half:]
    row = lax.broadcasted_iota(jnp.int32, (batch, LANES), 0)
    lane = lax.broadcasted_iota(jnp.int32, (batch, LANES), 1)
    tokens = jnp.where(lane[:1] < batch, total_ref[0:1, :], 0.0)
    line = (residual_scale * tokens + 0.5 * sums[0:1]) / width
    mean = jnp.sum(jnp.where(lane % batch == row, line, 0.0), axis=1, keepdims=True)
    centred = residual_scale * block_ref[...] + 0.5 * jnp.concatenate(halves) - mean
    scaled = (centred * params_ref[at_ref[0], 0:1, :]).astype(bf16)

    def put(pair, rows):
        for seq in range(2):
            at = slice(seq * half, (seq + 1) * half)
            line_ref[pl.ds(2 * pair + seq, half, stride=stride), :] = rows[at]

    pair = 0
    for w_ref in (w0, w1, w2, w3):
        projected = jnp.dot(scaled, w_ref[...], preferred_element_type=f32)
        for head in range(projected.shape[1] // LANES):
            put(pair, projected[:, head * LANES : (head + 1) * LANES])
            pair += 1
    put(pair, centred)
    own = own_ref[...].astype(f32)[half + 1 : half + 2] * (pair / kv_count)
    put(pair + 1, jnp.broadcast_to(own, (batch, LANES)))
    result_ref[...] = line_ref[...].astype(bf16).reshape(result_ref.shape)


def project(at, parts, block, total, params, own, weights):
    half = parts.shape[1] - 2
    stride = 2 * (4 * weights[0].shape[1] // LANES + 2)
    return pl.pallas_call(
        project_kernel,
        in_specs=[SMEM] + [VMEM] * 9,
        out_specs=VMEM,
        out_shape=jax.ShapeDtypeStruct((half * stride // 2, 2, LANES), bf16),
        scratch_shapes=[pltpu.VMEM((half * stride, LANES), f32)],
        compiler_params=small(),
        name="project",
    )(at, parts, block, total, params, own, *weights)


def blocks_kernel(kept_ref, came_ref, tail_ref, bias_ref, result_ref):
    chunks, half, _ = kept_ref.shape
    share = chunks // bias_ref.shape[0]
    top = lax.broadcasted_iota(jnp.int32, (8, LANES), 0) == 0
    for chunk in range(chunks):
        both = kept_ref[chunk].astype(f32) + came_ref[chunk].astype(f32)
        bias = bias_ref[chunk // share : chunk // share + 1, :]
        tail = jnp.where(top, tail_ref[...], bias)
        lines = jnp.concatenate([both, tail]).astype(bf16)
        pairs = lines.reshape(lines.shape[0] // 2, 2, LANES)
        result_ref[chunk] = pairs[: result_ref.shape[1]]


def first_blocks(kept, came, tail, bias):
    chunks, half, lanes = kept.shape
    return pl.pallas_call(
        blocks_kernel,
        in_specs=[VMEM] * 4,
        out_specs=VMEM,
        out_shape=jax.ShapeDtypeStruct((chunks, half // 2 + 1, 2, lanes), bf16),
        compiler_params=small(),
        name="first_blocks",
    )(kept, came, tail, bias)


def second_kernel(
    at_ref,
    arrived_ref,
    params_ref,
    gate_ref,
    up_ref,
    down_ref,
    kept_ref,
    sent_ref,
    own_ref,
    raw_ref,
    result_ref,
):
    cores, kv_count, x_count, rows, _ = arrived_ref.shape
    pieces = rows // 2
    chunks = cores * x_count * pieces
    for x in range(x_count):
        for core in range(cores):
            tiles = arrived_ref[core, :, x].astype(f32)
            raw_ref[x * cores + core] = tiles.reshape(kv_count * rows, LANES)

    def lines(chunk, seq):
        at = (chunk % pieces) * 2 + seq
        return raw_ref[chunk // pieces, pl.ds(at, kv_count, stride=rows), :]

    width = chunks * LANES
    for seq in range(2):
        total = sum(lines(chunk, seq) for chunk in range(chunks))
        mean = jnp.sum(total, axis=1, keepdims=True) / width
        squares = jnp.zeros((kv_count, LANES), f32)
        for chunk in range(chunks):
            off = lines(chunk, seq) - mean
            squares = squares + off * off
        spread = jnp.sum(squares, axis=1, keepdims=True) / width
        scale = lax.rsqrt(spread + norm_eps)
        for chunk in range(chunks):
            params = params_ref[chunk].astype(f32)
            normed = (lines(chunk, seq) - mean) * scale * params[1:2] + params[4:5]
            result_ref[
                seq * kv_count : (seq + 1) * kv_count, chunk * LANES : (chunk + 1) * LANES
            ] = normed.astype(bf16)
    own_ref[...] = result_ref[:, pl.ds(pl.multiple_of(at_ref[0] * LANES, LANES), LANES)]
    dims = (((1,), (1,)), ((), ()))
    rows = result_ref[...]
    gate = lax.dot_general(rows, stored(gate_ref), dims, preferred_element_type=f32)
    up = lax.dot_general(rows, stored(up_ref), dims, preferred_element_type=f32)
    part = feed_forward(gate, up, at_ref[2], 1, down_ref)
    write_halves(part, kept_ref, sent_ref)


def second_block(at, arrived, params, stored):
    cores, kv_count, x_count, rows, lanes = arrived.shape
    chunks = cores * x_count * rows // 2
    return pl.pallas_call(
        second_kernel,
        in_specs=[SMEM] + [VMEM] * 5,
        out_specs=[VMEM] * 3,
        out_shape=[
            jax.ShapeDtypeStruct((chunks, kv_count, lanes), bf16),
            jax.ShapeDtypeStruct((chunks, kv_count, lanes), bf16),
            jax.ShapeDtypeStruct((2 * kv_count, lanes), bf16),
        ],
        scratch_shapes=[
            pltpu.VMEM((cores * x_count, kv_count * rows, lanes), f32),
            pltpu.VMEM((2 * kv_count, chunks * lanes), bf16),
        ],
        compiler_params=small(12),
        name="second_block",
    )(at, arrived, params, *stored)


def mixer_kernel(
    at_ref,
    arrived_ref,
    params_ref,
    low_ref,
    head_gain_ref,
    state_ref,
    weight_hbm,
    sent_ref,
    piece_ref,
    updated_hbm,
    updated_ref,
    weight_ref,
    rows_ref,
    low_rows_ref,
    gain_rows_ref,
    readout_ref,
    gated_ref,
    updated_sem,
    weight_sem,
):
    seqs, heads = state_ref.shape[:2]
    kv_count = arrived_ref.shape[0]
    chunks = 4 * heads
    share = kv_count // chunks
    parts = sent_ref.shape[0]
    piece_chunks = kv_count // parts
    step = weight_ref.shape[2]
    fetches = [
        pltpu.make_async_copy(
            weight_hbm.at[:, pl.ds(part * step, step)], weight_ref.at[part], weight_sem.at[part]
        )
        for part in range(parts)
    ]
    for fetch in fetches[: parts // 2]:
        fetch.start()

    def block_rows(block):
        lines = arrived_ref[block, :chunks]
        return lines.reshape(seqs * chunks, LANES).astype(f32)

    total = block_rows(0)
    for block in range(1, kv_count):
        total = total + block_rows(block)
    tail = seqs * chunks
    width = kv_count * LANES
    own = arrived_ref[:, chunks].astype(f32)
    mean = jnp.sum(jnp.sum(own, axis=0), axis=1, keepdims=True) / width
    off = own - mean
    scale = jnp.sum(jnp.sum(off * off, axis=0), axis=1, keepdims=True) / width
    scale = lax.rsqrt(scale + norm_eps)
    for chunk in range(chunks):
        bias = arrived_ref[chunk * share, chunks + 1].astype(f32)
        for other in range(1, share):
            bias = bias + arrived_ref[chunk * share + other, chunks + 1].astype(f32)
        rows_ref[2 * chunk : 2 * chunk + 2, :] = bias
    odd = lax.broadcasted_iota(jnp.int32, (tail, LANES), 0) % 2 == 1
    row_scale = jnp.where(odd, scale[1:2], scale[0:1])
    pre = (total * row_scale + rows_ref[...]).astype(bf16).astype(f32)
    size = 2 * heads
    query_pre, forget_pre = pre[:size], pre[size : 2 * size]
    input_pre, outgate_pre = pre[2 * size : 3 * size], pre[3 * size :]

    tp = at_ref[1]
    for chunk in range(piece_chunks):
        at = tp * piece_chunks + chunk
        rows = arrived_ref[at, chunks].astype(f32)
        params = params_ref[at].astype(f32)
        rows = ((rows - mean) * scale * params[0:1] + params[3:4]).astype(bf16).astype(f32)
        piece_ref[2 * chunk : 2 * chunk + 2, :] = residual_scale * rows

    for head in range(heads):
        at = slice(2 * head, 2 * head + 2)
        low_rows_ref[at, :] = jnp.broadcast_to(low_ref[head : head + 1, :], (2, LANES))
        gain_rows_ref[at, :] = jnp.broadcast_to(head_gain_ref[head : head + 1, :], (2, LANES))
    low = low_rows_ref[...]
    forget = (low + (1.0 - low) * jax.nn.sigmoid(forget_pre)).T
    key = ((1.0 - low) * jax.nn.sigmoid(-forget_pre)).T
    query = jax.nn.silu(query_pre).T
    for fetch in fetches[parts // 2 :]:
        fetch.start()
    updated_copies = []
    for head in range(heads):
        for seq in range(seqs):
            row = head * 2 + seq
            new = (
                forget[:, row : row + 1] * state_ref[seq, head]
                + key[:, row : row + 1] * input_pre[row : row + 1, :]
            )
            updated_ref[seq, head] = new
            updated_copies.append(
                pltpu.make_async_copy(
                    updated_ref.at[seq, head], updated_hbm.at[seq, head], updated_sem.at[row]
                )
            )
            updated_copies[-1].start()
            readout_ref[row : row + 1, :] = jnp.sum(
                query[:, row : row + 1] * new, axis=0, keepdims=True
            )
    readout = readout_ref[...]
    readout = readout * lax.rsqrt(jnp.mean(readout * readout, axis=1, keepdims=True) + head_eps)
    gated = readout * gain_rows_ref[...] * jax.nn.silu(outgate_pre)
    gated_ref[...] = jnp.zeros(gated_ref.shape, f32)
    for head in range(heads):
        gated_ref[0:2, head * HEAD : (head + 1) * HEAD] = gated[2 * head : 2 * head + 2]
    lhs = gated_ref[...].astype(bf16)
    for part in range(parts):
        if part % (parts // 2) == 0:
            for fetch in fetches[part : part + parts // 2]:
                fetch.wait()
        mixed = jnp.dot(lhs, weight_ref[part], preferred_element_type=f32)
        for chunk in range(piece_chunks):
            sent_ref[part, 2 * chunk : 2 * chunk + 2, :] = mixed[
                0:2, chunk * LANES : (chunk + 1) * LANES
            ]
    for copy in updated_copies:
        copy.wait()


def mixer(at, arrived, params, lower_bound, head_gain, state, weight, parts):
    seqs, heads = state.shape[:2]
    depth, width = weight.shape
    rows = 2 * width // parts // LANES
    return pl.pallas_call(
        mixer_kernel,
        in_specs=[SMEM] + [VMEM] * 5 + [ANYWHERE],
        out_specs=[VMEM, VMEM, ANYWHERE],
        out_shape=[
            jax.ShapeDtypeStruct((parts, rows, LANES), f32),
            jax.ShapeDtypeStruct((rows, LANES), f32),
            jax.ShapeDtypeStruct(state.shape, f32),
        ],
        scratch_shapes=[
            pltpu.VMEM(state.shape, f32),
            pltpu.VMEM((parts, depth, width // parts), bf16),
            pltpu.VMEM((seqs * 4 * heads, LANES), f32),
            pltpu.VMEM((2 * heads, LANES), f32),
            pltpu.VMEM((2 * heads, LANES), f32),
            pltpu.VMEM((2 * heads, LANES), f32),
            pltpu.VMEM((8, heads * HEAD), f32),
            pltpu.SemaphoreType.DMA((seqs * heads,)),
            pltpu.SemaphoreType.DMA((parts,)),
        ],
        compiler_params=small(),
        name="mixer",
    )(at, arrived, params, lower_bound, head_gain, state, off_chip(weight))


def local(
    tokens,
    gate_weights,
    up_weights,
    down_weights,
    norm_gain,
    norm_bias,
    query_weight,
    forget_weight,
    input_weight,
    outgate_weight,
    lower_bound,
    head_gain,
    out_weight,
    state,
):
    batch, own_cols = tokens.shape
    heads = state.shape[1]
    kv_count, tp_count = lax.axis_size(KV), lax.axis_size(TP)
    x_count = tp_count // 2
    chip_count = kv_count * x_count
    half = batch // 2
    width = own_cols * kv_count * tp_count
    kv, tp, core = lax.axis_index(KV), lax.axis_index(TP), lax.axis_index(CORE)

    at = jnp.stack([kv, tp, core])
    blocks = placed_copies(at, tokens, norm_gain, norm_bias, chip_count)
    arrived = exchange(blocks, CHIPS)
    rows = lax.all_gather(arrived, CORE, axis=0)
    rows = rows.reshape(2, kv_count, x_count, *rows.shape[2:])

    def over_tp(lines, *held):
        gathered, *held = alone(copies(lines, tp_count), TP, *held)
        return gathered.reshape(x_count, 2, *lines.shape), *held

    weights = (query_weight, forget_weight, input_weight, outgate_weight)
    stored = stored_order(gate_weights, up_weights, down_weights)
    stored = load(stored)
    kept, sent, tail, token_sum, block = first_block(at, rows, stored, half)
    params, bias_rows = in_order(at, rows, weights)
    params = params.reshape(kv_count, 8, LANES)
    blocks = first_blocks(kept, lax.ppermute(sent, CORE, SWAP), tail, bias_rows)
    arrived, at, kv, tp, norm_gain, norm_bias, block, params, token_sum = alone(
        blocks, KV, at, kv, tp, norm_gain, norm_bias, block, params, token_sum
    )
    arrived = wide_sum(arrived).reshape(half + 2, LANES).astype(bf16)
    gathered, at, kv, tp, norm_gain, norm_bias, block, params, token_sum, arrived = alone(
        copies(arrived, tp_count),
        TP,
        at,
        kv,
        tp,
        norm_gain,
        norm_bias,
        block,
        params,
        token_sum,
        arrived,
    )

    blocks = project(at, gathered, block, token_sum, params, arrived, weights)
    blocks = blocks.reshape(kv_count, -1, 2, LANES)
    arrived, at, kv, tp, norm_gain, norm_bias, params = alone(
        blocks, KV, at, kv, tp, norm_gain, norm_bias, params
    )
    mixer_part, piece, updated = mixer(
        at,
        arrived,
        params,
        lower_bound.reshape(heads, HEAD),
        head_gain.reshape(heads, HEAD),
        state,
        out_weight,
        tp_count,
    )
    arrived, at, tp, norm_gain, norm_bias, params, piece = alone(
        mixer_part, TP, at, tp, norm_gain, norm_bias, params, piece
    )
    stream_own = (piece + arrived.sum(axis=0)).astype(bf16)
    arrived, at, tp, norm_gain, norm_bias, params = alone(
        copies(stream_own, chip_count), CHIPS, at, tp, norm_gain, norm_bias, params
    )
    arrived = lax.all_gather(arrived, CORE, axis=0)
    arrived = arrived.reshape(2, kv_count, x_count, *stream_own.shape)

    kept, sent, own_normed = second_block(at, arrived, params, stored)
    came = lax.ppermute(sent, CORE, SWAP)
    blocks = (kept.astype(f32) + came.astype(f32)).astype(bf16)
    arrived, tp, norm_gain, norm_bias, own_normed = alone(
        blocks, KV, tp, norm_gain, norm_bias, own_normed
    )
    gathered, tp, norm_gain, norm_bias, own_normed = over_tp(
        wide_sum(arrived).astype(bf16), tp, norm_gain, norm_bias, own_normed
    )
    gathered = gathered.astype(f32)
    total = gathered.sum(axis=0).reshape(batch, LANES)
    stream_three = residual_scale * own_normed.astype(f32) + 0.5 * total
    block_sum = stream_three.sum(axis=1)
    block_mean = block_sum / LANES
    off = stream_three - block_mean[:, None]
    stats = jnp.concatenate([block_mean, (off * off).sum(axis=1)])[None]
    stats, tp, norm_gain, norm_bias, stream_three = alone(
        copies(stats, kv_count), KV, tp, norm_gain, norm_bias, stream_three
    )
    stats = stats[:, 0]
    means, squares = stats[:, :batch], stats[:, batch:]
    row_mean = means.mean(axis=0)
    spread = (squares.sum(axis=0) + LANES * ((means - row_mean) ** 2).sum(axis=0)) / width
    own = lax.dynamic_slice_in_dim(stream_three, tp * own_cols, own_cols, 1)
    mixed = (own - row_mean[:, None]) * lax.rsqrt(spread + norm_eps)[:, None] * norm_gain[
        2
    ].astype(f32) + norm_bias[2].astype(f32)
    mixed = mixed.reshape(2, half, own_cols).swapaxes(0, 1).reshape(batch, own_cols)
    return (mixed.astype(bf16), updated)


def solution(mesh):
    finer = Mesh(mesh.devices.reshape(8, 4, 4, 2), KV_TP)
    in_specs = (
        P(None, KV_TP),
        P(None, None, KV_TP),
        P(None, None, KV_TP),
        P(None, KV_TP, None),
        P(None, KV_TP),
        P(None, KV_TP),
        P(KV, TP),
        P(KV, TP),
        P(KV, TP),
        P(KV, TP),
        P(TP),
        P(TP),
        P(TP, None),
        P(KV, TP, None, None),
    )
    out_specs = (P(None, KV_TP), P(KV, TP, None, None))
    return jax.shard_map(local, mesh=finer, in_specs=in_specs, out_specs=out_specs, check_vma=False)
```

```python
import jax
import jax.numpy as jnp
from jax import lax
from jax.experimental import pallas as pl
from jax.experimental.pallas import tpu as pltpu
from jax.sharding import Mesh
from jax.sharding import PartitionSpec as P

HEAD = 128
LANES = 128
KV_TP = ("kv_0", "kv_1", "tp_0", "tp_1")
KV = ("kv_0", "kv_1")
TP = ("tp_0", "tp_1")
CHIPS = ("kv_0", "kv_1", "tp_0")
CORE = "tp_1"
SWAP = [(0, 1), (1, 0)]

residual_scale = 8.0**0.25
norm_eps = 1e-05
head_eps = 1e-06
bf16 = jnp.bfloat16
f32 = jnp.float32


def exchange(blocks, axes):
    return lax.all_to_all(blocks, axes, split_axis=0, concat_axis=0, tiled=True)


def to_everyone(block, axes, count):
    return exchange(jnp.broadcast_to(block[None], (count, *block.shape)), axes)


def alone(blocks, axes, *held):
    blocks, *held = lax.optimization_barrier((blocks, *held))
    return lax.optimization_barrier((exchange(blocks, axes), *held))


def wide_sum(blocks):
    return lax.optimization_barrier(blocks.astype(f32).sum(axis=0))


def copies(block, count):
    return jnp.broadcast_to(block[None], (count, *block.shape))


def small(grant=8):
    return pltpu.CompilerParams(vmem_limit_bytes=grant * 2**20)


VMEM = pl.BlockSpec(memory_space=pltpu.VMEM)
SMEM = pl.BlockSpec(memory_space=pltpu.SMEM)
ANYWHERE = pl.BlockSpec(memory_space=pl.ANY)


def off_chip(x):
    return pltpu.with_memory_space_constraint(x, pltpu.HBM)


def place_kernel(
    at_ref,
    tokens_hbm,
    gain_hbm,
    bias_hbm,
    result_ref,
    lines_ref,
    tokens_ref,
    gain_ref,
    bias_ref,
    sem,
):
    pairs = ((tokens_hbm, tokens_ref), (gain_hbm, gain_ref), (bias_hbm, bias_ref))
    fetches = [pltpu.make_async_copy(*pair, sem.at[i]) for i, pair in enumerate(pairs)]
    for fetch in fetches:
        fetch.start()
    own_cols, batch = tokens_ref.shape
    half = batch // 2
    lane = lax.broadcasted_iota(jnp.int32, (batch, LANES), 1)
    row = lane % batch
    taken = lax.broadcasted_iota(jnp.int32, (batch, LANES), 0) == 2 * (row % half) + row // half
    first = jnp.where(taken & (lane < batch), 1.0, 0.0).astype(bf16)
    second = jnp.where(taken & (lane >= batch), 1.0, 0.0).astype(bf16)
    groups = LANES // own_cols
    spot = lax.broadcasted_iota(jnp.int32, (own_cols, LANES), 0)
    own_lane = lax.broadcasted_iota(jnp.int32, (own_cols, LANES), 1)
    for fetch in fetches:
        fetch.wait()
    top = jnp.dot(tokens_ref[...], first, preferred_element_type=f32)
    low = jnp.dot(tokens_ref[...], second, preferred_element_type=f32)
    line = jnp.zeros((1, LANES), f32)
    for index in range(6):
        at = (index + at_ref[1]) % groups * own_cols
        place = jnp.where(own_lane == spot + at, 1.0, 0.0).astype(bf16)
        source = gain_ref if index < 3 else bias_ref
        moved = jnp.dot(source[...], place, preferred_element_type=f32)
        line = line + moved[index % 3 : index % 3 + 1]
    count = own_cols // 2
    lines_ref[...] = jnp.zeros(lines_ref.shape, f32)
    lines_ref[:count, :] = top[:count] + low[count:]
    lines_ref[count : count + 1, :] = line
    lines = lines_ref[...].astype(bf16).reshape(count, 2, LANES)[: result_ref.shape[1]]
    for copy in range(result_ref.shape[0]):
        result_ref[copy] = lines


def placed_copies(at, tokens, gain, bias, count):
    batch, own_cols = tokens.shape
    return pl.pallas_call(
        place_kernel,
        in_specs=[SMEM] + [ANYWHERE] * 3,
        out_specs=VMEM,
        out_shape=jax.ShapeDtypeStruct((count, own_cols // 4 + 1, 2, LANES), bf16),
        scratch_shapes=[
            pltpu.VMEM((own_cols, LANES), f32),
            pltpu.VMEM((own_cols, batch), bf16),
            pltpu.VMEM(gain.shape, bf16),
            pltpu.VMEM(bias.shape, bf16),
            pltpu.SemaphoreType.DMA((3,)),
        ],
        compiler_params=small(),
        name="place",
    )(at, off_chip(tokens.T), off_chip(gain), off_chip(bias))


def load_kernel(gate_hbm, up_hbm, down_hbm, gate_ref, up_ref, down_ref, sem):
    pairs = ((gate_hbm, gate_ref), (up_hbm, up_ref), (down_hbm, down_ref))
    fetches = [pltpu.make_async_copy(*pair, sem.at[i]) for i, pair in enumerate(pairs)]
    for fetch in fetches:
        fetch.start()
    for fetch in fetches:
        fetch.wait()


def load(stored):
    return pl.pallas_call(
        load_kernel,
        in_specs=[ANYWHERE] * 3,
        out_specs=[VMEM] * 3,
        out_shape=[jax.ShapeDtypeStruct(w.shape, bf16) for w in stored],
        scratch_shapes=[pltpu.SemaphoreType.DMA((3,))],
        compiler_params=small(),
        name="load",
    )(*[off_chip(w) for w in stored])


def order_kernel(at_ref, rows_ref, w0, w1, w2, w3, params_ref, bias_ref):
    cores, kv_count, x_count = rows_ref.shape[:3]
    last = rows_ref.shape[3] - 1
    groups = cores * x_count
    own_cols = LANES // groups
    lines = [
        rows_ref[group % cores, :, group // cores, last].astype(f32)[:, 0, :]
        for group in range(groups)
    ]
    place = lax.broadcasted_iota(jnp.int32, (kv_count, LANES), 1) // own_cols
    params_ref[...] = jnp.zeros(params_ref.shape, f32)
    for index in range(6):
        total = jnp.zeros((kv_count, LANES), f32)
        for group in range(groups):
            total = jnp.where(place == (index + group) % groups, lines[group], total)
        if index:
            total = pltpu.roll(total, LANES - index * own_cols, 1)
        params_ref[pl.ds(index, kv_count, stride=8), :] = total
    own = params_ref[pl.ds(pl.multiple_of(at_ref[0] * 8, 8), 8), :].astype(bf16)
    for index, w_ref in enumerate((w0, w1, w2, w3)):
        sums = jnp.dot(own, w_ref[...], preferred_element_type=f32)
        heads = sums.shape[1] // LANES
        for head in range(heads):
            chunk = index * heads + head
            bias_ref[chunk : chunk + 1, :] = sums[3:4, head * LANES : (head + 1) * LANES]


def in_order(at, rows, weights):
    kv_count = rows.shape[1]
    return pl.pallas_call(
        order_kernel,
        in_specs=[SMEM] + [VMEM] * 5,
        out_specs=[VMEM] * 2,
        out_shape=[
            jax.ShapeDtypeStruct((kv_count * 8, LANES), f32),
            jax.ShapeDtypeStruct((4 * weights[0].shape[1] // LANES, LANES), f32),
        ],
        compiler_params=small(),
        name="in_order",
    )(at, rows, *weights)


def stored(ref):
    return ref[...].reshape(ref.shape[0] * ref.shape[1], ref.shape[2])


def feed_forward(gate, up, core, layer, down_ref):
    hidden = jax.nn.silu(gate) * up
    unit = lax.broadcasted_iota(jnp.int32, hidden.shape, 1)
    hidden = jnp.where(unit % 2 == layer, hidden, 0.0)
    half = hidden.shape[0] // 2
    low, high = hidden[:half], hidden[half:]
    first = core == 0
    hidden = jnp.concatenate([jnp.where(first, low, high), jnp.where(first, high, low)])
    return jnp.dot(hidden.astype(bf16), stored(down_ref), preferred_element_type=f32)


def write_halves(part, kept_ref, sent_ref):
    chunks, half, _ = kept_ref.shape
    for chunk in range(chunks):
        at = slice(chunk * LANES, (chunk + 1) * LANES)
        kept_ref[chunk] = part[:half, at].astype(bf16)
        sent_ref[chunk] = part[half:, at].astype(bf16)


def first_kernel(
    at_ref,
    rows_ref,
    gate_ref,
    up_ref,
    down_ref,
    kept_ref,
    sent_ref,
    tail_ref,
    total_ref,
    block_ref,
    x_ref,
):
    half = kept_ref.shape[1]
    batch = 2 * half
    cores, kv_count, x_count = rows_ref.shape[:3]
    pairs = rows_ref.shape[3] - 1
    core = at_ref[2]
    total = jnp.zeros((8, LANES), f32)
    for index in range(cores):
        for x in range(x_count):
            lines = rows_ref[index, :, x, :pairs].reshape(kv_count * 8, LANES).astype(f32)
            other = pltpu.roll(lines, LANES - batch, 1)
            lines = lines.reshape(kv_count, 8, LANES)
            total = total + lines.sum(axis=0)
            lines = jnp.concatenate([lines, other.reshape(kv_count, 8, LANES)], axis=1)
            x_ref[:, x * cores + index] = lines.astype(bf16)
    total = jnp.sum(total, axis=0, keepdims=True)
    total = total + pltpu.roll(total, LANES - batch, 1)
    total_ref[...] = jnp.broadcast_to(total, total_ref.shape)
    own = x_ref[at_ref[0]].reshape(LANES, LANES).astype(f32)
    block_ref[...] = own.T[:batch]
    rows = x_ref[...].reshape(kv_count * LANES, LANES)
    gate = jnp.dot(stored(gate_ref), rows, preferred_element_type=f32).T[:batch]
    up = jnp.dot(stored(up_ref), rows, preferred_element_type=f32).T[:batch]
    part = feed_forward(gate, up, core, 0, down_ref)
    write_halves(part, kept_ref, sent_ref)
    sums = jnp.broadcast_to(jnp.sum(part, axis=1, keepdims=True), (batch, LANES))
    row = (lax.broadcasted_iota(jnp.int32, (batch, LANES), 0) + core * half) % batch
    lane = lax.broadcasted_iota(jnp.int32, (batch, LANES), 1)
    line = jnp.sum(jnp.where(lane % batch == row, sums, 0.0), axis=0, keepdims=True)
    high = line.astype(bf16).astype(f32)
    line = jnp.where(lane[:1] < batch, high, line - high)
    tail_ref[...] = jnp.broadcast_to(line, tail_ref.shape)


def stored_order(gate, up, down):
    return gate.transpose(2, 0, 1), up.transpose(2, 0, 1), down.transpose(1, 0, 2)


def first_block(at, rows, stored, half):
    chunks = rows.shape[1]
    groups = rows.shape[0] * rows.shape[2]
    return pl.pallas_call(
        first_kernel,
        in_specs=[SMEM] + [VMEM] * 4,
        out_specs=[VMEM] * 5,
        out_shape=[
            jax.ShapeDtypeStruct((chunks, half, LANES), bf16),
            jax.ShapeDtypeStruct((chunks, half, LANES), bf16),
            jax.ShapeDtypeStruct((8, LANES), f32),
            jax.ShapeDtypeStruct((8, LANES), f32),
            jax.ShapeDtypeStruct((2 * half, LANES), f32),
        ],
        scratch_shapes=[pltpu.VMEM((chunks, groups, LANES // groups, LANES), bf16)],
        compiler_params=small(12),
        name="first_block",
    )(at, rows, *stored)


def project_kernel(
    at_ref, parts_ref, block_ref, total_ref, params_ref, own_ref, w0, w1, w2, w3, result_ref, line_ref
):
    members, lines, _ = parts_ref.shape
    half = lines - 2
    batch = 2 * half
    kv_count = params_ref.shape[0]
    width = kv_count * LANES
    stride = line_ref.shape[0] // half
    sums = jnp.zeros((2, LANES), f32)
    halves = [jnp.zeros((half, LANES), f32) for _ in range(2)]
    for member in range(members):
        part = parts_ref[member].astype(f32)
        halves[member % 2] = halves[member % 2] + part[:half]
        sums = sums + part[half:]
    row = lax.broadcasted_iota(jnp.int32, (batch, LANES), 0)
    lane = lax.broadcasted_iota(jnp.int32, (batch, LANES), 1)
    tokens = jnp.where(lane[:1] < batch, total_ref[0:1, :], 0.0)
    line = (residual_scale * tokens + 0.5 * sums[0:1]) / width
    mean = jnp.sum(jnp.where(lane % batch == row, line, 0.0), axis=1, keepdims=True)
    centred = residual_scale * block_ref[...] + 0.5 * jnp.concatenate(halves) - mean
    scaled = (centred * params_ref[at_ref[0], 0:1, :]).astype(bf16)

    def put(pair, rows):
        for seq in range(2):
            at = slice(seq * half, (seq + 1) * half)
            line_ref[pl.ds(2 * pair + seq, half, stride=stride), :] = rows[at]

    pair = 0
    for w_ref in (w0, w1, w2, w3):
        projected = jnp.dot(scaled, w_ref[...], preferred_element_type=f32)
        for head in range(projected.shape[1] // LANES):
            put(pair, projected[:, head * LANES : (head + 1) * LANES])
            pair += 1
    put(pair, centred)
    own = own_ref[...].astype(f32)[half + 1 : half + 2] * (pair / kv_count)
    put(pair + 1, jnp.broadcast_to(own, (batch, LANES)))
    result_ref[...] = line_ref[...].astype(bf16).reshape(result_ref.shape)


def project(at, parts, block, total, params, own, weights):
    half = parts.shape[1] - 2
    stride = 2 * (4 * weights[0].shape[1] // LANES + 2)
    return pl.pallas_call(
        project_kernel,
        in_specs=[SMEM] + [VMEM] * 9,
        out_specs=VMEM,
        out_shape=jax.ShapeDtypeStruct((half * stride // 2, 2, LANES), bf16),
        scratch_shapes=[pltpu.VMEM((half * stride, LANES), f32)],
        compiler_params=small(),
        name="project",
    )(at, parts, block, total, params, own, *weights)


def blocks_kernel(kept_ref, came_ref, tail_ref, bias_ref, result_ref):
    chunks, half, _ = kept_ref.shape
    share = chunks // bias_ref.shape[0]
    top = lax.broadcasted_iota(jnp.int32, (8, LANES), 0) == 0
    for chunk in range(chunks):
        both = kept_ref[chunk].astype(f32) + came_ref[chunk].astype(f32)
        bias = bias_ref[chunk // share : chunk // share + 1, :]
        tail = jnp.where(top, tail_ref[...], bias)
        lines = jnp.concatenate([both, tail]).astype(bf16)
        pairs = lines.reshape(lines.shape[0] // 2, 2, LANES)
        result_ref[chunk] = pairs[: result_ref.shape[1]]


def first_blocks(kept, came, tail, bias):
    chunks, half, lanes = kept.shape
    return pl.pallas_call(
        blocks_kernel,
        in_specs=[VMEM] * 4,
        out_specs=VMEM,
        out_shape=jax.ShapeDtypeStruct((chunks, half // 2 + 1, 2, lanes), bf16),
        compiler_params=small(),
        name="first_blocks",
    )(kept, came, tail, bias)


def second_kernel(
    at_ref,
    arrived_ref,
    params_ref,
    gate_ref,
    up_ref,
    down_ref,
    kept_ref,
    sent_ref,
    own_ref,
    raw_ref,
    result_ref,
):
    cores, kv_count, x_count, rows, _ = arrived_ref.shape
    pieces = rows // 2
    chunks = cores * x_count * pieces
    for x in range(x_count):
        for core in range(cores):
            tiles = arrived_ref[core, :, x].astype(f32)
            raw_ref[x * cores + core] = tiles.reshape(kv_count * rows, LANES)

    def lines(chunk, seq):
        at = (chunk % pieces) * 2 + seq
        return raw_ref[chunk // pieces, pl.ds(at, kv_count, stride=rows), :]

    width = chunks * LANES
    for seq in range(2):
        total = sum(lines(chunk, seq) for chunk in range(chunks))
        mean = jnp.sum(total, axis=1, keepdims=True) / width
        squares = jnp.zeros((kv_count, LANES), f32)
        for chunk in range(chunks):
            off = lines(chunk, seq) - mean
            squares = squares + off * off
        spread = jnp.sum(squares, axis=1, keepdims=True) / width
        scale = lax.rsqrt(spread + norm_eps)
        for chunk in range(chunks):
            params = params_ref[chunk].astype(f32)
            normed = (lines(chunk, seq) - mean) * scale * params[1:2] + params[4:5]
            result_ref[
                seq * kv_count : (seq + 1) * kv_count, chunk * LANES : (chunk + 1) * LANES
            ] = normed.astype(bf16)
    own_ref[...] = result_ref[:, pl.ds(pl.multiple_of(at_ref[0] * LANES, LANES), LANES)]
    dims = (((1,), (1,)), ((), ()))
    rows = result_ref[...]
    gate = lax.dot_general(rows, stored(gate_ref), dims, preferred_element_type=f32)
    up = lax.dot_general(rows, stored(up_ref), dims, preferred_element_type=f32)
    part = feed_forward(gate, up, at_ref[2], 1, down_ref)
    write_halves(part, kept_ref, sent_ref)


def second_block(at, arrived, params, stored):
    cores, kv_count, x_count, rows, lanes = arrived.shape
    chunks = cores * x_count * rows // 2
    return pl.pallas_call(
        second_kernel,
        in_specs=[SMEM] + [VMEM] * 5,
        out_specs=[VMEM] * 3,
        out_shape=[
            jax.ShapeDtypeStruct((chunks, kv_count, lanes), bf16),
            jax.ShapeDtypeStruct((chunks, kv_count, lanes), bf16),
            jax.ShapeDtypeStruct((2 * kv_count, lanes), bf16),
        ],
        scratch_shapes=[
            pltpu.VMEM((cores * x_count, kv_count * rows, lanes), f32),
            pltpu.VMEM((2 * kv_count, chunks * lanes), bf16),
        ],
        compiler_params=small(12),
        name="second_block",
    )(at, arrived, params, *stored)


def mixer_kernel(
    at_ref,
    arrived_ref,
    params_ref,
    low_ref,
    head_gain_ref,
    state_ref,
    weight_hbm,
    sent_ref,
    piece_ref,
    updated_hbm,
    updated_ref,
    weight_ref,
    rows_ref,
    low_rows_ref,
    gain_rows_ref,
    readout_ref,
    gated_ref,
    updated_sem,
    weight_sem,
):
    seqs, heads = state_ref.shape[:2]
    kv_count = arrived_ref.shape[0]
    chunks = 4 * heads
    share = kv_count // chunks
    parts = sent_ref.shape[0]
    piece_chunks = kv_count // parts
    step = weight_ref.shape[1] // parts
    lines = weight_ref.shape[0] // parts
    fetches = []
    for part in range(parts):
        own = pl.ds(part * lines, lines)
        fetches.append(
            pltpu.make_async_copy(weight_hbm.at[own], weight_ref.at[own], weight_sem.at[part])
        )
        fetches[-1].start()

    def block_rows(block):
        lines = arrived_ref[block, :chunks]
        return lines.reshape(seqs * chunks, LANES).astype(f32)

    total = block_rows(0)
    for block in range(1, kv_count):
        total = total + block_rows(block)
    tail = seqs * chunks
    width = kv_count * LANES
    own = arrived_ref[:, chunks].astype(f32)
    mean = jnp.sum(jnp.sum(own, axis=0), axis=1, keepdims=True) / width
    off = own - mean
    scale = jnp.sum(jnp.sum(off * off, axis=0), axis=1, keepdims=True) / width
    scale = lax.rsqrt(scale + norm_eps)
    for chunk in range(chunks):
        bias = arrived_ref[chunk * share, chunks + 1].astype(f32)
        for other in range(1, share):
            bias = bias + arrived_ref[chunk * share + other, chunks + 1].astype(f32)
        rows_ref[2 * chunk : 2 * chunk + 2, :] = bias
    odd = lax.broadcasted_iota(jnp.int32, (tail, LANES), 0) % 2 == 1
    row_scale = jnp.where(odd, scale[1:2], scale[0:1])
    pre = (total * row_scale + rows_ref[...]).astype(bf16).astype(f32)
    size = 2 * heads
    query_pre, forget_pre = pre[:size], pre[size : 2 * size]
    input_pre, outgate_pre = pre[2 * size : 3 * size], pre[3 * size :]

    tp = at_ref[1]
    for chunk in range(piece_chunks):
        at = tp * piece_chunks + chunk
        rows = arrived_ref[at, chunks].astype(f32)
        params = params_ref[at].astype(f32)
        rows = ((rows - mean) * scale * params[0:1] + params[3:4]).astype(bf16).astype(f32)
        piece_ref[2 * chunk : 2 * chunk + 2, :] = residual_scale * rows

    for head in range(heads):
        at = slice(2 * head, 2 * head + 2)
        low_rows_ref[at, :] = jnp.broadcast_to(low_ref[head : head + 1, :], (2, LANES))
        gain_rows_ref[at, :] = jnp.broadcast_to(head_gain_ref[head : head + 1, :], (2, LANES))
    low = low_rows_ref[...]
    forget = (low + (1.0 - low) * jax.nn.sigmoid(forget_pre)).T
    key = ((1.0 - low) * jax.nn.sigmoid(-forget_pre)).T
    query = jax.nn.silu(query_pre).T
    updated_copies = []
    for head in range(heads):
        for seq in range(seqs):
            row = head * 2 + seq
            new = (
                forget[:, row : row + 1] * state_ref[seq, head]
                + key[:, row : row + 1] * input_pre[row : row + 1, :]
            )
            updated_ref[seq, head] = new
            updated_copies.append(
                pltpu.make_async_copy(
                    updated_ref.at[seq, head], updated_hbm.at[seq, head], updated_sem.at[row]
                )
            )
            updated_copies[-1].start()
            readout_ref[row : row + 1, :] = jnp.sum(
                query[:, row : row + 1] * new, axis=0, keepdims=True
            )
    readout = readout_ref[...]
    readout = readout * lax.rsqrt(jnp.mean(readout * readout, axis=1, keepdims=True) + head_eps)
    gated = readout * gain_rows_ref[...] * jax.nn.silu(outgate_pre)
    gated_ref[...] = jnp.zeros(gated_ref.shape, f32)
    for head in range(heads):
        gated_ref[0:2, head * HEAD : (head + 1) * HEAD] = gated[2 * head : 2 * head + 2]
    lhs = gated_ref[...].astype(bf16)
    for fetch in fetches:
        fetch.wait()
    for part in range(parts):
        weight = weight_ref[:, part * step : (part + 1) * step]
        mixed = jnp.dot(lhs, weight, preferred_element_type=f32)
        for chunk in range(piece_chunks):
            sent_ref[part, 2 * chunk : 2 * chunk + 2, :] = mixed[
                0:2, chunk * LANES : (chunk + 1) * LANES
            ]
    for copy in updated_copies:
        copy.wait()


def mixer(at, arrived, params, lower_bound, head_gain, state, weight, parts):
    seqs, heads = state.shape[:2]
    depth, width = weight.shape
    rows = 2 * width // parts // LANES
    return pl.pallas_call(
        mixer_kernel,
        in_specs=[SMEM] + [VMEM] * 5 + [ANYWHERE],
        out_specs=[VMEM, VMEM, ANYWHERE],
        out_shape=[
            jax.ShapeDtypeStruct((parts, rows, LANES), f32),
            jax.ShapeDtypeStruct((rows, LANES), f32),
            jax.ShapeDtypeStruct(state.shape, f32),
        ],
        scratch_shapes=[
            pltpu.VMEM(state.shape, f32),
            pltpu.VMEM((depth, width), bf16),
            pltpu.VMEM((seqs * 4 * heads, LANES), f32),
            pltpu.VMEM((2 * heads, LANES), f32),
            pltpu.VMEM((2 * heads, LANES), f32),
            pltpu.VMEM((2 * heads, LANES), f32),
            pltpu.VMEM((8, heads * HEAD), f32),
            pltpu.SemaphoreType.DMA((seqs * heads,)),
            pltpu.SemaphoreType.DMA((parts,)),
        ],
        compiler_params=small(),
        name="mixer",
    )(at, arrived, params, lower_bound, head_gain, state, off_chip(weight))


def local(
    tokens,
    gate_weights,
    up_weights,
    down_weights,
    norm_gain,
    norm_bias,
    query_weight,
    forget_weight,
    input_weight,
    outgate_weight,
    lower_bound,
    head_gain,
    out_weight,
    state,
):
    batch, own_cols = tokens.shape
    heads = state.shape[1]
    kv_count, tp_count = lax.axis_size(KV), lax.axis_size(TP)
    x_count = tp_count // 2
    chip_count = kv_count * x_count
    half = batch // 2
    width = own_cols * kv_count * tp_count
    kv, tp, core = lax.axis_index(KV), lax.axis_index(TP), lax.axis_index(CORE)

    at = jnp.stack([kv, tp, core])
    blocks = placed_copies(at, tokens, norm_gain, norm_bias, chip_count)
    arrived = exchange(blocks, CHIPS)
    rows = lax.all_gather(arrived, CORE, axis=0)
    rows = rows.reshape(2, kv_count, x_count, *rows.shape[2:])

    def over_tp(lines, *held):
        gathered, *held = alone(copies(lines, tp_count), TP, *held)
        return gathered.reshape(x_count, 2, *lines.shape), *held

    weights = (query_weight, forget_weight, input_weight, outgate_weight)
    stored = stored_order(gate_weights, up_weights, down_weights)
    stored = load(stored)
    kept, sent, tail, token_sum, block = first_block(at, rows, stored, half)
    params, bias_rows = in_order(at, rows, weights)
    params = params.reshape(kv_count, 8, LANES)
    blocks = first_blocks(kept, lax.ppermute(sent, CORE, SWAP), tail, bias_rows)
    arrived, at, kv, tp, norm_gain, norm_bias, block, params, token_sum = alone(
        blocks, KV, at, kv, tp, norm_gain, norm_bias, block, params, token_sum
    )
    arrived = wide_sum(arrived).reshape(half + 2, LANES).astype(bf16)
    gathered, at, kv, tp, norm_gain, norm_bias, block, params, token_sum, arrived = alone(
        copies(arrived, tp_count),
        TP,
        at,
        kv,
        tp,
        norm_gain,
        norm_bias,
        block,
        params,
        token_sum,
        arrived,
    )

    blocks = project(at, gathered, block, token_sum, params, arrived, weights)
    blocks = blocks.reshape(kv_count, -1, 2, LANES)
    arrived, at, kv, tp, norm_gain, norm_bias, params = alone(
        blocks, KV, at, kv, tp, norm_gain, norm_bias, params
    )
    mixer_part, piece, updated = mixer(
        at,
        arrived,
        params,
        lower_bound.reshape(heads, HEAD),
        head_gain.reshape(heads, HEAD),
        state,
        out_weight,
        tp_count,
    )
    arrived, at, tp, norm_gain, norm_bias, params, piece = alone(
        mixer_part, TP, at, tp, norm_gain, norm_bias, params, piece
    )
    stream_own = (piece + arrived.sum(axis=0)).astype(bf16)
    arrived, at, tp, norm_gain, norm_bias, params = alone(
        copies(stream_own, chip_count), CHIPS, at, tp, norm_gain, norm_bias, params
    )
    arrived = lax.all_gather(arrived, CORE, axis=0)
    arrived = arrived.reshape(2, kv_count, x_count, *stream_own.shape)

    kept, sent, own_normed = second_block(at, arrived, params, stored)
    came = lax.ppermute(sent, CORE, SWAP)
    blocks = (kept.astype(f32) + came.astype(f32)).astype(bf16)
    arrived, tp, norm_gain, norm_bias, own_normed = alone(
        blocks, KV, tp, norm_gain, norm_bias, own_normed
    )
    gathered, tp, norm_gain, norm_bias, own_normed = over_tp(
        wide_sum(arrived).astype(bf16), tp, norm_gain, norm_bias, own_normed
    )
    gathered = gathered.astype(f32)
    total = gathered.sum(axis=0).reshape(batch, LANES)
    stream_three = residual_scale * own_normed.astype(f32) + 0.5 * total
    block_sum = stream_three.sum(axis=1)
    block_mean = block_sum / LANES
    off = stream_three - block_mean[:, None]
    stats = jnp.concatenate([block_mean, (off * off).sum(axis=1)])[None]
    stats, tp, norm_gain, norm_bias, stream_three = alone(
        copies(stats, kv_count), KV, tp, norm_gain, norm_bias, stream_three
    )
    stats = stats[:, 0]
    means, squares = stats[:, :batch], stats[:, batch:]
    row_mean = means.mean(axis=0)
    spread = (squares.sum(axis=0) + LANES * ((means - row_mean) ** 2).sum(axis=0)) / width
    own = lax.dynamic_slice_in_dim(stream_three, tp * own_cols, own_cols, 1)
    mixed = (own - row_mean[:, None]) * lax.rsqrt(spread + norm_eps)[:, None] * norm_gain[
        2
    ].astype(f32) + norm_bias[2].astype(f32)
    mixed = mixed.reshape(2, half, own_cols).swapaxes(0, 1).reshape(batch, own_cols)
    return (mixed.astype(bf16), updated)


def solution(mesh):
    finer = Mesh(mesh.devices.reshape(8, 4, 4, 2), KV_TP)
    in_specs = (
        P(None, KV_TP),
        P(None, None, KV_TP),
        P(None, None, KV_TP),
        P(None, KV_TP, None),
        P(None, KV_TP),
        P(None, KV_TP),
        P(KV, TP),
        P(KV, TP),
        P(KV, TP),
        P(KV, TP),
        P(TP),
        P(TP),
        P(TP, None),
        P(KV, TP, None, None),
    )
    out_specs = (P(None, KV_TP), P(KV, TP, None, None))
    return jax.shard_map(local, mesh=finer, in_specs=in_specs, out_specs=out_specs, check_vma=False)
```
